128 devices in a mesh: sp: 32 (over z, y, core), tp: 4 (over x).
Axes of the slice: x: 4, y: 4, z: 4, core: 2. Of those that a mesh axis runs over, the one named last changes fastest.
Arguments:
- residual_entry_input: bfloat16 [32768, 2048], P(('sp', 'tp')), may hold values from -6 to 6
- query_matrix_rows: bfloat16 [32768, 1024], P('sp', 'tp'), may hold values from -6 to 6
- key_matrix_rows: bfloat16 [32768, 1024], P('sp', 'tp'), may hold values from -6 to 6
- value_matrix_rows: bfloat16 [32768, 2048], P('sp', 'tp'), may hold values from -6 to 6
- output_gate_logits: bfloat16 [32768, 2048], P('sp', 'tp'), may hold values from -6 to 6
- input_gate_logits: float32 [32768, 8], P('sp', 'tp'), may hold values from -6 to 6
- forget_gate_logits: float32 [32768, 8], P('sp', 'tp'), may hold values from -8 to 31
- forget_decay_offset: float32 [32768, 8], P('sp', 'tp'), may hold values from -0.7 to 0
- head_norm_gain: float32 [8, 256], P('tp'), may hold values from 0.1 to 1.9
- cell_output_weight: bfloat16 [2048, 2048], P('tp'), may hold values from -0.125 to 0.125
- feedforward_norm_gain: float32 [2048], replicated, may hold values from 0.1 to 1.9
- gate_up_weight: bfloat16 [2048, 5632], P('sp', 'tp'), may hold values from -0.125 to 0.125
- value_up_weight: bfloat16 [2048, 5632], P('sp', 'tp'), may hold values from -0.125 to 0.125
- gate_filter_taps: float32 [3, 5632], P(None, 'tp'), may hold values from -3 to 3
- value_filter_taps: float32 [3, 5632], P(None, 'tp'), may hold values from -3 to 3
- down_projection_weight: bfloat16 [5632, 2048], P('tp', 'sp'), may hold values from -0.078125 to 0.078125
Outputs:
- result: bfloat16 [32768, 2048], P(('sp', 'tp'))
The draws below stay inside these ranges and needn't reach their ends.
All inputs are finite; a program needn't handle non-finite values.
Results may differ from the reference program's by a relative error of at most 0.025.
Values may be sent and summed in bfloat16 or wider, within the bound.
A program may use at most 128 MiB of HBM per device.

```python
import math
import jax
import jax.numpy as jnp
from jax import lax

D = 2048
HEADS = 8
DK = 128
DV = 256
FF = 5632
BLOCK = 128
TOK_DEV = 1024
TOKENS = 32768
HV = 2048
FF_DEV = 1408
N_TP = 4


def draw_forget_gate_logits(key, part):
    key_order = jax.random.fold_in(key, 11)
    key_slow = jax.random.fold_in(key, 12)
    key_fast = jax.random.fold_in(key, 13)
    key_noise = jax.random.fold_in(key, 14)
    order = jax.random.permutation(key_order, HEADS)
    slow_heads = order < HEADS // 2
    slow_rate = math.log(10.0) / (6.0 * TOKENS) * jnp.exp(jax.random.uniform(key_slow, (HEADS,), jnp.float32, math.log(0.5), 0.0))
    fast_rate = 1.0 / 40.0 * jnp.exp(jax.random.uniform(key_fast, (HEADS,), jnp.float32, math.log(0.6), math.log(1.6)))
    head_rate = jnp.where(slow_heads, slow_rate, fast_rate)
    block_index = jnp.arange(TOKENS) // TOK_DEV
    device_factor = (1 + block_index % 2).astype(jnp.float32)
    noise = jnp.clip(jax.random.normal(key_noise, (TOKENS, HEADS), jnp.float32), -4.0, 4.0)
    rate = head_rate[None, :] * device_factor[:, None] * jnp.exp(0.7 * noise)
    capped = jnp.clip(-jnp.log(jnp.expm1(rate)), -6.0, 14.5)
    ratio = capped / 15.0
    return (7.5 * jnp.log((1.0 + ratio) / (1.0 - ratio))).astype(jnp.float32)


def draw_forget_decay_offset(key, part):
    key_where = jax.random.fold_in(key, 21)
    key_depth = jax.random.fold_in(key, 22)
    spots = jax.random.randint(key_where, (2,), 0, TOKENS)
    depth = jax.random.uniform(key_depth, (2, HEADS), jnp.float32, math.log(0.5), math.log(0.8))
    positions = jnp.arange(TOKENS)
    first = jnp.where((positions == spots[0])[:, None], depth[0][None, :], 0.0)
    second = jnp.where((positions == spots[1])[:, None], depth[1][None, :], 0.0)
    return (first + second).astype(jnp.float32)


def steps_of(rng, extent, split, low, top_value):
    def one(axis_at, blocks):
        draws = jax.random.uniform(jax.random.fold_in(jax.random.fold_in(rng, 6), axis_at), (blocks,), jnp.float32, low / len(split), top_value / len(split))
        return jnp.repeat(jnp.exp(draws), extent[axis_at] // blocks).reshape((-1,) + (1,) * (len(extent) - axis_at - 1))

    factor_of = one(*split[0])
    for cut in split[1:]:
        factor_of = factor_of * one(*cut)
    return factor_of


def normal_values(own_key, dims, width, most, cuts=(), kind=jnp.bfloat16):
    array = width * jax.random.normal(own_key, dims, jnp.float32)
    if cuts:
        array = array * steps_of(own_key, dims, cuts, -0.22, 0.18)
    return jnp.clip(array, -most, most).astype(kind)


def setup_inputs(seed: int = 0) -> dict:
    keys = jax.random.split(jax.random.key(seed), 17)
    return {
        "residual_entry_input": normal_values(keys[0], (TOKENS, D), 1.0, 6.0, ((0, 128),)),
        "query_matrix_rows": normal_values(keys[1], (TOKENS, HEADS * DK), 1.0, 6.0, ((0, 32), (1, 4))),
        "key_matrix_rows": normal_values(keys[2], (TOKENS, HEADS * DK), 1.0, 6.0, ((0, 32), (1, 4))),
        "value_matrix_rows": normal_values(keys[3], (TOKENS, HV), 1.0, 6.0, ((0, 32), (1, 4))),
        "output_gate_logits": normal_values(keys[4], (TOKENS, HV), 1.0, 6.0, ((0, 32), (1, 4))),
        "input_gate_logits": normal_values(keys[5], (TOKENS, HEADS), 1.0, 6.0, ((0, 32), (1, 4)), jnp.float32),
        "forget_gate_logits": draw_forget_gate_logits(jax.random.fold_in(keys[16], 71), 0),
        "forget_decay_offset": draw_forget_decay_offset(jax.random.fold_in(keys[16], 71), 0),
        "head_norm_gain": jnp.clip(1.0 + 0.18 * jax.random.normal(keys[8], (HEADS, DV), jnp.float32), 0.1, 1.9),
        "cell_output_weight": normal_values(keys[9], (HV, D), HV ** -0.5, 0.125, ((0, 4),)),
        "feedforward_norm_gain": jnp.clip(1.0 + 0.18 * jax.random.normal(keys[10], (D,), jnp.float32), 0.1, 1.9),
        "gate_up_weight": normal_values(keys[11], (D, FF), D ** -0.5, 0.125, ((0, 32), (1, 4))),
        "value_up_weight": normal_values(keys[12], (D, FF), D ** -0.5, 0.125, ((0, 32), (1, 4))),
        "gate_filter_taps": normal_values(keys[13], (3, FF), 0.577, 3.0, ((1, 4),), jnp.float32),
        "value_filter_taps": normal_values(keys[14], (3, FF), 0.577, 3.0, ((1, 4),), jnp.float32),
        "down_projection_weight": normal_values(keys[15], (FF, D), FF ** -0.5, 0.078125, ((0, 4), (1, 32))),
    }


eps = 1e-06

def gate_log_values(input_gate_logits, forget_gate_logits, forget_decay_offset):
    input_log_value = 15.0 * jnp.tanh(input_gate_logits / 15.0)
    forget_log_sigmoid = jax.nn.log_sigmoid(15.0 * jnp.tanh(forget_gate_logits / 15.0)) + forget_decay_offset
    return (input_log_value, forget_log_sigmoid)

def block_step(state_carry, inputs):
    memory, normer, running = state_carry
    query_block, key_block, value_block, input_block, forget_block = inputs
    length = query_block.shape[0]
    highest = lax.Precision.HIGHEST
    query_scale = DK ** (-0.5)
    query_wide = query_block.astype(jnp.float32)
    key_wide = key_block.astype(jnp.float32)
    value_wide = value_block.astype(jnp.float32)
    causal = jnp.tril(jnp.ones((length, length), dtype=bool))[:, :, None]
    cumulative = jnp.cumsum(forget_block, axis=0)
    logits = cumulative[:, None, :] - cumulative[None, :, :] + input_block[None, :, :]
    logits = jnp.where(causal, logits, -jnp.inf)
    carried = cumulative + running[None, :]
    stable = jnp.maximum(carried, lax.optimization_barrier(jnp.max(logits, axis=1)))
    carry_weight = jnp.exp(carried - stable)
    raw = jnp.einsum('thd,shd->tsh', query_wide, key_wide) * query_scale
    scores = raw * jnp.exp(logits - stable[:, None, :])
    scores_low = scores.astype(jnp.bfloat16).astype(jnp.float32)
    scaled_query = query_wide * query_scale
    numerator = carry_weight[:, :, None] * jnp.einsum('hvd,thd->thv', memory, scaled_query, precision=highest)
    numerator = numerator + jnp.einsum('tsh,shv->thv', scores_low, value_wide)
    denominator = carry_weight * jnp.einsum('hd,thd->th', normer, scaled_query, precision=highest) + lax.optimization_barrier(jnp.sum(scores, axis=1))
    output = numerator / jnp.maximum(jnp.abs(denominator), jnp.exp(-stable))[:, :, None]
    last_sum = cumulative[-1]
    weights_log = last_sum[None, :] - cumulative + input_block
    new_running = jnp.maximum(last_sum + running, lax.optimization_barrier(jnp.max(weights_log, axis=0)))
    decay_factor = jnp.exp(last_sum + running - new_running)
    weighted = key_wide * jnp.exp(weights_log - new_running[None, :])[:, :, None]
    weighted_low = weighted.astype(jnp.bfloat16).astype(jnp.float32)
    memory = decay_factor[:, None, None] * memory + jnp.einsum('shv,shd->hvd', value_wide, weighted_low)
    normer = decay_factor[:, None] * normer + lax.optimization_barrier(jnp.sum(weighted, axis=0))
    return ((memory, normer, new_running), output)

def reference(residual_entry_input, query_matrix_rows, key_matrix_rows, value_matrix_rows, output_gate_logits, input_gate_logits, forget_gate_logits, forget_decay_offset, head_norm_gain, cell_output_weight, feedforward_norm_gain, gate_up_weight, value_up_weight, gate_filter_taps, value_filter_taps, down_projection_weight):
    token_count = query_matrix_rows.shape[0]
    queries = query_matrix_rows.reshape(token_count, HEADS, DK)
    keys_all = key_matrix_rows.reshape(token_count, HEADS, DK)
    values_all = value_matrix_rows.reshape(token_count, HEADS, DV)
    input_log_value, forget_log_sigmoid = gate_log_values(input_gate_logits, forget_gate_logits, forget_decay_offset)
    block_count = token_count // BLOCK

    def blocks(tensor):
        return tensor.reshape((block_count, BLOCK) + tensor.shape[1:])
    initial = (jnp.zeros((HEADS, DV, DK), jnp.float32), jnp.zeros((HEADS, DK), jnp.float32), jnp.zeros((HEADS,), jnp.float32))
    _, outputs = lax.scan(block_step, initial, (blocks(queries), blocks(keys_all), blocks(values_all), blocks(input_log_value), blocks(forget_log_sigmoid)))
    memory_out = outputs.reshape(token_count, HEADS, DV)
    normed = memory_out * lax.rsqrt(lax.optimization_barrier(jnp.mean(memory_out * memory_out, axis=-1, keepdims=True)) + eps) * head_norm_gain[None, :, :]
    gated_rows = (normed.reshape(token_count, HEADS * DV) * jax.nn.sigmoid(output_gate_logits.astype(jnp.float32))).astype(jnp.bfloat16)
    mixed_rows = jnp.dot(gated_rows, cell_output_weight, preferred_element_type=jnp.float32)
    stream = (residual_entry_input.astype(jnp.float32) + mixed_rows).astype(jnp.bfloat16)
    stream_wide = lax.optimization_barrier(stream).astype(jnp.float32)
    normed_rows = (stream_wide * lax.rsqrt(lax.optimization_barrier(jnp.mean(stream_wide * stream_wide, axis=-1, keepdims=True)) + eps) * feedforward_norm_gain[None, :]).astype(jnp.bfloat16)
    padded = jnp.concatenate([jnp.zeros((2, D), jnp.bfloat16), normed_rows], axis=0)
    row_block = min(token_count, 4096)
    pieces = []
    for offset in range(0, token_count, row_block):
        window = padded[offset:offset + row_block + 2]
        up_gate = jnp.dot(window, gate_up_weight, preferred_element_type=jnp.float32)
        up_value = jnp.dot(window, value_up_weight, preferred_element_type=jnp.float32)
        conv_g = gate_filter_taps[0][None, :] * up_gate[:-2] + gate_filter_taps[1][None, :] * up_gate[1:-1] + gate_filter_taps[2][None, :] * up_gate[2:]
        conv_v = value_filter_taps[0][None, :] * up_value[:-2] + value_filter_taps[1][None, :] * up_value[1:-1] + value_filter_taps[2][None, :] * up_value[2:]
        hidden = (jax.nn.silu(conv_g) * conv_v).astype(jnp.bfloat16)
        running_sum = jnp.zeros((row_block, D), jnp.float32)
        for member in range(N_TP):
            lower = member * FF_DEV
            partial_value = jnp.dot(hidden[:, lower:lower + FF_DEV], down_projection_weight[lower:lower + FF_DEV], preferred_element_type=jnp.float32).astype(jnp.bfloat16)
            running_sum = running_sum + lax.optimization_barrier(partial_value).astype(jnp.float32)
        pieces.append((stream_wide[offset:offset + row_block] + running_sum).astype(jnp.bfloat16))
    return jnp.concatenate(pieces, axis=0)
```

```python
import jax
import jax.numpy as jnp
from jax import lax
from jax.experimental import pallas as pl
from jax.experimental.pallas import tpu as pltpu
from jax.sharding import Mesh
from jax.sharding import PartitionSpec as P

SP = ("sp_0", "sp_1", "sp_2")
SP_TP = ("sp_0", "sp_1", "sp_2", "tp")
MESH = pl.DeviceIdType.MESH

EPS = 1e-06
NEG = -1e30
L = 128
CH = 8
DK = 128
DV = 256
D = 2048
FFD = 1408
NT = FFD // 128
SCALE = DK**-0.5
F32 = jnp.float32
BF = jnp.bfloat16


def log1p_of(e):
    series = e * (1.0 - e * (0.5 - e * (1.0 / 3.0 - e * (0.25 - e * 0.2))))
    return jnp.where(e < 0.03, series, jnp.log(1.0 + e))


def kernel(
    res, q_in, k_in, v_in, og_in, ig, fg, off, gain, wo_in, fgain, gup, vup, dwn, gtap, vtap,
    out,
    q, k, v, og, rsd, wgv, wd, wo, dc, nl, colt, rows, cs, cpri, mpri, rs_rows,
    st1, ax1, st1r, ax1r, st2, ax2, st3, ax3, st4, ax4, st4r, ax4r,
    gated, orr, stream, gr, hs, hr, hp, hid, ps, rr,
    lsem, ssem, rsem,
):
    z, y, c, tp = (lax.axis_index(a) for a in SP_TP)

    def up(i, n):
        return lax.rem(i + n, 4)

    y1, y3 = up(y, 1), up(y, 3)
    z1, z3 = up(z, 1), up(z, 3)
    x1, x2, x3 = up(tp, 1), up(tp, 2), up(tp, 3)
    other = 1 - c
    place = z * 8 + y * 2 + c

    def at_place(n):
        n = lax.rem(n + 32, 32)
        return {"sp_0": n // 8, "sp_1": lax.rem(n // 2, 4), "sp_2": lax.rem(n, 2)}

    count = {"l": 0, "s": 0, "r": 0}
    open_sends = []

    def take(kind):
        count[kind] += 1
        return count[kind] - 1

    def load(src, dst):
        cp = pltpu.make_async_copy(src, dst, lsem.at[take("l")])
        cp.start()
        return cp

    def send(src, dst, dev):
        cp = pltpu.make_async_remote_copy(
            src_ref=src, dst_ref=dst, send_sem=ssem.at[take("s")], recv_sem=rsem.at[take("r")],
            device_id=dev, device_id_type=MESH,
        )
        cp.start()
        open_sends.append(cp)
        return cp

    def arrived(copies):
        for cp in copies:
            cp.wait_recv()

    ld_k = load(k_in, k)
    ld_v = load(v_in, v)
    ld_w = [load(dwn, wd.at[z, y, c])]
    for n in range(NT):
        ld_w.append(load(gup.at[:, pl.ds(n * 128, 128)], wgv.at[z, y, c, :, pl.ds(n * 256, 128)]))
        ld_w.append(load(vup.at[:, pl.ds(n * 128, 128)], wgv.at[z, y, c, :, pl.ds(n * 256 + 128, 128)]))
    ld_wo = load(wo_in, wo.at[tp])
    ld_q = load(q_in, q)
    ld_og = load(og_in, og)
    ld_res = load(res, rsd)

    barrier = pltpu.get_barrier_semaphore()

    def hello(dev):
        pl.semaphore_signal(barrier, inc=1, device_id=dev, device_id_type=MESH)

    hello({"sp_2": other})
    for n in (1, 2, 3):
        hello({"sp_1": up(y, n)})
        hello({"sp_0": up(z, n)})
        hello({"tp": up(tp, n)})
    hello({**at_place(place - 1), "tp": 3})

    @pl.when(tp == 3)
    def _():
        for t in range(4):
            hello({**at_place(place + 1), "tp": t})
        pl.semaphore_wait(barrier, 15)

    @pl.when(tp != 3)
    def _():
        pl.semaphore_wait(barrier, 11)

    def halves(ref, zz, yy, lo, n):
        return ref.at[zz, yy, c, pl.ds(lo, n)]

    for cp in ld_w:
        cp.wait()
    p1 = []
    for ref in (wgv, wd):
        mine_a, mine_b = halves(ref, z, y, 0, 32), halves(ref, z, y, 32, 32)
        p1 += [
            send(mine_a, mine_a, {"sp_1": y1}),
            send(mine_a, mine_a, {"sp_1": y3}),
            send(mine_b, mine_b, {"sp_0": z1}),
            send(mine_b, mine_b, {"sp_0": z3}),
        ]
    ld_wo.wait()
    wo_half = wo.at[tp, pl.ds(c * 256, 256)]
    w1 = [send(wo_half, wo_half, {"tp": x1}), send(wo_half, wo_half, {"tp": x3})]

    il = 15.0 * jnp.tanh(ig[...] / 15.0)
    xf = 15.0 * jnp.tanh(fg[...] / 15.0)
    fl = jnp.minimum(xf, 0.0) - log1p_of(jnp.exp(-jnp.abs(xf))) + off[...]
    r_i = lax.broadcasted_iota(jnp.int32, (L, L), 0)
    c_i = lax.broadcasted_iota(jnp.int32, (L, L), 1)
    causal = r_i >= c_i
    upper = (r_i <= c_i).astype(F32)
    cum = jnp.dot(fl, upper, preferred_element_type=F32, precision=lax.Precision.HIGHEST)
    a = il - cum
    lane = lax.broadcasted_iota(jnp.int32, (2 * CH, L), 1)
    cm = a
    for s in (1, 2, 4, 8, 16, 32, 64):
        cm = jnp.where(lane >= s, jnp.maximum(cm, pltpu.roll(cm, s, 1)), cm)
    last = jnp.broadcast_to(cum[:, L - 1 :], (2 * CH, L))
    peak = jnp.broadcast_to(cm[:, L - 1 :], (2 * CH, L))
    weight = jnp.exp(a - peak)
    mm = last + peak
    rows[0], rows[1], rows[2], rows[3] = a, weight, last, mm
    colt[...] = jnp.transpose(jnp.concatenate([cm, cum, jnp.zeros((96, L), F32)], axis=0))

    ld_k.wait()
    ld_v.wait()

    def chunk_state(j, _):
        at = pl.ds(pl.multiple_of(j * L, L), L)
        for h in range(2):
            kt = jnp.transpose(k[at, h * DK : (h + 1) * DK].astype(F32))
            kw = kt * rows[1, pl.ds(2 * j + h, 1), :]
            dc[j, h, :, :DV] = jnp.dot(
                kw.astype(BF), v[at, h * DV : (h + 1) * DV], preferred_element_type=F32
            )
            dc[j, h, :, DV:] = jnp.broadcast_to(jnp.sum(kw, axis=1, keepdims=True), (DK, L))
        return 0

    lax.fori_loop(0, CH, chunk_state, 0)

    for h in range(2):
        tot = jnp.zeros((1, L), F32)
        logs = [None] * CH
        for j in reversed(range(CH)):
            row = 2 * j + h
            logs[j] = mm[row : row + 1] + tot
            tot = tot + last[row : row + 1]
        m = logs[0]
        for j in range(1, CH):
            m = jnp.maximum(m, logs[j])
        total = jnp.zeros((DK, DV + L), F32)
        for j in range(CH):
            total = total + jnp.exp(logs[j] - m)[:, 0:1] * dc[j, h]
        st1[h] = total[:, :DV].astype(BF)
        n_row = jnp.transpose(total[:, DV:])[0:1]
        ax1[h] = jnp.concatenate([n_row, tot, m, jnp.zeros((5, L), F32)], axis=0)

    s1 = [send(st1, st1r, {"sp_2": other}), send(ax1, ax1r, {"sp_2": other})]

    ld_q.wait()

    def within(j, _):
        at = pl.ds(pl.multiple_of(j * L, L), L)
        turned = pltpu.roll(colt[...], lax.rem(L - 2 * j, L), 1)
        for h in range(2):
            raw = lax.dot_general(
                q[at, h * DK : (h + 1) * DK], k[at, h * DK : (h + 1) * DK],
                (((1,), (1,)), ((), ())), preferred_element_type=F32,
            ) * SCALE
            logit = rows[0, pl.ds(2 * j + h, 1), :] - turned[:, h : h + 1]
            sc = raw * jnp.exp(jnp.where(causal, logit, NEG))
            nl[j, h, :, :DV] = jnp.dot(
                sc.astype(BF), v[at, h * DV : (h + 1) * DV], preferred_element_type=F32
            )
            nl[j, h, :, DV:] = jnp.broadcast_to(jnp.sum(sc, axis=1, keepdims=True), (L, L))
        return 0

    lax.fori_loop(0, 2, within, 0)

    cf = jnp.full((1, L), c, jnp.int32).astype(F32)
    arrived(s1)

    def aux(ref, *at):
        block = ref[at] if at else ref[...]
        return block[0:1], block[1:2], block[2:3]

    def pack(n, tot, m):
        return jnp.concatenate([n, tot, m, jnp.zeros((5, L), F32)], axis=0)

    n_o, t_o, m_o = aux(ax1, c)
    n_r, t_r, m_r = aux(ax1r, c)
    log_o = m_o + (1.0 - cf) * t_r
    log_r = m_r + cf * t_o
    m = jnp.maximum(log_o, log_r)
    w_o, w_r = jnp.exp(log_o - m), jnp.exp(log_r - m)
    st2[0] = (w_o[:, 0:1] * st1[c].astype(F32) + w_r[:, 0:1] * st1r[c].astype(F32)).astype(BF)
    ax2[0] = pack(w_o * n_o + w_r * n_r, t_o + t_r, m)
    s2 = []
    for n in (1, 2, 3):
        s2.append(send(st2.at[0], st2.at[n], {"sp_1": up(y, n)}))
        s2.append(send(ax2.at[0], ax2.at[n], {"sp_1": up(y, n)}))

    lax.fori_loop(2, 5, within, 0)

    def scan_of(st, ax, me, whole):
        parts = [aux(ax, n) for n in range(4)]
        mine = jnp.full((1, L), me, jnp.int32)
        below = [None] + [mine >= n for n in (1, 2, 3)]
        zero = jnp.zeros((1, L), F32)
        after = zero
        for n in (1, 2, 3):
            after = after + jnp.where(below[n], 0.0, parts[n][1])
        run, run_up = zero, zero
        log_in, log_all = [None] * 4, [parts[0][2] + after] + [None] * 3
        for n in (1, 2, 3):
            log_in[n] = jnp.where(below[n], parts[n][2] + run, NEG)
            log_all[n] = jnp.where(
                below[n], parts[n][2] + run + parts[0][1] + after, parts[n][2] + run_up
            )
            run = run + jnp.where(below[n], parts[n][1], 0.0)
            run_up = run_up + jnp.where(below[n], 0.0, parts[n][1])
        m_in = jnp.maximum(jnp.maximum(log_in[1], log_in[2]), log_in[3])
        w_in = [None] + [jnp.where(below[n], jnp.exp(log_in[n] - m_in), 0.0) for n in (1, 2, 3)]
        blocks = [st[n].astype(F32) for n in range(4)]
        c_in = sum(w_in[n][:, 0:1] * blocks[n] for n in (1, 2, 3))
        n_in = sum(w_in[n] * parts[n][0] for n in (1, 2, 3))
        inside = (c_in, n_in, run, m_in)
        if not whole:
            return inside, None
        m_all = jnp.maximum(
            jnp.maximum(log_all[0], log_all[1]), jnp.maximum(log_all[2], log_all[3])
        )
        w_all = [jnp.exp(t - m_all) for t in log_all]
        c_all = sum(w_all[n][:, 0:1] * blocks[n] for n in range(4))
        n_all = sum(w_all[n] * parts[n][0] for n in range(4))
        return inside, (c_all, n_all, run + run_up + parts[0][1], m_all)

    arrived(s2)
    y_in, y_all = scan_of(st2, ax2, y, True)
    st3[0] = y_all[0].astype(BF)
    ax3[0] = pack(*y_all[1:])
    s3 = []
    for n in (1, 2, 3):
        s3.append(send(st3.at[0], st3.at[n], {"sp_0": up(z, n)}))
        s3.append(send(ax3.at[0], ax3.at[n], {"sp_0": up(z, n)}))
    cpri[0, :, :DV] = y_in[0]

    lax.fori_loop(5, CH, within, 0)

    arrived(s3)
    z_in, _ = scan_of(st3, ax3, z, False)
    m = jnp.maximum(y_in[2] + z_in[3], y_in[3])
    w_z, w_y = jnp.exp(y_in[2] + z_in[3] - m), jnp.exp(y_in[3] - m)
    st4[...] = (w_z[:, 0:1] * z_in[0] + w_y[:, 0:1] * cpri[0, :, :DV]).astype(BF)
    ax4[...] = pack(w_z * z_in[1] + w_y * y_in[1], z_in[2] + y_in[2], m)
    s4 = [send(st4, st4r, {"sp_2": other}), send(ax4, ax4r, {"sp_2": other})]

    arrived(p1)
    p2 = []
    for ref in (wgv, wd):
        for src, dev in (
            (halves(ref, z, y3, 0, 16), {"sp_1": y1}),
            (halves(ref, z, y1, 16, 16), {"sp_1": y3}),
            (halves(ref, z3, y, 32, 16), {"sp_0": z1}),
            (halves(ref, z1, y, 48, 16), {"sp_0": z3}),
        ):
            p2.append(send(src, src, dev))

    arrived(s4)
    last_in = jnp.full((1, L), c, jnp.int32) == 1
    for h, st, ax in ((c, st4, ax4), (other, st4r, ax4r)):
        n_b, t_b, m_b = aux(ax)
        n_p, t_p, m_p = aux(ax1r, h)
        m_p = jnp.where(last_in, m_p, NEG)
        m_b = m_b + cf * t_p
        m = jnp.maximum(m_b, m_p)
        w_b, w_p = jnp.exp(m_b - m), jnp.where(last_in, jnp.exp(m_p - m), 0.0)
        cpri[h, :, :DV] = w_b[:, 0:1] * st[...].astype(F32) + w_p[:, 0:1] * st1r[h].astype(F32)
        n_row = w_b * n_b + w_p * n_p
        cpri[h, :, DV:] = jnp.transpose(jnp.broadcast_to(n_row, (L, L)))
        mpri[h] = m

    def carry(j, _):
        for h in range(2):
            state, m_old = cpri[h], mpri[h]
            cs[j, h] = state.astype(BF)
            row = pl.ds(2 * j + h, 1)
            rs_rows[row, :] = m_old
            decayed, fresh = rows[2, row, :] + m_old, rows[3, row, :]
            m_new = jnp.maximum(decayed, fresh)
            cpri[h] = (
                jnp.exp(decayed - m_new)[:, 0:1] * state
                + jnp.exp(fresh - m_new)[:, 0:1] * dc[j, h]
            )
            mpri[h] = m_new
        return 0

    lax.fori_loop(0, CH, carry, 0)

    ld_og.wait()

    def finish(j, _):
        at = pl.ds(pl.multiple_of(j * L, L), L)
        turned = pltpu.roll(colt[...], lax.rem(L - 2 * j, L), 1)
        for h in range(2):
            r = rs_rows[pl.ds(2 * j + h, 1), :][:, 0:1]
            cmc, cuc = turned[:, h : h + 1], turned[:, 16 + h : 17 + h]
            g = jnp.maximum(cmc, r)
            e1, e2 = jnp.exp(cmc - g), jnp.exp(r - g) * SCALE
            qc = jnp.dot(q[at, h * DK : (h + 1) * DK], cs[j, h], preferred_element_type=F32)
            both = e1 * nl[j, h] + e2 * qc
            inv = 1.0 / jnp.maximum(jnp.abs(both[:, DV:]), jnp.exp(-cuc - g))
            mo = both[:, :DV] * jnp.concatenate([inv, inv], axis=1)
            norm = lax.rsqrt(jnp.mean(mo * mo, axis=1, keepdims=True) + EPS)
            gate = jax.nn.sigmoid(og[at, h * DV : (h + 1) * DV].astype(F32))
            gated[at, h * DV : (h + 1) * DV] = (mo * norm * gain[h : h + 1, :] * gate).astype(BF)
        return 0

    a2a = []
    for n in (2, 1, 3, 0):
        b = up(tp, n)
        lax.fori_loop(2 * b, 2 * b + 2, finish, 0)
        block = pl.ds(pl.multiple_of(b * 256, 256), 256)
        if n:
            a2a.append(send(gated.at[block], orr.at[tp], {"tp": b}))
        else:
            orr[tp] = gated[block, :]
        if n == 1:
            arrived(w1)
            w2 = []
            for src, lo, dev in ((x3, 0, x1), (x1, 128, x3)):
                part = wo.at[src, pl.ds(c * 256 + lo, 128)]
                w2.append(send(part, part, {"tp": dev}))
            wpair = []
            for src in (x1, x3):
                part = wo.at[src, pl.ds(c * 256, 256)]
                wpair.append(send(part, part, {"sp_2": other}))

    def swap(ref, zz, yy, lo):
        part = ref.at[zz, yy, c, pl.ds(lo, 32)]
        return send(part, part, {"sp_2": other})

    arrived(p2)
    p3, pair = [], []
    for ref in (wgv, wd):
        row_a = ref.at[z, :, c, pl.ds(0, 32)]
        row_b = ref.at[:, y, c, pl.ds(32, 32)]
        p3 += [
            send(row_a, row_a, {"sp_0": z1}),
            send(row_a, row_a, {"sp_0": z3}),
            send(row_b, row_b, {"sp_1": y1}),
            send(row_b, row_b, {"sp_1": y3}),
        ]
        pair.append(send(row_a, row_a, {"sp_2": other}))
        pair.append(send(row_b, row_b, {"sp_2": other}))

    arrived(w2)
    part = wo.at[x2, pl.ds(c * 256, 256)]
    wpair.append(send(part, part, {"sp_2": other}))
    arrived(a2a)
    arrived(wpair)
    ld_res.wait()

    def project(n, ss):
        cols = pl.ds(pl.multiple_of(n * 256, 256), 256)
        acc = rsd[:, cols].astype(F32)
        for t in range(4):
            acc = acc + jnp.dot(orr[t], wo[t, :, cols], preferred_element_type=F32)
        low = acc.astype(BF)
        stream[:, cols] = low
        wide = low.astype(F32)
        sq = wide * wide
        return ss + sq[:, :L] + sq[:, L:]

    ss = lax.fori_loop(0, 8, project, jnp.zeros((256, L), F32))
    norm = lax.rsqrt(jnp.sum(ss, axis=1, keepdims=True) * (1.0 / D) + EPS)

    def normed(n, _):
        cols = pl.ds(pl.multiple_of(n * 256, 256), 256)
        rows_n = (stream[:, cols].astype(F32) * norm * fgain[:, cols]).astype(BF)
        gr[tp, pl.ds(16, 256), cols] = rows_n
        hs[:, cols] = rows_n[254:256].astype(F32)
        return 0

    lax.fori_loop(0, 8, normed, 0)

    hr[tp] = hs[...]
    halo = [send(hs, hr.at[tp], {"tp": up(tp, n)}) for n in (1, 2, 3)]
    s_next = [take("s") for _ in range(4)]
    r_next = take("r")

    def next_copy(t):
        return pltpu.make_async_remote_copy(
            src_ref=hs, dst_ref=hp, send_sem=ssem.at[s_next[t]], recv_sem=rsem.at[r_next],
            device_id={**at_place(place + 1), "tp": t}, device_id_type=MESH,
        )

    @pl.when(tp == 3)
    def _():
        for t in range(4):
            next_copy(t).start()

    own_rows = gr.at[tp, pl.ds(16, 256)]
    g1 = [send(own_rows, own_rows, {"tp": x1}), send(own_rows, own_rows, {"tp": x3})]

    arrived(p3)
    p4 = []
    for ref in (wgv, wd):
        for src, dev in (
            (ref.at[z3, :, c, pl.ds(0, 16)], {"sp_0": z1}),
            (ref.at[z1, :, c, pl.ds(16, 16)], {"sp_0": z3}),
            (ref.at[:, y3, c, pl.ds(32, 16)], {"sp_1": y1}),
            (ref.at[:, y1, c, pl.ds(48, 16)], {"sp_1": y3}),
        ):
            p4.append(send(src, src, dev))
        for src in (
            ref.at[z1, :, c, pl.ds(0, 32)],
            ref.at[z3, :, c, pl.ds(0, 32)],
            ref.at[:, y1, c, pl.ds(32, 32)],
            ref.at[:, y3, c, pl.ds(32, 32)],
        ):
            pair.append(send(src, src, {"sp_2": other}))
    z2, y2 = up(z, 2), up(y, 2)
    arrived(p4)
    for ref in (wgv, wd):
        for src in (ref.at[z2, :, c, pl.ds(0, 32)], ref.at[:, y2, c, pl.ds(32, 32)]):
            pair.append(send(src, src, {"sp_2": other}))
    arrived(halo)
    next_copy(0).wait_recv()
    arrived(pair)

    first = jnp.full((2, D), place, jnp.int32) == 0

    def feed(b, slot):
        from_here = hr[up(b, 3)]
        from_before = jnp.where(first, 0.0, hp[...])
        is_zero = jnp.full((2, D), b, jnp.int32) == 0
        two = jnp.where(is_zero, from_before, from_here)
        gr[b, pl.ds(0, 16), :] = jnp.concatenate([jnp.zeros((14, D), F32), two], axis=0).astype(BF)

        def up_tile(n, _):
            wide = pl.ds(pl.multiple_of(n * 256, 256), 256)
            cols = pl.ds(pl.multiple_of(n * L, L), L)
            w = wgv[:, :, :, :, wide].reshape(D, 256)
            gv = jnp.dot(gr[b], w, preferred_element_type=F32)

            def conv(u, tap):
                return (
                    tap[0:1, cols] * u[14:270] + tap[1:2, cols] * u[15:271] + tap[2:3, cols] * u[16:272]
                )

            cg, cv = conv(gv[:, :L], gtap), conv(gv[:, L:], vtap)
            hid[:, cols] = (cg / (1.0 + jnp.exp(-cg)) * cv).astype(BF)
            return 0

        lax.fori_loop(0, NT, up_tile, 0)

        def down_tile(n, _):
            cols = pl.ds(pl.multiple_of(n * 256, 256), 256)
            w = wd[n // 2, pl.ds(2 * lax.rem(n, 2), 2)].reshape(256, FFD)
            p = lax.dot_general(
                hid[...], w, (((1,), (1,)), ((), ())), preferred_element_type=F32
            )
            ps[slot, :, cols] = p.astype(BF)
            return 0

        lax.fori_loop(0, 8, down_tile, 0)

    feed(tp, 0)
    arrived(g1)
    g2 = []
    for src, lo, dev in ((x3, 16, x1), (x1, 144, x3)):
        part = gr.at[src, pl.ds(lo, 128)]
        g2.append(send(part, part, {"tp": dev}))
    back = []
    for n in (1, 3, 2):
        if n == 2:
            arrived(g2)
        feed(up(tp, n), n)
        back.append(send(ps.at[n], rr.at[n], {"tp": up(tp, n)}))
    arrived(back)

    def add(n, _):
        cols = pl.ds(pl.multiple_of(n * 256, 256), 256)
        s = ps[0, :, cols].astype(F32)
        for t in (1, 2, 3):
            s = s + rr[t, :, cols].astype(F32)
        out[:, cols] = (stream[:, cols].astype(F32) + s).astype(BF)
        return 0

    lax.fori_loop(0, 8, add, 0)

    for cp in open_sends:
        cp.wait_send()

    @pl.when(tp == 3)
    def _():
        for t in range(4):
            next_copy(t).wait_send()


def local(
    residual_entry_input, query_matrix_rows, key_matrix_rows, value_matrix_rows,
    output_gate_logits, input_gate_logits, forget_gate_logits, forget_decay_offset,
    head_norm_gain, cell_output_weight, feedforward_norm_gain, gate_up_weight,
    value_up_weight, gate_filter_taps, value_filter_taps, down_projection_weight,
):
    def chunks(gate):
        return gate.T.reshape(2, CH, L).transpose(1, 0, 2).reshape(2 * CH, L)

    hbm = pl.BlockSpec(memory_space=pl.ANY)
    vmem = pl.BlockSpec(memory_space=pltpu.VMEM)
    scratch = [
        pltpu.VMEM((1024, 256), BF), pltpu.VMEM((1024, 256), BF), pltpu.VMEM((1024, 512), BF),
        pltpu.VMEM((1024, 512), BF), pltpu.VMEM((256, D), BF),
        pltpu.VMEM((4, 4, 2, 64, 2 * FFD), BF), pltpu.VMEM((4, 4, 2, 64, FFD), BF),
        pltpu.VMEM((4, 512, D), BF),
        pltpu.VMEM((CH, 2, DK, DV + L), F32), pltpu.VMEM((CH, 2, L, DV + L), F32),
        pltpu.VMEM((L, L), F32), pltpu.VMEM((4, 2 * CH, L), F32),
        pltpu.VMEM((CH, 2, DK, DV + L), BF), pltpu.VMEM((2, DK, DV + L), F32),
        pltpu.VMEM((2, 1, L), F32), pltpu.VMEM((2 * CH, L), F32),
        pltpu.VMEM((2, DK, DV), BF), pltpu.VMEM((2, 8, L), F32),
        pltpu.VMEM((2, DK, DV), BF), pltpu.VMEM((2, 8, L), F32),
        pltpu.VMEM((4, DK, DV), BF), pltpu.VMEM((4, 8, L), F32),
        pltpu.VMEM((4, DK, DV), BF), pltpu.VMEM((4, 8, L), F32),
        pltpu.VMEM((DK, DV), BF), pltpu.VMEM((8, L), F32),
        pltpu.VMEM((DK, DV), BF), pltpu.VMEM((8, L), F32),
        pltpu.VMEM((1024, 512), BF), pltpu.VMEM((4, 256, 512), BF), pltpu.VMEM((256, D), BF),
        pltpu.VMEM((4, 272, D), BF), pltpu.VMEM((2, D), F32), pltpu.VMEM((4, 2, D), F32),
        pltpu.VMEM((2, D), F32), pltpu.VMEM((256, FFD), BF),
        pltpu.VMEM((4, 256, D), BF), pltpu.VMEM((4, 256, D), BF),
        pltpu.SemaphoreType.DMA((32,)), pltpu.SemaphoreType.DMA((100,)),
        pltpu.SemaphoreType.DMA((100,)),
    ]
    return pl.pallas_call(
        kernel,
        out_shape=jax.ShapeDtypeStruct((256, D), BF),
        in_specs=[hbm, hbm, hbm, hbm, hbm, vmem, vmem, vmem, vmem, hbm, vmem, hbm, hbm, hbm, vmem, vmem],
        out_specs=vmem,
        scratch_shapes=scratch,
        compiler_params=pltpu.CompilerParams(
            collective_id=0, has_side_effects=True, vmem_limit_bytes=67_043_328
        ),
    )(
        residual_entry_input, query_matrix_rows, key_matrix_rows, value_matrix_rows,
        output_gate_logits, chunks(input_gate_logits), chunks(forget_gate_logits),
        chunks(forget_decay_offset), head_norm_gain, cell_output_weight,
        feedforward_norm_gain.reshape(1, D), gate_up_weight, value_up_weight,
        down_projection_weight.T, gate_filter_taps, value_filter_taps,
    )


def solution(mesh):
    split = Mesh(mesh.devices.reshape(4, 4, 2, mesh.shape["tp"]), SP_TP)
    placed = (
        P(SP_TP, None), P(SP, "tp"), P(SP, "tp"), P(SP, "tp"), P(SP, "tp"), P(SP, "tp"),
        P(SP, "tp"), P(SP, "tp"), P("tp", None), P("tp", None), P(), P(SP, "tp"), P(SP, "tp"),
        P(None, "tp"), P(None, "tp"), P("tp", SP),
    )
    return jax.shard_map(
        local, mesh=split, in_specs=placed, out_specs=P(SP_TP, None), check_vma=False
    )
```

```python
import jax
import jax.numpy as jnp
from jax import lax
from jax.experimental import pallas as pl
from jax.experimental.pallas import tpu as pltpu
from jax.sharding import Mesh
from jax.sharding import PartitionSpec as P

SP = ("sp_0", "sp_1", "sp_2")
SP_TP = ("sp_0", "sp_1", "sp_2", "tp")
MESH = pl.DeviceIdType.MESH

EPS = 1e-06
NEG = -1e30
L = 128
CH = 8
DK = 128
DV = 256
D = 2048
FFD = 1408
NT = FFD // 128
SCALE = DK**-0.5
F32 = jnp.float32
BF = jnp.bfloat16


def log1p_of(e):
    series = e * (1.0 - e * (0.5 - e * (1.0 / 3.0 - e * (0.25 - e * 0.2))))
    return jnp.where(e < 0.03, series, jnp.log(1.0 + e))


def kernel(
    res, q_in, k_in, v_in, og_in, ig, fg, off, gain, wo_in, fgain, gup, vup, dwn, gtap, vtap,
    out,
    q, k, v, og, rsd, wgv, wd, wo, dc, nl, colt, rows, cs, cpri, mpri, rs_rows,
    st1, ax1, st1r, ax1r, st2, ax2, st3, ax3, st4, ax4, st4r, ax4r,
    gated, al, orr, stream, gr, hs, hr, hp, gvs, hid, ps, rl, rr,
    lsem, ssem, rsem,
):
    z, y, c, tp = (lax.axis_index(a) for a in SP_TP)

    def up(i, n):
        return lax.rem(i + n, 4)

    y1, y3 = up(y, 1), up(y, 3)
    z1, z3 = up(z, 1), up(z, 3)
    x1, x2, x3 = up(tp, 1), up(tp, 2), up(tp, 3)
    other = 1 - c
    place = z * 8 + y * 2 + c

    def at_place(n):
        n = lax.rem(n + 32, 32)
        return {"sp_0": n // 8, "sp_1": lax.rem(n // 2, 4), "sp_2": lax.rem(n, 2)}

    count = {"l": 0, "s": 0, "r": 0}
    open_sends = []

    def take(kind):
        count[kind] += 1
        return count[kind] - 1

    def load(src, dst):
        cp = pltpu.make_async_copy(src, dst, lsem.at[take("l")])
        cp.start()
        return cp

    def send(src, dst, dev):
        cp = pltpu.make_async_remote_copy(
            src_ref=src, dst_ref=dst, send_sem=ssem.at[take("s")], recv_sem=rsem.at[take("r")],
            device_id=dev, device_id_type=MESH,
        )
        cp.start()
        open_sends.append(cp)
        return cp

    def arrived(copies):
        for cp in copies:
            cp.wait_recv()

    def mark(name):
        pass

    mark('entry')
    ld_k = load(k_in, k)
    ld_v = load(v_in, v)
    ld_w = [load(dwn, wd.at[z, y, c])]
    for n in range(NT):
        ld_w.append(load(gup.at[:, pl.ds(n * 128, 128)], wgv.at[z, y, c, :, pl.ds(n * 256, 128)]))
        ld_w.append(load(vup.at[:, pl.ds(n * 128, 128)], wgv.at[z, y, c, :, pl.ds(n * 256 + 128, 128)]))
    ld_wo = load(wo_in, wo.at[tp])
    ld_q = load(q_in, q)
    ld_og = load(og_in, og)
    ld_res = load(res, rsd)

    barrier = pltpu.get_barrier_semaphore()

    def hello(dev):
        pl.semaphore_signal(barrier, inc=1, device_id=dev, device_id_type=MESH)

    hello({"sp_2": other})
    for n in (1, 2, 3):
        hello({"sp_1": up(y, n)})
        hello({"sp_0": up(z, n)})
        hello({"tp": up(tp, n)})
    hello({**at_place(place - 1), "tp": 3})

    @pl.when(tp == 3)
    def _():
        for t in range(4):
            hello({**at_place(place + 1), "tp": t})
        pl.semaphore_wait(barrier, 15)

    @pl.when(tp != 3)
    def _():
        pl.semaphore_wait(barrier, 11)

    def halves(ref, zz, yy, lo, n):
        return ref.at[zz, yy, c, pl.ds(lo, n)]

    mark('barrier_done')
    for cp in ld_w:
        cp.wait()
    p1 = []
    for ref in (wgv, wd):
        mine_a, mine_b = halves(ref, z, y, 0, 32), halves(ref, z, y, 32, 32)
        p1 += [
            send(mine_a, mine_a, {"sp_1": y1}),
            send(mine_a, mine_a, {"sp_1": y3}),
            send(mine_b, mine_b, {"sp_0": z1}),
            send(mine_b, mine_b, {"sp_0": z3}),
        ]
    mark('w_issued')
    ld_wo.wait()
    wo_half = wo.at[tp, pl.ds(c * 256, 256)]
    w1 = [send(wo_half, wo_half, {"tp": x1}), send(wo_half, wo_half, {"tp": x3})]

    mark('wo_issued')
    il = 15.0 * jnp.tanh(ig[...] / 15.0)
    xf = 15.0 * jnp.tanh(fg[...] / 15.0)
    fl = jnp.minimum(xf, 0.0) - log1p_of(jnp.exp(-jnp.abs(xf))) + off[...]
    r_i = lax.broadcasted_iota(jnp.int32, (L, L), 0)
    c_i = lax.broadcasted_iota(jnp.int32, (L, L), 1)
    causal = r_i >= c_i
    upper = (r_i <= c_i).astype(F32)
    cum = jnp.dot(fl, upper, preferred_element_type=F32, precision=lax.Precision.HIGHEST)
    a = il - cum
    lane = lax.broadcasted_iota(jnp.int32, (2 * CH, L), 1)
    cm = a
    for s in (1, 2, 4, 8, 16, 32, 64):
        cm = jnp.where(lane >= s, jnp.maximum(cm, pltpu.roll(cm, s, 1)), cm)
    last = jnp.broadcast_to(cum[:, L - 1 :], (2 * CH, L))
    peak = jnp.broadcast_to(cm[:, L - 1 :], (2 * CH, L))
    weight = jnp.exp(a - peak)
    mm = last + peak
    rows[0], rows[1], rows[2], rows[3] = a, weight, last, mm
    colt[...] = jnp.transpose(jnp.concatenate([cm, cum, jnp.zeros((96, L), F32)], axis=0))

    mark('gates')
    ld_k.wait()
    ld_v.wait()

    def chunk_state(j, _):
        at = pl.ds(pl.multiple_of(j * L, L), L)
        for h in range(2):
            kt = jnp.transpose(k[at, h * DK : (h + 1) * DK].astype(F32))
            kw = kt * rows[1, pl.ds(2 * j + h, 1), :]
            dc[j, h, :, :DV] = jnp.dot(
                kw.astype(BF), v[at, h * DV : (h + 1) * DV], preferred_element_type=F32
            )
            dc[j, h, :, DV:] = jnp.broadcast_to(jnp.sum(kw, axis=1, keepdims=True), (DK, L))
        return 0

    lax.fori_loop(0, CH, chunk_state, 0)

    mark('chunkstates')
    for h in range(2):
        tot = jnp.zeros((1, L), F32)
        logs = [None] * CH
        for j in reversed(range(CH)):
            row = 2 * j + h
            logs[j] = mm[row : row + 1] + tot
            tot = tot + last[row : row + 1]
        m = logs[0]
        for j in range(1, CH):
            m = jnp.maximum(m, logs[j])
        total = jnp.zeros((DK, DV + L), F32)
        for j in range(CH):
            total = total + jnp.exp(logs[j] - m)[:, 0:1] * dc[j, h]
        st1[h] = total[:, :DV].astype(BF)
        n_row = jnp.transpose(total[:, DV:])[0:1]
        ax1[h] = jnp.concatenate([n_row, tot, m, jnp.zeros((5, L), F32)], axis=0)

    mark('devstate')
    s1 = [send(st1, st1r, {"sp_2": other}), send(ax1, ax1r, {"sp_2": other})]

    ld_q.wait()

    def within(j, _):
        at = pl.ds(pl.multiple_of(j * L, L), L)
        turned = pltpu.roll(colt[...], lax.rem(L - 2 * j, L), 1)
        for h in range(2):
            raw = lax.dot_general(
                q[at, h * DK : (h + 1) * DK], k[at, h * DK : (h + 1) * DK],
                (((1,), (1,)), ((), ())), preferred_element_type=F32,
            ) * SCALE
            logit = rows[0, pl.ds(2 * j + h, 1), :] - turned[:, h : h + 1]
            sc = raw * jnp.exp(jnp.where(causal, logit, NEG))
            nl[j, h, :, :DV] = jnp.dot(
                sc.astype(BF), v[at, h * DV : (h + 1) * DV], preferred_element_type=F32
            )
            nl[j, h, :, DV:] = jnp.broadcast_to(jnp.sum(sc, axis=1, keepdims=True), (L, L))
        return 0

    lax.fori_loop(0, 2, within, 0)

    mark('within2')
    cf = jnp.full((1, L), c, jnp.int32).astype(F32)
    arrived(s1)

    def aux(ref, *at):
        block = ref[at] if at else ref[...]
        return block[0:1], block[1:2], block[2:3]

    def pack(n, tot, m):
        return jnp.concatenate([n, tot, m, jnp.zeros((5, L), F32)], axis=0)

    mark('s1_arr')
    n_o, t_o, m_o = aux(ax1, c)
    n_r, t_r, m_r = aux(ax1r, c)
    log_o = m_o + (1.0 - cf) * t_r
    log_r = m_r + cf * t_o
    m = jnp.maximum(log_o, log_r)
    w_o, w_r = jnp.exp(log_o - m), jnp.exp(log_r - m)
    st2[0] = (w_o[:, 0:1] * st1[c].astype(F32) + w_r[:, 0:1] * st1r[c].astype(F32)).astype(BF)
    ax2[0] = pack(w_o * n_o + w_r * n_r, t_o + t_r, m)
    s2 = []
    for n in (1, 2, 3):
        s2.append(send(st2.at[0], st2.at[n], {"sp_1": up(y, n)}))
        s2.append(send(ax2.at[0], ax2.at[n], {"sp_1": up(y, n)}))

    mark('s2_sent')
    lax.fori_loop(2, 5, within, 0)

    def scan_of(st, ax, me, whole):
        parts = [aux(ax, n) for n in range(4)]
        mine = jnp.full((1, L), me, jnp.int32)
        below = [None] + [mine >= n for n in (1, 2, 3)]
        zero = jnp.zeros((1, L), F32)
        after = zero
        for n in (1, 2, 3):
            after = after + jnp.where(below[n], 0.0, parts[n][1])
        run, run_up = zero, zero
        log_in, log_all = [None] * 4, [parts[0][2] + after] + [None] * 3
        for n in (1, 2, 3):
            log_in[n] = jnp.where(below[n], parts[n][2] + run, NEG)
            log_all[n] = jnp.where(
                below[n], parts[n][2] + run + parts[0][1] + after, parts[n][2] + run_up
            )
            run = run + jnp.where(below[n], parts[n][1], 0.0)
            run_up = run_up + jnp.where(below[n], 0.0, parts[n][1])
        m_in = jnp.maximum(jnp.maximum(log_in[1], log_in[2]), log_in[3])
        w_in = [None] + [jnp.where(below[n], jnp.exp(log_in[n] - m_in), 0.0) for n in (1, 2, 3)]
        blocks = [st[n].astype(F32) for n in range(4)]
        c_in = sum(w_in[n][:, 0:1] * blocks[n] for n in (1, 2, 3))
        n_in = sum(w_in[n] * parts[n][0] for n in (1, 2, 3))
        inside = (c_in, n_in, run, m_in)
        if not whole:
            return inside, None
        m_all = jnp.maximum(
            jnp.maximum(log_all[0], log_all[1]), jnp.maximum(log_all[2], log_all[3])
        )
        w_all = [jnp.exp(t - m_all) for t in log_all]
        c_all = sum(w_all[n][:, 0:1] * blocks[n] for n in range(4))
        n_all = sum(w_all[n] * parts[n][0] for n in range(4))
        return inside, (c_all, n_all, run + run_up + parts[0][1], m_all)

    mark('within5')
    arrived(s2)
    mark('s2_arr')
    y_in, y_all = scan_of(st2, ax2, y, True)
    st3[0] = y_all[0].astype(BF)
    ax3[0] = pack(*y_all[1:])
    s3 = []
    for n in (1, 2, 3):
        s3.append(send(st3.at[0], st3.at[n], {"sp_0": up(z, n)}))
        s3.append(send(ax3.at[0], ax3.at[n], {"sp_0": up(z, n)}))
    cpri[0, :, :DV] = y_in[0]

    mark('s3_sent')
    arrived(p1)
    p2 = []
    for ref in (wgv, wd):
        for src, dev in (
            (halves(ref, z, y3, 0, 16), {"sp_1": y1}),
            (halves(ref, z, y1, 16, 16), {"sp_1": y3}),
            (halves(ref, z3, y, 32, 16), {"sp_0": z1}),
            (halves(ref, z1, y, 48, 16), {"sp_0": z3}),
        ):
            p2.append(send(src, src, dev))
    mark('p2_sent')
    lax.fori_loop(5, CH, within, 0)

    mark('within8')
    arrived(s3)
    mark('s3_arr')
    z_in, _ = scan_of(st3, ax3, z, False)
    m = jnp.maximum(y_in[2] + z_in[3], y_in[3])
    w_z, w_y = jnp.exp(y_in[2] + z_in[3] - m), jnp.exp(y_in[3] - m)
    st4[...] = (w_z[:, 0:1] * z_in[0] + w_y[:, 0:1] * cpri[0, :, :DV]).astype(BF)
    ax4[...] = pack(w_z * z_in[1] + w_y * y_in[1], z_in[2] + y_in[2], m)
    s4 = [send(st4, st4r, {"sp_2": other}), send(ax4, ax4r, {"sp_2": other})]

    def across(ref):
        row_a = ref.at[z, :, c, pl.ds(0, 32)]
        row_b = ref.at[:, y, c, pl.ds(32, 32)]
        return [
            send(row_a, row_a, {"sp_0": z1}),
            send(row_a, row_a, {"sp_0": z3}),
            send(row_b, row_b, {"sp_1": y1}),
            send(row_b, row_b, {"sp_1": y3}),
        ], [send(row_a, row_a, {"sp_2": other}), send(row_b, row_b, {"sp_2": other})]

    def across_two(ref):
        far = [
            send(src, src, dev)
            for src, dev in (
                (ref.at[z3, :, c, pl.ds(0, 16)], {"sp_0": z1}),
                (ref.at[z1, :, c, pl.ds(16, 16)], {"sp_0": z3}),
                (ref.at[:, y3, c, pl.ds(32, 16)], {"sp_1": y1}),
                (ref.at[:, y1, c, pl.ds(48, 16)], {"sp_1": y3}),
            )
        ]
        swap = [
            send(src, src, {"sp_2": other})
            for src in (
                ref.at[z1, :, c, pl.ds(0, 32)],
                ref.at[z3, :, c, pl.ds(0, 32)],
                ref.at[:, y1, c, pl.ds(32, 32)],
                ref.at[:, y3, c, pl.ds(32, 32)],
            )
        ]
        return far, swap

    def last_swap(ref):
        z2, y2 = up(z, 2), up(y, 2)
        return [
            send(src, src, {"sp_2": other})
            for src in (ref.at[z2, :, c, pl.ds(0, 32)], ref.at[:, y2, c, pl.ds(32, 32)])
        ]

    mark('s4_sent')
    arrived(p2)
    mark('p2_arr')
    g_far1, g_pair = across(wgv)
    mark('p3_sent')
    arrived(s4)
    mark('s4_arr')
    last_in = jnp.full((1, L), c, jnp.int32) == 1
    for h, st, ax in ((c, st4, ax4), (other, st4r, ax4r)):
        n_b, t_b, m_b = aux(ax)
        n_p, t_p, m_p = aux(ax1r, h)
        m_p = jnp.where(last_in, m_p, NEG)
        m_b = m_b + cf * t_p
        m = jnp.maximum(m_b, m_p)
        w_b, w_p = jnp.exp(m_b - m), jnp.where(last_in, jnp.exp(m_p - m), 0.0)
        cpri[h, :, :DV] = w_b[:, 0:1] * st[...].astype(F32) + w_p[:, 0:1] * st1r[h].astype(F32)
        n_row = w_b * n_b + w_p * n_p
        cpri[h, :, DV:] = jnp.transpose(jnp.broadcast_to(n_row, (L, L)))
        mpri[h] = m

    def carry(j, _):
        for h in range(2):
            state, m_old = cpri[h], mpri[h]
            cs[j, h] = state.astype(BF)
            row = pl.ds(2 * j + h, 1)
            rs_rows[row, :] = m_old
            decayed, fresh = rows[2, row, :] + m_old, rows[3, row, :]
            m_new = jnp.maximum(decayed, fresh)
            cpri[h] = (
                jnp.exp(decayed - m_new)[:, 0:1] * state
                + jnp.exp(fresh - m_new)[:, 0:1] * dc[j, h]
            )
            mpri[h] = m_new
        return 0

    mark('prior')
    lax.fori_loop(0, CH, carry, 0)

    mark('carried')
    ld_og.wait()

    def finish(j, _):
        at = pl.ds(pl.multiple_of(j * L, L), L)
        turned = pltpu.roll(colt[...], lax.rem(L - 2 * j, L), 1)
        for h in range(2):
            r = rs_rows[pl.ds(2 * j + h, 1), :][:, 0:1]
            cmc, cuc = turned[:, h : h + 1], turned[:, 16 + h : 17 + h]
            g = jnp.maximum(cmc, r)
            e1, e2 = jnp.exp(cmc - g), jnp.exp(r - g) * SCALE
            qc = jnp.dot(q[at, h * DK : (h + 1) * DK], cs[j, h], preferred_element_type=F32)
            both = e1 * nl[j, h] + e2 * qc
            inv = 1.0 / jnp.maximum(jnp.abs(both[:, DV:]), jnp.exp(-cuc - g))
            mo = both[:, :DV] * jnp.concatenate([inv, inv], axis=1)
            norm = lax.rsqrt(jnp.mean(mo * mo, axis=1, keepdims=True) + EPS)
            gate = jax.nn.sigmoid(og[at, h * DV : (h + 1) * DV].astype(F32))
            gated[at, h * DV : (h + 1) * DV] = (mo * norm * gain[h : h + 1, :] * gate).astype(BF)
        return 0

    a2a = []
    for n in (2, 1, 3, 0):
        b = up(tp, n)
        lax.fori_loop(2 * b, 2 * b + 2, finish, 0)
        block = pl.ds(pl.multiple_of(b * 256, 256), 256)
        half0 = pl.ds(pl.multiple_of(b * 256, 128), 128)
        half1 = pl.ds(pl.multiple_of(b * 256 + 128, 128), 128)
        if n == 2:
            first_leg = [
                send(gated.at[half0], al.at[0], {"tp": x1}),
                send(gated.at[half1], al.at[1], {"tp": x3}),
            ]
        elif n:
            a2a.append(send(gated.at[block], orr.at[tp], {"tp": b}))
        else:
            orr[tp] = gated[block, :]
        if n == 3:
            arrived(first_leg)
            relayed = [
                send(al.at[0], orr.at[x3, pl.ds(0, 128)], {"tp": x1}),
                send(al.at[1], orr.at[x1, pl.ds(128, 128)], {"tp": x3}),
            ]
    mark('before_w1')
    arrived(w1)
    mark('w1_arr')
    w2 = []
    for src, lo, dev in ((x3, 0, x1), (x1, 128, x3)):
        part = wo.at[src, pl.ds(c * 256 + lo, 128)]
        w2.append(send(part, part, {"tp": dev}))
    wpair = []
    for src in (x1, x3):
        part = wo.at[src, pl.ds(c * 256, 256)]
        wpair.append(send(part, part, {"sp_2": other}))

    mark('cell_done')
    arrived(g_far1)
    mark('gfar1_arr')
    g_far2, more = across_two(wgv)
    g_pair += more
    d_far1, d_pair = across(wd)

    mark('p3_sent')
    arrived(w2)
    part = wo.at[x2, pl.ds(c * 256, 256)]
    wpair.append(send(part, part, {"sp_2": other}))
    mark('w2_arr')
    arrived(relayed)
    arrived(a2a)
    mark('a2a_arr')
    arrived(wpair)
    mark('wpair_arr')
    ld_res.wait()

    def project(n, ss):
        cols = pl.ds(pl.multiple_of(n * 256, 256), 256)
        acc = rsd[:, cols].astype(F32)
        for t in range(4):
            acc = acc + jnp.dot(orr[t], wo[t, :, cols], preferred_element_type=F32)
        low = acc.astype(BF)
        stream[:, cols] = low
        wide = low.astype(F32)
        sq = wide * wide
        return ss + sq[:, :L] + sq[:, L:]

    ss = lax.fori_loop(0, 8, project, jnp.zeros((256, L), F32))
    mark('projected')
    norm = lax.rsqrt(jnp.sum(ss, axis=1, keepdims=True) * (1.0 / D) + EPS)

    def normed(n, _):
        cols = pl.ds(pl.multiple_of(n * 256, 256), 256)
        rows_n = (stream[:, cols].astype(F32) * norm * fgain[:, cols]).astype(BF)
        gr[tp, pl.ds(16, 256), cols] = rows_n
        hs[:, cols] = rows_n[254:256].astype(F32)
        return 0

    lax.fori_loop(0, 8, normed, 0)

    mark('normed')
    hr[tp] = hs[...]
    halo = [send(hs, hr.at[tp], {"tp": up(tp, n)}) for n in (1, 2, 3)]
    s_next = [take("s") for _ in range(4)]
    r_next = take("r")

    def next_copy(t):
        return pltpu.make_async_remote_copy(
            src_ref=hs, dst_ref=hp, send_sem=ssem.at[s_next[t]], recv_sem=rsem.at[r_next],
            device_id={**at_place(place + 1), "tp": t}, device_id_type=MESH,
        )

    @pl.when(tp == 3)
    def _():
        for t in range(4):
            next_copy(t).start()

    own_rows = gr.at[tp, pl.ds(16, 256)]
    g1 = [send(own_rows, own_rows, {"tp": x1}), send(own_rows, own_rows, {"tp": x3})]

    mark('g1_sent')
    arrived(g_far2)
    mark('gfar2_arr')
    g_pair += last_swap(wgv)
    arrived(d_far1)
    mark('dfar1_arr')
    d_far2, more = across_two(wd)
    d_pair += more
    arrived(halo)
    next_copy(0).wait_recv()
    mark('halo_arr')
    arrived(g_pair)
    mark('gpair_arr')

    first = jnp.full((2, D), place, jnp.int32) == 0

    def copy_of(src, dst, dev):
        cp = pltpu.make_async_remote_copy(
            src_ref=src, dst_ref=dst, send_sem=ssem.at[take("s")], recv_sem=rsem.at[take("r")],
            device_id=dev, device_id_type=MESH,
        )
        open_sends.append(cp)
        return cp

    lo, hi = pl.ds(0, 128), pl.ds(128, 128)
    part_a, part_b = gr.at[x3, pl.ds(16, 128)], gr.at[x1, pl.ds(144, 128)]
    g2 = [copy_of(part_a, part_a, {"tp": x1}), copy_of(part_b, part_b, {"tp": x3})]
    far = [
        copy_of(ps.at[2, lo], rl.at[0], {"tp": x1}),
        copy_of(ps.at[2, hi], rl.at[1], {"tp": x3}),
    ]
    direct = [
        copy_of(ps.at[1, hi], rr.at[0, hi], {"tp": x1}),
        copy_of(ps.at[3, lo], rr.at[1, lo], {"tp": x3}),
    ]
    summed = [
        copy_of(ps.at[1, lo], rr.at[0, lo], {"tp": x1}),
        copy_of(ps.at[3, hi], rr.at[1, hi], {"tp": x3}),
    ]
    d_near = list(d_pair)
    z2, y2 = up(z, 2), up(y, 2)
    d_last = [
        copy_of(src, src, {"sp_2": other})
        for src in (wd.at[z2, :, c, pl.ds(0, 32)], wd.at[:, y2, c, pl.ds(32, 32)])
    ]

    def feed(i, _):
        slot = i ^ (i >> 1)
        b = up(tp, slot)

        @pl.when(i == 1)
        def _():
            mark('feed0')
            arrived(g1)
            mark('g1_arr')
            for cp in g2:
                cp.start()

        @pl.when(i == 3)
        def _():
            mark('feed2')
            arrived(g2)
            mark('g2_arr')

        from_here = hr[up(b, 3)]
        from_before = jnp.where(first, 0.0, hp[...])
        is_zero = jnp.full((2, D), b, jnp.int32) == 0
        two = jnp.where(is_zero, from_before, from_here)
        gr[b, pl.ds(0, 16), :] = jnp.concatenate([jnp.zeros((14, D), F32), two], axis=0).astype(BF)

        def product(n):
            w = wgv[:, :, :, :, n * 256 : n * 256 + 256].reshape(D, 256)
            gvs[n % 2] = jnp.dot(gr[b], w, preferred_element_type=F32)

        def gate_of(n):
            cols = slice(n * L, n * L + L)

            def conv(lanes, tap):
                return (
                    tap[0:1, cols] * gvs[n % 2, 14:270, lanes]
                    + tap[1:2, cols] * gvs[n % 2, 15:271, lanes]
                    + tap[2:3, cols] * gvs[n % 2, 16:272, lanes]
                )

            cg, cv = conv(slice(0, L), gtap), conv(slice(L, 256), vtap)
            hid[:, cols] = (cg / (1.0 + jnp.exp(-cg)) * cv).astype(BF)

        product(0)
        for n in range(1, NT):
            product(n)
            gate_of(n - 1)
        gate_of(NT - 1)
        mark('up_done')

        @pl.when(i == 0)
        def _():
            arrived(d_far2)
            mark('dfar2_arr')
            for cp in d_last:
                cp.start()
            arrived(d_near)
            arrived(d_last)
            mark('dpair_arr')

        for n in range(8):
            w = wd[n // 2, 2 * (n % 2) : 2 * (n % 2) + 2].reshape(256, FFD)
            p = lax.dot_general(
                hid[...], w, (((1,), (1,)), ((), ())), preferred_element_type=F32
            )
            ps[slot, :, n * 256 : n * 256 + 256] = p.astype(BF)
        mark('down_done')

        @pl.when(i == 1)
        def _():
            direct[0].start()

        @pl.when(i == 2)
        def _():
            direct[1].start()

        @pl.when(i == 3)
        def _():
            for cp in far:
                cp.start()

        return 0

    lax.fori_loop(0, 4, feed, 0)
    mark('fed')
    for n, (cp, half) in enumerate(zip(far, (lo, hi))):
        cp.wait_recv()
        mark('far_arr')

        def relay(m, _):
            cols = pl.ds(pl.multiple_of(m * 256, 256), 256)
            ps[2 * n + 1, half, cols] = (
                ps[2 * n + 1, half, cols].astype(F32) + rl[n, :, cols].astype(F32)
            ).astype(BF)
            return 0

        lax.fori_loop(0, 8, relay, 0)
        summed[n].start()
    arrived(direct)
    mark('direct_arr')
    arrived(summed)
    mark('back_arr')

    def add(n, _):
        cols = pl.ds(pl.multiple_of(n * 256, 256), 256)
        s = ps[0, :, cols].astype(F32) + rr[0, :, cols].astype(F32) + rr[1, :, cols].astype(F32)
        out[:, cols] = (stream[:, cols].astype(F32) + s).astype(BF)
        return 0

    lax.fori_loop(0, 8, add, 0)

    mark('added')
    for cp in open_sends:
        cp.wait_send()

    mark('sends_done')
    @pl.when(tp == 3)
    def _():
        for t in range(4):
            next_copy(t).wait_send()


def local(
    residual_entry_input, query_matrix_rows, key_matrix_rows, value_matrix_rows,
    output_gate_logits, input_gate_logits, forget_gate_logits, forget_decay_offset,
    head_norm_gain, cell_output_weight, feedforward_norm_gain, gate_up_weight,
    value_up_weight, gate_filter_taps, value_filter_taps, down_projection_weight,
):
    def chunks(gate):
        return gate.T.reshape(2, CH, L).transpose(1, 0, 2).reshape(2 * CH, L)

    hbm = pl.BlockSpec(memory_space=pl.ANY)
    vmem = pl.BlockSpec(memory_space=pltpu.VMEM)
    scratch = [
        pltpu.VMEM((1024, 256), BF), pltpu.VMEM((1024, 256), BF), pltpu.VMEM((1024, 512), BF),
        pltpu.VMEM((1024, 512), BF), pltpu.VMEM((256, D), BF),
        pltpu.VMEM((4, 4, 2, 64, 2 * FFD), BF), pltpu.VMEM((4, 4, 2, 64, FFD), BF),
        pltpu.VMEM((4, 512, D), BF),
        pltpu.VMEM((CH, 2, DK, DV + L), F32), pltpu.VMEM((CH, 2, L, DV + L), F32),
        pltpu.VMEM((L, L), F32), pltpu.VMEM((4, 2 * CH, L), F32),
        pltpu.VMEM((CH, 2, DK, DV + L), BF), pltpu.VMEM((2, DK, DV + L), F32),
        pltpu.VMEM((2, 1, L), F32), pltpu.VMEM((2 * CH, L), F32),
        pltpu.VMEM((2, DK, DV), BF), pltpu.VMEM((2, 8, L), F32),
        pltpu.VMEM((2, DK, DV), BF), pltpu.VMEM((2, 8, L), F32),
        pltpu.VMEM((4, DK, DV), BF), pltpu.VMEM((4, 8, L), F32),
        pltpu.VMEM((4, DK, DV), BF), pltpu.VMEM((4, 8, L), F32),
        pltpu.VMEM((DK, DV), BF), pltpu.VMEM((8, L), F32),
        pltpu.VMEM((DK, DV), BF), pltpu.VMEM((8, L), F32),
        pltpu.VMEM((1024, 512), BF), pltpu.VMEM((2, 128, 512), BF), pltpu.VMEM((4, 256, 512), BF),
        pltpu.VMEM((256, D), BF),
        pltpu.VMEM((4, 272, D), BF), pltpu.VMEM((2, D), F32), pltpu.VMEM((4, 2, D), F32),
        pltpu.VMEM((2, D), F32), pltpu.VMEM((2, 272, 256), F32), pltpu.VMEM((256, FFD), BF),
        pltpu.VMEM((4, 256, D), BF), pltpu.VMEM((2, 128, D), BF), pltpu.VMEM((2, 256, D), BF),
        pltpu.SemaphoreType.DMA((32,)), pltpu.SemaphoreType.DMA((100,)),
        pltpu.SemaphoreType.DMA((100,)),
    ]
    return pl.pallas_call(
        kernel,
        out_shape=jax.ShapeDtypeStruct((256, D), BF),
        in_specs=[hbm, hbm, hbm, hbm, hbm, vmem, vmem, vmem, vmem, hbm, vmem, hbm, hbm, hbm, vmem, vmem],
        out_specs=vmem,
        scratch_shapes=scratch,
        compiler_params=pltpu.CompilerParams(
            collective_id=0, has_side_effects=True, vmem_limit_bytes=67_043_328
        ),
    )(
        residual_entry_input, query_matrix_rows, key_matrix_rows, value_matrix_rows,
        output_gate_logits, chunks(input_gate_logits), chunks(forget_gate_logits),
        chunks(forget_decay_offset), head_norm_gain, cell_output_weight,
        feedforward_norm_gain.reshape(1, D), gate_up_weight, value_up_weight,
        down_projection_weight.T, gate_filter_taps, value_filter_taps,
    )


def solution(mesh):
    split = Mesh(mesh.devices.reshape(4, 4, 2, mesh.shape["tp"]), SP_TP)
    placed = (
        P(SP_TP, None), P(SP, "tp"), P(SP, "tp"), P(SP, "tp"), P(SP, "tp"), P(SP, "tp"),
        P(SP, "tp"), P(SP, "tp"), P("tp", None), P("tp", None), P(), P(SP, "tp"), P(SP, "tp"),
        P(None, "tp"), P(None, "tp"), P("tp", SP),
    )
    return jax.shard_map(
        local, mesh=split, in_specs=placed, out_specs=P(SP_TP, None), check_vma=False
    )
```

```python
import jax
import jax.numpy as jnp
from jax import lax
from jax.experimental import pallas as pl
from jax.experimental.pallas import tpu as pltpu
from jax.sharding import Mesh
from jax.sharding import PartitionSpec as P

SP = ("sp_0", "sp_1", "sp_2")
SP_TP = ("sp_0", "sp_1", "sp_2", "tp")
MESH = pl.DeviceIdType.MESH

EPS = 1e-06
NEG = -1e30
L = 128
CH = 8
DK = 128
DV = 256
D = 2048
FFD = 1408
NT = FFD // 128
SCALE = DK**-0.5
F32 = jnp.float32
BF = jnp.bfloat16


def log1p_of(e):
    series = e * (1.0 - e * (0.5 - e * (1.0 / 3.0 - e * (0.25 - e * 0.2))))
    return jnp.where(e < 0.03, series, jnp.log(1.0 + e))


def kernel(
    res, q_in, k_in, v_in, og_in, ig, fg, off, gain, wo_in, fgain, gup, vup, dwn, gtap, vtap,
    out,
    q, k, v, og, rsd, wgv, wd, wo, dc, nl, colt, rows, cs, cpri, mpri, rs_rows,
    st1, ax1, st1r, ax1r, st2, ax2, st3, ax3, st4, ax4, st4r, ax4r,
    gated, al, orr, stream, gr, hs, hr, hp, gvs, hid, ps, rl, rr,
    lsem, ssem, rsem,
):
    z, y, c, tp = (lax.axis_index(a) for a in SP_TP)

    def up(i, n):
        return lax.rem(i + n, 4)

    y1, y3 = up(y, 1), up(y, 3)
    z1, z3 = up(z, 1), up(z, 3)
    x1, x2, x3 = up(tp, 1), up(tp, 2), up(tp, 3)
    other = 1 - c
    place = z * 8 + y * 2 + c

    def at_place(n):
        n = lax.rem(n + 32, 32)
        return {"sp_0": n // 8, "sp_1": lax.rem(n // 2, 4), "sp_2": lax.rem(n, 2)}

    count = {"l": 0, "s": 0, "r": 0}
    open_sends = []

    def take(kind):
        count[kind] += 1
        return count[kind] - 1

    def load(src, dst):
        cp = pltpu.make_async_copy(src, dst, lsem.at[take("l")])
        cp.start()
        return cp

    def send(src, dst, dev):
        cp = pltpu.make_async_remote_copy(
            src_ref=src, dst_ref=dst, send_sem=ssem.at[take("s")], recv_sem=rsem.at[take("r")],
            device_id=dev, device_id_type=MESH,
        )
        cp.start()
        open_sends.append(cp)
        return cp

    def arrived(copies):
        for cp in copies:
            cp.wait_recv()

    def mark(name):
        pass

    mark('entry')
    ld_k = load(k_in, k)
    ld_v = load(v_in, v)
    ld_w = [load(dwn, wd.at[z, y, c])]
    for n in range(NT):
        ld_w.append(load(gup.at[:, pl.ds(n * 128, 128)], wgv.at[z, y, c, :, pl.ds(n * 256, 128)]))
        ld_w.append(load(vup.at[:, pl.ds(n * 128, 128)], wgv.at[z, y, c, :, pl.ds(n * 256 + 128, 128)]))
    ld_wo = load(wo_in, wo.at[tp])
    ld_q = load(q_in, q)
    ld_og = load(og_in, og)
    ld_res = load(res, rsd)

    barrier = pltpu.get_barrier_semaphore()

    def hello(dev):
        pl.semaphore_signal(barrier, inc=1, device_id=dev, device_id_type=MESH)

    hello({"sp_2": other})
    for n in (1, 2, 3):
        hello({"sp_1": up(y, n)})
        hello({"sp_0": up(z, n)})
        hello({"tp": up(tp, n)})
    hello({**at_place(place - 1), "tp": 3})

    @pl.when(tp == 3)
    def _():
        for t in range(4):
            hello({**at_place(place + 1), "tp": t})
        pl.semaphore_wait(barrier, 15)

    @pl.when(tp != 3)
    def _():
        pl.semaphore_wait(barrier, 11)

    def halves(ref, zz, yy, lo, n):
        return ref.at[zz, yy, c, pl.ds(lo, n)]

    mark('barrier_done')
    for cp in ld_w:
        cp.wait()
    p1 = []
    for ref in (wgv, wd):
        mine_a, mine_b = halves(ref, z, y, 0, 32), halves(ref, z, y, 32, 32)
        p1 += [
            send(mine_a, mine_a, {"sp_1": y1}),
            send(mine_a, mine_a, {"sp_1": y3}),
            send(mine_b, mine_b, {"sp_0": z1}),
            send(mine_b, mine_b, {"sp_0": z3}),
        ]
    mark('w_issued')
    ld_wo.wait()
    y2, z2 = up(y, 2), up(z, 2)

    def wo_pieces(t, far):
        return wo.at[t, c, 0, y2 if far else y], wo.at[t, c, 1, z2 if far else z]

    xo1a, xo1b = (
        [send(piece, piece, {"tp": dev}) for piece in wo_pieces(tp, n) for dev in (x1, x3)]
        for n in (False, True)
    )

    def wo_swap(piece):
        return send(piece, piece, {"sp_2": other})

    def wo_onward(far):
        py, pz = wo_pieces(x3, far)[0], wo_pieces(x1, far)[1]
        return [send(py, py, {"tp": x1}), send(pz, pz, {"tp": x3})]

    def wo_spread(t):
        py, pz = wo_pieces(t, False)
        near = [
            send(py, py, {"sp_1": y1}), send(py, py, {"sp_1": y3}),
            send(pz, pz, {"sp_0": z1}), send(pz, pz, {"sp_0": z3}),
        ]
        return near, [wo_swap(py), wo_swap(pz)]

    def wo_near_swaps(t):
        return [
            wo_swap(piece)
            for piece in (
                wo.at[t, c, 0, y1], wo.at[t, c, 0, y3], wo.at[t, c, 1, z1], wo.at[t, c, 1, z3]
            )
        ]

    def slab(ref, n):
        piece_a, piece_b = halves(ref, z, up(y, n), 0, 32), halves(ref, up(z, n), y, 32, 32)
        return [
            send(piece_a, piece_a, {"sp_0": z1}),
            send(piece_a, piece_a, {"sp_0": z3}),
            send(piece_b, piece_b, {"sp_1": y1}),
            send(piece_b, piece_b, {"sp_1": y3}),
        ]

    def row_swap(ref):
        row_a = ref.at[z, :, c, pl.ds(0, 32)]
        row_b = ref.at[:, y, c, pl.ds(32, 32)]
        return [send(row_a, row_a, {"sp_2": other}), send(row_b, row_b, {"sp_2": other})]

    def across(ref):
        row_a = ref.at[z, :, c, pl.ds(0, 32)]
        row_b = ref.at[:, y, c, pl.ds(32, 32)]
        return [
            send(row_a, row_a, {"sp_0": z1}),
            send(row_a, row_a, {"sp_0": z3}),
            send(row_b, row_b, {"sp_1": y1}),
            send(row_b, row_b, {"sp_1": y3}),
        ]

    def across_two(ref):
        far = [
            send(src, src, dev)
            for src, dev in (
                (ref.at[z3, :, c, pl.ds(0, 16)], {"sp_0": z1}),
                (ref.at[z1, :, c, pl.ds(16, 16)], {"sp_0": z3}),
                (ref.at[:, y3, c, pl.ds(32, 16)], {"sp_1": y1}),
                (ref.at[:, y1, c, pl.ds(48, 16)], {"sp_1": y3}),
            )
        ]
        swap = [
            send(src, src, {"sp_2": other})
            for src in (
                ref.at[z1, :, c, pl.ds(0, 32)],
                ref.at[z3, :, c, pl.ds(0, 32)],
                ref.at[:, y1, c, pl.ds(32, 32)],
                ref.at[:, y3, c, pl.ds(32, 32)],
            )
        ]
        return far, swap

    def last_swap(ref):
        return [
            send(src, src, {"sp_2": other})
            for src in (ref.at[z2, :, c, pl.ds(0, 32)], ref.at[:, y2, c, pl.ds(32, 32)])
        ]

    mark('wo_issued')
    il = 15.0 * jnp.tanh(ig[...] / 15.0)
    xf = 15.0 * jnp.tanh(fg[...] / 15.0)
    fl = jnp.minimum(xf, 0.0) - log1p_of(jnp.exp(-jnp.abs(xf))) + off[...]
    r_i = lax.broadcasted_iota(jnp.int32, (L, L), 0)
    c_i = lax.broadcasted_iota(jnp.int32, (L, L), 1)
    causal = r_i >= c_i
    upper = (r_i <= c_i).astype(F32)
    cum = jnp.dot(fl, upper, preferred_element_type=F32, precision=lax.Precision.HIGHEST)
    a = il - cum
    lane = lax.broadcasted_iota(jnp.int32, (2 * CH, L), 1)
    cm = a
    for s in (1, 2, 4, 8, 16, 32, 64):
        cm = jnp.where(lane >= s, jnp.maximum(cm, pltpu.roll(cm, s, 1)), cm)
    last = jnp.broadcast_to(cum[:, L - 1 :], (2 * CH, L))
    peak = jnp.broadcast_to(cm[:, L - 1 :], (2 * CH, L))
    weight = jnp.exp(a - peak)
    mm = last + peak
    rows[0], rows[1], rows[2], rows[3] = a, weight, last, mm
    colt[...] = jnp.transpose(jnp.concatenate([cm, cum, jnp.zeros((96, L), F32)], axis=0))

    mark('gates')
    ld_k.wait()
    ld_v.wait()

    def chunk_state(j, _):
        at = pl.ds(pl.multiple_of(j * L, L), L)
        for h in range(2):
            kt = jnp.transpose(k[at, h * DK : (h + 1) * DK].astype(F32))
            kw = kt * rows[1, pl.ds(2 * j + h, 1), :]
            dc[j, h, :, :DV] = jnp.dot(
                kw.astype(BF), v[at, h * DV : (h + 1) * DV], preferred_element_type=F32
            )
            dc[j, h, :, DV:] = jnp.broadcast_to(jnp.sum(kw, axis=1, keepdims=True), (DK, L))
        return 0

    lax.fori_loop(0, CH, chunk_state, 0)

    mark('chunkstates')
    for h in range(2):
        tot = jnp.zeros((1, L), F32)
        logs = [None] * CH
        for j in reversed(range(CH)):
            row = 2 * j + h
            logs[j] = mm[row : row + 1] + tot
            tot = tot + last[row : row + 1]
        m = logs[0]
        for j in range(1, CH):
            m = jnp.maximum(m, logs[j])
        total = jnp.zeros((DK, DV + L), F32)
        for j in range(CH):
            total = total + jnp.exp(logs[j] - m)[:, 0:1] * dc[j, h]
        st1[h] = total[:, :DV].astype(BF)
        n_row = jnp.transpose(total[:, DV:])[0:1]
        ax1[h] = jnp.concatenate([n_row, tot, m, jnp.zeros((5, L), F32)], axis=0)

    mark('devstate')
    s1 = [send(st1, st1r, {"sp_2": other}), send(ax1, ax1r, {"sp_2": other})]

    ld_q.wait()

    def within(j, _):
        at = pl.ds(pl.multiple_of(j * L, L), L)
        turned = pltpu.roll(colt[...], lax.rem(L - 2 * j, L), 1)
        for h in range(2):
            raw = lax.dot_general(
                q[at, h * DK : (h + 1) * DK], k[at, h * DK : (h + 1) * DK],
                (((1,), (1,)), ((), ())), preferred_element_type=F32,
            ) * SCALE
            logit = rows[0, pl.ds(2 * j + h, 1), :] - turned[:, h : h + 1]
            sc = raw * jnp.exp(jnp.where(causal, logit, NEG))
            nl[j, h, :, :DV] = jnp.dot(
                sc.astype(BF), v[at, h * DV : (h + 1) * DV], preferred_element_type=F32
            )
            nl[j, h, :, DV:] = jnp.broadcast_to(jnp.sum(sc, axis=1, keepdims=True), (L, L))
        return 0

    lax.fori_loop(0, 2, within, 0)

    mark('within2')
    cf = jnp.full((1, L), c, jnp.int32).astype(F32)
    arrived(s1)

    def aux(ref, *at):
        block = ref[at] if at else ref[...]
        return block[0:1], block[1:2], block[2:3]

    def pack(n, tot, m):
        return jnp.concatenate([n, tot, m, jnp.zeros((5, L), F32)], axis=0)

    mark('s1_arr')
    n_o, t_o, m_o = aux(ax1, c)
    n_r, t_r, m_r = aux(ax1r, c)
    log_o = m_o + (1.0 - cf) * t_r
    log_r = m_r + cf * t_o
    m = jnp.maximum(log_o, log_r)
    w_o, w_r = jnp.exp(log_o - m), jnp.exp(log_r - m)
    st2[0] = (w_o[:, 0:1] * st1[c].astype(F32) + w_r[:, 0:1] * st1r[c].astype(F32)).astype(BF)
    ax2[0] = pack(w_o * n_o + w_r * n_r, t_o + t_r, m)
    s2 = []
    for n in (1, 2, 3):
        s2.append(send(st2.at[0], st2.at[n], {"sp_1": up(y, n)}))
        s2.append(send(ax2.at[0], ax2.at[n], {"sp_1": up(y, n)}))

    mark('s2_sent')
    lax.fori_loop(2, 5, within, 0)

    def scan_of(st, ax, me, whole):
        parts = [aux(ax, n) for n in range(4)]
        mine = jnp.full((1, L), me, jnp.int32)
        below = [None] + [mine >= n for n in (1, 2, 3)]
        zero = jnp.zeros((1, L), F32)
        after = zero
        for n in (1, 2, 3):
            after = after + jnp.where(below[n], 0.0, parts[n][1])
        run, run_up = zero, zero
        log_in, log_all = [None] * 4, [parts[0][2] + after] + [None] * 3
        for n in (1, 2, 3):
            log_in[n] = jnp.where(below[n], parts[n][2] + run, NEG)
            log_all[n] = jnp.where(
                below[n], parts[n][2] + run + parts[0][1] + after, parts[n][2] + run_up
            )
            run = run + jnp.where(below[n], parts[n][1], 0.0)
            run_up = run_up + jnp.where(below[n], 0.0, parts[n][1])
        m_in = jnp.maximum(jnp.maximum(log_in[1], log_in[2]), log_in[3])
        w_in = [None] + [jnp.where(below[n], jnp.exp(log_in[n] - m_in), 0.0) for n in (1, 2, 3)]
        blocks = [st[n].astype(F32) for n in range(4)]
        c_in = sum(w_in[n][:, 0:1] * blocks[n] for n in (1, 2, 3))
        n_in = sum(w_in[n] * parts[n][0] for n in (1, 2, 3))
        inside = (c_in, n_in, run, m_in)
        if not whole:
            return inside, None
        m_all = jnp.maximum(
            jnp.maximum(log_all[0], log_all[1]), jnp.maximum(log_all[2], log_all[3])
        )
        w_all = [jnp.exp(t - m_all) for t in log_all]
        c_all = sum(w_all[n][:, 0:1] * blocks[n] for n in range(4))
        n_all = sum(w_all[n] * parts[n][0] for n in range(4))
        return inside, (c_all, n_all, run + run_up + parts[0][1], m_all)

    mark('within5')
    arrived(s2)
    mark('s2_arr')
    y_in, y_all = scan_of(st2, ax2, y, True)
    st3[0] = y_all[0].astype(BF)
    ax3[0] = pack(*y_all[1:])
    s3 = []
    for n in (1, 2, 3):
        s3.append(send(st3.at[0], st3.at[n], {"sp_0": up(z, n)}))
        s3.append(send(ax3.at[0], ax3.at[n], {"sp_0": up(z, n)}))
    cpri[0, :, :DV] = y_in[0]

    mark('s3_sent')
    arrived(xo1a)
    xo2a = wo_onward(False)
    near_a, wpair = wo_spread(x1)
    near_b, more = wo_spread(x3)
    wpair += more
    mark('xo1_arr')
    mark('p2_sent')
    lax.fori_loop(5, CH, within, 0)

    mark('within8')
    arrived(xo1b)
    xo2b = wo_onward(True)
    arrived(xo2a)
    mark('xo2_arr')
    near_c, more = wo_spread(x2)
    wpair += more
    arrived(p1)
    p2 = []
    for ref in (wgv, wd):
        for src, dev in (
            (halves(ref, z, y3, 0, 16), {"sp_1": y1}),
            (halves(ref, z, y1, 16, 16), {"sp_1": y3}),
            (halves(ref, z3, y, 32, 16), {"sp_0": z1}),
            (halves(ref, z1, y, 48, 16), {"sp_0": z3}),
        ):
            p2.append(send(src, src, dev))
    g_far1 = slab(wgv, 0) + slab(wgv, 1) + slab(wgv, 3)
    arrived(s3)
    mark('s3_arr')
    z_in, _ = scan_of(st3, ax3, z, False)
    m = jnp.maximum(y_in[2] + z_in[3], y_in[3])
    w_z, w_y = jnp.exp(y_in[2] + z_in[3] - m), jnp.exp(y_in[3] - m)
    st4[...] = (w_z[:, 0:1] * z_in[0] + w_y[:, 0:1] * cpri[0, :, :DV]).astype(BF)
    ax4[...] = pack(w_z * z_in[1] + w_y * y_in[1], z_in[2] + y_in[2], m)
    s4 = [send(st4, st4r, {"sp_2": other}), send(ax4, ax4r, {"sp_2": other})]

    mark('s4_sent')
    arrived(s4)
    mark('s4_arr')
    last_in = jnp.full((1, L), c, jnp.int32) == 1
    for h, st, ax in ((c, st4, ax4), (other, st4r, ax4r)):
        n_b, t_b, m_b = aux(ax)
        n_p, t_p, m_p = aux(ax1r, h)
        m_p = jnp.where(last_in, m_p, NEG)
        m_b = m_b + cf * t_p
        m = jnp.maximum(m_b, m_p)
        w_b, w_p = jnp.exp(m_b - m), jnp.where(last_in, jnp.exp(m_p - m), 0.0)
        cpri[h, :, :DV] = w_b[:, 0:1] * st[...].astype(F32) + w_p[:, 0:1] * st1r[h].astype(F32)
        n_row = w_b * n_b + w_p * n_p
        cpri[h, :, DV:] = jnp.transpose(jnp.broadcast_to(n_row, (L, L)))
        mpri[h] = m

    def carry(j, _):
        for h in range(2):
            state, m_old = cpri[h], mpri[h]
            cs[j, h] = state.astype(BF)
            row = pl.ds(2 * j + h, 1)
            rs_rows[row, :] = m_old
            decayed, fresh = rows[2, row, :] + m_old, rows[3, row, :]
            m_new = jnp.maximum(decayed, fresh)
            cpri[h] = (
                jnp.exp(decayed - m_new)[:, 0:1] * state
                + jnp.exp(fresh - m_new)[:, 0:1] * dc[j, h]
            )
            mpri[h] = m_new
        return 0

    mark('prior')
    lax.fori_loop(0, CH, carry, 0)

    mark('carried')
    ld_og.wait()

    def finish(j, _):
        at = pl.ds(pl.multiple_of(j * L, L), L)
        turned = pltpu.roll(colt[...], lax.rem(L - 2 * j, L), 1)
        for h in range(2):
            r = rs_rows[pl.ds(2 * j + h, 1), :][:, 0:1]
            cmc, cuc = turned[:, h : h + 1], turned[:, 16 + h : 17 + h]
            g = jnp.maximum(cmc, r)
            e1, e2 = jnp.exp(cmc - g), jnp.exp(r - g) * SCALE
            qc = jnp.dot(q[at, h * DK : (h + 1) * DK], cs[j, h], preferred_element_type=F32)
            both = e1 * nl[j, h] + e2 * qc
            inv = 1.0 / jnp.maximum(jnp.abs(both[:, DV:]), jnp.exp(-cuc - g))
            mo = both[:, :DV] * jnp.concatenate([inv, inv], axis=1)
            norm = lax.rsqrt(jnp.mean(mo * mo, axis=1, keepdims=True) + EPS)
            gate = jax.nn.sigmoid(og[at, h * DV : (h + 1) * DV].astype(F32))
            gated[at, h * DV : (h + 1) * DV] = (mo * norm * gain[h : h + 1, :] * gate).astype(BF)
        return 0

    a2a = []
    for n in (2, 1, 3, 0):
        b = up(tp, n)
        lax.fori_loop(2 * b, 2 * b + 2, finish, 0)
        block = pl.ds(pl.multiple_of(b * 256, 256), 256)
        half0 = pl.ds(pl.multiple_of(b * 256, 128), 128)
        half1 = pl.ds(pl.multiple_of(b * 256 + 128, 128), 128)
        if n == 2:
            first_leg = [
                send(gated.at[half0], al.at[0], {"tp": x1}),
                send(gated.at[half1], al.at[1], {"tp": x3}),
            ]
        elif n:
            a2a.append(send(gated.at[block], orr.at[tp], {"tp": b}))
        else:
            orr[tp] = gated[block, :]
        if n == 1:
            mark('cell_two')
            arrived(near_a)
            arrived(near_b)
            mark('near_ab')
            wpair += wo_near_swaps(x1) + wo_near_swaps(x3)
            for t in (x1, x3):
                wpair += [wo_swap(piece) for piece in wo_pieces(t, True)]
        if n == 3:
            mark('cell_three')
            arrived(first_leg)
            mark('leg_arr')
            relayed = [
                send(al.at[0], orr.at[x3, pl.ds(0, 128)], {"tp": x1}),
                send(al.at[1], orr.at[x1, pl.ds(128, 128)], {"tp": x3}),
            ]
    mark('cell_done')
    arrived(near_c)
    mark('near_c')
    arrived(xo2b)
    wpair += wo_near_swaps(x2) + [wo_swap(piece) for piece in wo_pieces(x2, True)]
    arrived(p2)
    mark('p2_arr')
    g_far1 += slab(wgv, 2)
    g_pair = row_swap(wgv)

    mark('w2_arr')
    arrived(relayed)
    arrived(a2a)
    mark('a2a_arr')
    arrived(wpair)
    mark('wpair_arr')
    ld_res.wait()

    def project(n, ss):
        cols = pl.ds(pl.multiple_of(n * 256, 256), 256)
        acc = rsd[:, cols].astype(F32)
        for t in range(4):
            acc = acc + jnp.dot(orr[t], wo[t, :, :, :, :, cols].reshape(512, 256), preferred_element_type=F32)
        low = acc.astype(BF)
        stream[:, cols] = low
        wide = low.astype(F32)
        sq = wide * wide
        return ss + sq[:, :L] + sq[:, L:]

    ss = lax.fori_loop(0, 8, project, jnp.zeros((256, L), F32))
    mark('projected')
    norm = lax.rsqrt(jnp.sum(ss, axis=1, keepdims=True) * (1.0 / D) + EPS)

    def normed(n, _):
        cols = pl.ds(pl.multiple_of(n * 256, 256), 256)
        rows_n = (stream[:, cols].astype(F32) * norm * fgain[:, cols]).astype(BF)
        gr[2 * tp, pl.ds(16, 128), cols] = rows_n[:128]
        gr[2 * tp + 1, pl.ds(16, 128), cols] = rows_n[128:]
        hs[0, :, cols] = rows_n[254:256].astype(F32)
        hs[1, :, cols] = rows_n[126:128].astype(F32)
        return 0

    lax.fori_loop(0, 8, normed, 0)

    mark('normed')
    hr[tp] = hs[...]
    s_next = [take("s") for _ in range(4)]
    r_next = take("r")

    def next_copy(t):
        return pltpu.make_async_remote_copy(
            src_ref=hs.at[0], dst_ref=hp, send_sem=ssem.at[s_next[t]], recv_sem=rsem.at[r_next],
            device_id={**at_place(place + 1), "tp": t}, device_id_type=MESH,
        )

    def half_rows(b, h):
        return gr.at[2 * b + h, pl.ds(16, 128)]

    own_lo, own_hi = half_rows(tp, 0), half_rows(tp, 1)
    g1a = [send(own_lo, own_lo, {"tp": x1}), send(own_hi, own_hi, {"tp": x3})]
    halo = [send(hs, hr.at[tp], {"tp": up(tp, n)}) for n in (1, 2, 3)]
    @pl.when(tp == 3)
    def _():
        for t in range(4):
            next_copy(t).start()

    g1b = [send(own_hi, own_hi, {"tp": x1}), send(own_lo, own_lo, {"tp": x3})]

    mark('g1_sent')
    arrived(g_far1)
    mark('gfar1_arr')
    g_far2, more = across_two(wgv)
    g_pair += more
    d_far1 = across(wd)
    d_pair = row_swap(wd)
    arrived(halo)
    next_copy(0).wait_recv()
    mark('halo_arr')
    arrived(g1a)
    mark('g1a_arr')
    part_a, part_b = half_rows(x3, 0), half_rows(x1, 1)
    g2 = [send(part_a, part_a, {"tp": x1}), send(part_b, part_b, {"tp": x3})]
    arrived(g_far2)
    mark('gfar2_arr')
    g_pair += last_swap(wgv)
    arrived(d_far1)
    mark('dfar1_arr')
    d_far2, more = across_two(wd)
    d_pair += more
    arrived(g_pair)
    mark('gpair_arr')

    first = jnp.full((2, D), place, jnp.int32) == 0

    def copy_of(src, dst, dev):
        cp = pltpu.make_async_remote_copy(
            src_ref=src, dst_ref=dst, send_sem=ssem.at[take("s")], recv_sem=rsem.at[take("r")],
            device_id=dev, device_id_type=MESH,
        )
        open_sends.append(cp)
        return cp

    lo, hi = pl.ds(0, 128), pl.ds(128, 128)
    direct = [
        copy_of(ps.at[0, lo], rr.at[0, hi], {"tp": x1}),
        copy_of(ps.at[0, hi], rr.at[1, lo], {"tp": x3}),
    ]
    far = [
        copy_of(ps.at[2, lo], rl.at[0], {"tp": x1}),
        copy_of(ps.at[2, hi], rl.at[1], {"tp": x3}),
    ]
    summed = [
        copy_of(ps.at[1, lo], rr.at[0, lo], {"tp": x1}),
        copy_of(ps.at[1, hi], rr.at[1, hi], {"tp": x3}),
    ]

    def rows_of(i):
        pair = i // 2
        h0 = (1 - pair) * (1 - i)
        b0 = up(tp, 1 - pair + pair * (6 - 2 * i))
        b1 = up(tp, 3 * (1 - pair) + pair * (6 - 2 * i))
        return (b0, h0), (b1, 1 - h0)

    def widen(i):
        spots = rows_of(i)
        for b, h in spots:
            from_last = jnp.where(
                jnp.full((2, D), b, jnp.int32) == 0,
                jnp.where(first, 0.0, hp[...]),
                hr[up(b, 3), 0],
            )
            two = jnp.where(jnp.full((2, D), h, jnp.int32) == 1, hr[b, 1], from_last)
            gr[2 * b + h, pl.ds(0, 16), :] = jnp.concatenate(
                [jnp.zeros((14, D), F32), two], axis=0
            ).astype(BF)
        e0, e1 = (2 * b + h for b, h in spots)

        def product(n):
            w = wgv[:, :, :, :, n * 256 : n * 256 + 256].reshape(D, 256)
            both = jnp.concatenate([gr[e0], gr[e1]], axis=0)
            gvs[n % 2] = jnp.dot(both, w, preferred_element_type=F32)

        def gate_of(n):
            cols = slice(n * L, n * L + L)
            for p in range(2):
                at = 144 * p + 14

                def conv(lanes, tap):
                    return (
                        tap[0:1, cols] * gvs[n % 2, at : at + 128, lanes]
                        + tap[1:2, cols] * gvs[n % 2, at + 1 : at + 129, lanes]
                        + tap[2:3, cols] * gvs[n % 2, at + 2 : at + 130, lanes]
                    )

                cg, cv = conv(slice(0, L), gtap), conv(slice(L, 256), vtap)
                hid[lax.rem(i, 2), 128 * p : 128 * p + 128, cols] = (
                    cg / (1.0 + jnp.exp(-cg)) * cv
                ).astype(BF)

        product(0)
        for n in range(1, NT):
            product(n)
            gate_of(n - 1)
        gate_of(NT - 1)

    def narrow(i):
        for n in range(8):
            w = wd[n // 2, 2 * (n % 2) : 2 * (n % 2) + 2].reshape(256, FFD)
            p = lax.dot_general(
                hid[lax.rem(i, 2)], w, (((1,), (1,)), ((), ())), preferred_element_type=F32
            )
            ps[i, :, n * 256 : n * 256 + 256] = p.astype(BF)

    widen(0)
    mark('up0')
    arrived(g1b)
    mark('g1b_arr')
    widen(1)
    mark('up1')
    arrived(d_far2)
    mark('dfar2_arr')
    d_pair += last_swap(wd)
    arrived(d_pair)
    mark('dpair_arr')

    def near_down(i, _):
        narrow(i)

        @pl.when(i == 0)
        def _():
            mark('down0')
            for cp in direct:
                cp.start()

        return 0

    lax.fori_loop(0, 2, near_down, 0)
    mark('down1')
    arrived(g2)
    mark('g2_arr')

    def rest(i, _):
        widen(i)
        narrow(i)

        @pl.when(i == 2)
        def _():
            mark('down2')
            for cp in far:
                cp.start()

        return 0

    lax.fori_loop(2, 4, rest, 0)
    mark('fed')
    for n, (cp, half) in enumerate(zip(far, (lo, hi))):
        cp.wait_recv()
        mark('far_arr')

        def relay(m, _):
            cols = pl.ds(pl.multiple_of(m * 256, 256), 256)
            ps[1, half, cols] = (
                ps[1, half, cols].astype(F32) + rl[n, :, cols].astype(F32)
            ).astype(BF)
            return 0

        lax.fori_loop(0, 8, relay, 0)
        summed[n].start()
    arrived(direct)
    mark('direct_arr')
    arrived(summed)
    mark('back_arr')

    def add(n, _):
        cols = pl.ds(pl.multiple_of(n * 256, 256), 256)
        s = ps[3, :, cols].astype(F32) + rr[0, :, cols].astype(F32) + rr[1, :, cols].astype(F32)
        out[:, cols] = (stream[:, cols].astype(F32) + s).astype(BF)
        return 0

    lax.fori_loop(0, 8, add, 0)

    mark('added')
    assert count['s'] <= ssem.shape[0] and count['r'] <= rsem.shape[0], count
    for cp in open_sends:
        cp.wait_send()

    mark('sends_done')
    @pl.when(tp == 3)
    def _():
        for t in range(4):
            next_copy(t).wait_send()


def local(
    residual_entry_input, query_matrix_rows, key_matrix_rows, value_matrix_rows,
    output_gate_logits, input_gate_logits, forget_gate_logits, forget_decay_offset,
    head_norm_gain, cell_output_weight, feedforward_norm_gain, gate_up_weight,
    value_up_weight, gate_filter_taps, value_filter_taps, down_projection_weight,
):
    def chunks(gate):
        return gate.T.reshape(2, CH, L).transpose(1, 0, 2).reshape(2 * CH, L)

    hbm = pl.BlockSpec(memory_space=pl.ANY)
    vmem = pl.BlockSpec(memory_space=pltpu.VMEM)
    scratch = [
        pltpu.VMEM((1024, 256), BF), pltpu.VMEM((1024, 256), BF), pltpu.VMEM((1024, 512), BF),
        pltpu.VMEM((1024, 512), BF), pltpu.VMEM((256, D), BF),
        pltpu.VMEM((4, 4, 2, 64, 2 * FFD), BF), pltpu.VMEM((4, 4, 2, 64, FFD), BF),
        pltpu.VMEM((4, 2, 2, 4, 32, D), BF),
        pltpu.VMEM((CH, 2, DK, DV + L), F32), pltpu.VMEM((CH, 2, L, DV + L), F32),
        pltpu.VMEM((L, L), F32), pltpu.VMEM((4, 2 * CH, L), F32),
        pltpu.VMEM((CH, 2, DK, DV + L), BF), pltpu.VMEM((2, DK, DV + L), F32),
        pltpu.VMEM((2, 1, L), F32), pltpu.VMEM((2 * CH, L), F32),
        pltpu.VMEM((2, DK, DV), BF), pltpu.VMEM((2, 8, L), F32),
        pltpu.VMEM((2, DK, DV), BF), pltpu.VMEM((2, 8, L), F32),
        pltpu.VMEM((4, DK, DV), BF), pltpu.VMEM((4, 8, L), F32),
        pltpu.VMEM((4, DK, DV), BF), pltpu.VMEM((4, 8, L), F32),
        pltpu.VMEM((DK, DV), BF), pltpu.VMEM((8, L), F32),
        pltpu.VMEM((DK, DV), BF), pltpu.VMEM((8, L), F32),
        pltpu.VMEM((1024, 512), BF), pltpu.VMEM((2, 128, 512), BF), pltpu.VMEM((4, 256, 512), BF),
        pltpu.VMEM((256, D), BF),
        pltpu.VMEM((8, 144, D), BF), pltpu.VMEM((2, 2, D), F32), pltpu.VMEM((4, 2, 2, D), F32),
        pltpu.VMEM((2, D), F32), pltpu.VMEM((2, 288, 256), F32), pltpu.VMEM((2, 256, FFD), BF),
        pltpu.VMEM((4, 256, D), BF), pltpu.VMEM((2, 128, D), BF), pltpu.VMEM((2, 256, D), BF),
        pltpu.SemaphoreType.DMA((32,)), pltpu.SemaphoreType.DMA((176,)),
        pltpu.SemaphoreType.DMA((176,)),
    ]
    return pl.pallas_call(
        kernel,
        out_shape=jax.ShapeDtypeStruct((256, D), BF),
        in_specs=[hbm, hbm, hbm, hbm, hbm, vmem, vmem, vmem, vmem, hbm, vmem, hbm, hbm, hbm, vmem, vmem],
        out_specs=vmem,
        scratch_shapes=scratch,
        compiler_params=pltpu.CompilerParams(
            collective_id=0, has_side_effects=True, vmem_limit_bytes=67_043_328
        ),
    )(
        residual_entry_input, query_matrix_rows, key_matrix_rows, value_matrix_rows,
        output_gate_logits, chunks(input_gate_logits), chunks(forget_gate_logits),
        chunks(forget_decay_offset), head_norm_gain, cell_output_weight.reshape(2, 2, 4, 32, D),
        feedforward_norm_gain.reshape(1, D), gate_up_weight, value_up_weight,
        down_projection_weight.T, gate_filter_taps, value_filter_taps,
    )


def solution(mesh):
    split = Mesh(mesh.devices.reshape(4, 4, 2, mesh.shape["tp"]), SP_TP)
    placed = (
        P(SP_TP, None), P(SP, "tp"), P(SP, "tp"), P(SP, "tp"), P(SP, "tp"), P(SP, "tp"),
        P(SP, "tp"), P(SP, "tp"), P("tp", None), P("tp", None), P(), P(SP, "tp"), P(SP, "tp"),
        P(None, "tp"), P(None, "tp"), P("tp", SP),
    )
    return jax.shard_map(
        local, mesh=split, in_specs=placed, out_specs=P(SP_TP, None), check_vma=False
    )
```

```python
import jax
import jax.numpy as jnp
from jax import lax
from jax.experimental import pallas as pl
from jax.experimental.pallas import tpu as pltpu
from jax.sharding import Mesh
from jax.sharding import PartitionSpec as P

SP = ("sp_0", "sp_1", "sp_2")
SP_TP = ("sp_0", "sp_1", "sp_2", "tp")
MESH = pl.DeviceIdType.MESH

EPS = 1e-06
FIRST = 0
NEG = -1e30
L = 128
CH = 8
DK = 128
DV = 256
D = 2048
FFD = 1408
NT = FFD // 128
SCALE = DK**-0.5
F32 = jnp.float32
BF = jnp.bfloat16


def log1p_of(e):
    series = e * (1.0 - e * (0.5 - e * (1.0 / 3.0 - e * (0.25 - e * 0.2))))
    return jnp.where(e < 0.03, series, jnp.log(1.0 + e))


def kernel(
    res, q_in, k_in, v_in, og_in, ig, fg, off, gain, wo_in, fgain, gup, vup, dwn, gtap, vtap,
    out,
    q, k, v, og, rsd, wgv, wd, wo, dc, nl, colt, rows, cs, cpri, mpri, rs_rows,
    st1, ax1, st1r, ax1r, st2, ax2, st3, ax3, st4, ax4, st4r, ax4r,
    gated, al, orr, stream, gr, hs, hl, hp, gvs, hid, ps, rl, rr,
    lsem, ssem, rsem,
):
    z, y, c, tp = (lax.axis_index(a) for a in SP_TP)

    def up(i, n):
        return lax.rem(i + n, 4)

    y1, y3 = up(y, 1), up(y, 3)
    z1, z3 = up(z, 1), up(z, 3)
    x1, x2, x3 = up(tp, 1), up(tp, 2), up(tp, 3)
    other = 1 - c
    place = z * 8 + y * 2 + c

    def at_place(n):
        n = lax.rem(n + 32, 32)
        return {"sp_0": n // 8, "sp_1": lax.rem(n // 2, 4), "sp_2": lax.rem(n, 2)}

    count = {"l": 0, "s": 0, "r": 0}
    open_sends = []

    def take(kind):
        count[kind] += 1
        return count[kind] - 1

    def load(src, dst):
        cp = pltpu.make_async_copy(src, dst, lsem.at[take("l")])
        cp.start()
        return cp

    def send(src, dst, dev):
        cp = pltpu.make_async_remote_copy(
            src_ref=src, dst_ref=dst, send_sem=ssem.at[take("s")], recv_sem=rsem.at[take("r")],
            device_id=dev, device_id_type=MESH,
        )
        cp.start()
        open_sends.append(cp)
        return cp

    def arrived(copies):
        for cp in copies:
            cp.wait_recv()

    def mark(name):
        pass

    mark('entry')
    ld_k = load(k_in, k)
    ld_v = load(v_in, v)
    ld_w = [load(dwn, wd.at[z, y, c])]
    for n in range(NT):
        ld_w.append(load(gup.at[:, pl.ds(n * 128, 128)], wgv.at[z, y, c, :, pl.ds(n * 256, 128)]))
        ld_w.append(load(vup.at[:, pl.ds(n * 128, 128)], wgv.at[z, y, c, :, pl.ds(n * 256 + 128, 128)]))
    ld_wo = load(wo_in, wo.at[tp])
    ld_q = load(q_in, q)
    ld_og = load(og_in, og)
    ld_res = load(res, rsd)

    barrier = pltpu.get_barrier_semaphore()

    def hello(dev):
        pl.semaphore_signal(barrier, inc=1, device_id=dev, device_id_type=MESH)

    hello({"sp_2": other})
    for n in (1, 2, 3):
        hello({"sp_1": up(y, n)})
        hello({"sp_0": up(z, n)})
        hello({"tp": up(tp, n)})
    hello({**at_place(place - 1), "tp": 3})

    @pl.when(tp == 3)
    def _():
        for t in range(4):
            hello({**at_place(place + 1), "tp": t})
        pl.semaphore_wait(barrier, 15)

    @pl.when(tp != 3)
    def _():
        pl.semaphore_wait(barrier, 11)

    def halves(ref, zz, yy, lo, n):
        return ref.at[zz, yy, c, pl.ds(lo, n)]

    mark('barrier_done')
    for cp in ld_w:
        cp.wait()
    p1 = []
    for ref in (wgv, wd):
        mine_a, mine_b = halves(ref, z, y, 0, 32), halves(ref, z, y, 32, 32)
        p1 += [
            send(mine_a, mine_a, {"sp_1": y1}),
            send(mine_a, mine_a, {"sp_1": y3}),
            send(mine_b, mine_b, {"sp_0": z1}),
            send(mine_b, mine_b, {"sp_0": z3}),
        ]
    mark('w_issued')
    ld_wo.wait()
    y2, z2 = up(y, 2), up(z, 2)

    def wo_pieces(t, far):
        return wo.at[t, c, 0, y2 if far else y], wo.at[t, c, 1, z2 if far else z]

    xo1a, xo1b = (
        [send(piece, piece, {"tp": dev}) for piece in wo_pieces(tp, n) for dev in (x1, x3)]
        for n in (False, True)
    )

    def wo_swap(piece):
        return send(piece, piece, {"sp_2": other})

    def wo_onward(far):
        py, pz = wo_pieces(x3, far)[0], wo_pieces(x1, far)[1]
        return [send(py, py, {"tp": x1}), send(pz, pz, {"tp": x3})]

    def wo_spread(t):
        py, pz = wo_pieces(t, False)
        near = [
            send(py, py, {"sp_1": y1}), send(py, py, {"sp_1": y3}),
            send(pz, pz, {"sp_0": z1}), send(pz, pz, {"sp_0": z3}),
        ]
        return near, [wo_swap(py), wo_swap(pz)]

    def wo_near_swaps(t):
        return [
            wo_swap(piece)
            for piece in (
                wo.at[t, c, 0, y1], wo.at[t, c, 0, y3], wo.at[t, c, 1, z1], wo.at[t, c, 1, z3]
            )
        ]

    def slab(ref, n):
        piece_a, piece_b = halves(ref, z, up(y, n), 0, 32), halves(ref, up(z, n), y, 32, 32)
        return [
            send(piece_a, piece_a, {"sp_0": z1}),
            send(piece_a, piece_a, {"sp_0": z3}),
            send(piece_b, piece_b, {"sp_1": y1}),
            send(piece_b, piece_b, {"sp_1": y3}),
        ]

    def row_swap(ref):
        row_a = ref.at[z, :, c, pl.ds(0, 32)]
        row_b = ref.at[:, y, c, pl.ds(32, 32)]
        return [send(row_a, row_a, {"sp_2": other}), send(row_b, row_b, {"sp_2": other})]

    def across_two(ref):
        far = [
            send(src, src, dev)
            for src, dev in (
                (ref.at[z3, :, c, pl.ds(0, 16)], {"sp_0": z1}),
                (ref.at[z1, :, c, pl.ds(16, 16)], {"sp_0": z3}),
                (ref.at[:, y3, c, pl.ds(32, 16)], {"sp_1": y1}),
                (ref.at[:, y1, c, pl.ds(48, 16)], {"sp_1": y3}),
            )
        ]
        swap = [
            send(src, src, {"sp_2": other})
            for src in (
                ref.at[z1, :, c, pl.ds(0, 32)],
                ref.at[z3, :, c, pl.ds(0, 32)],
                ref.at[:, y1, c, pl.ds(32, 32)],
                ref.at[:, y3, c, pl.ds(32, 32)],
            )
        ]
        return far, swap

    def last_swap(ref):
        return [
            send(src, src, {"sp_2": other})
            for src in (ref.at[z2, :, c, pl.ds(0, 32)], ref.at[:, y2, c, pl.ds(32, 32)])
        ]

    mark('wo_issued')
    il = 15.0 * jnp.tanh(ig[...] / 15.0)
    xf = 15.0 * jnp.tanh(fg[...] / 15.0)
    fl = jnp.minimum(xf, 0.0) - log1p_of(jnp.exp(-jnp.abs(xf))) + off[...]
    r_i = lax.broadcasted_iota(jnp.int32, (L, L), 0)
    c_i = lax.broadcasted_iota(jnp.int32, (L, L), 1)
    causal = r_i >= c_i
    upper = (r_i <= c_i).astype(F32)
    cum = jnp.dot(fl, upper, preferred_element_type=F32, precision=lax.Precision.HIGHEST)
    a = il - cum
    lane = lax.broadcasted_iota(jnp.int32, (2 * CH, L), 1)
    cm = a
    for s in (1, 2, 4, 8, 16, 32, 64):
        cm = jnp.where(lane >= s, jnp.maximum(cm, pltpu.roll(cm, s, 1)), cm)
    last = jnp.broadcast_to(cum[:, L - 1 :], (2 * CH, L))
    peak = jnp.broadcast_to(cm[:, L - 1 :], (2 * CH, L))
    weight = jnp.exp(a - peak)
    mm = last + peak
    rows[0], rows[1], rows[2], rows[3] = a, weight, last, mm
    colt[...] = jnp.transpose(jnp.concatenate([cm, cum, jnp.zeros((96, L), F32)], axis=0))

    mark('gates')
    ld_k.wait()
    ld_v.wait()

    def chunk_state(j, _):
        at = pl.ds(pl.multiple_of(j * L, L), L)
        for h in range(2):
            kt = jnp.transpose(k[at, h * DK : (h + 1) * DK].astype(F32))
            kw = kt * rows[1, pl.ds(2 * j + h, 1), :]
            dc[j, h, :, :DV] = jnp.dot(
                kw.astype(BF), v[at, h * DV : (h + 1) * DV], preferred_element_type=F32
            )
            dc[j, h, :, DV:] = jnp.broadcast_to(jnp.sum(kw, axis=1, keepdims=True), (DK, L))
        return 0

    lax.fori_loop(0, CH, chunk_state, 0)

    mark('chunkstates')
    for h in range(2):
        tot = jnp.zeros((1, L), F32)
        logs = [None] * CH
        for j in reversed(range(CH)):
            row = 2 * j + h
            logs[j] = mm[row : row + 1] + tot
            tot = tot + last[row : row + 1]
        m = logs[0]
        for j in range(1, CH):
            m = jnp.maximum(m, logs[j])
        total = jnp.zeros((DK, DV + L), F32)
        for j in range(CH):
            total = total + jnp.exp(logs[j] - m)[:, 0:1] * dc[j, h]
        st1[h] = total[:, :DV].astype(BF)
        n_row = jnp.transpose(total[:, DV:])[0:1]
        ax1[h] = jnp.concatenate([n_row, tot, m, jnp.zeros((5, L), F32)], axis=0)

    mark('devstate')
    s1 = [send(st1, st1r, {"sp_2": other}), send(ax1, ax1r, {"sp_2": other})]

    ld_q.wait()

    def within(j, _):
        at = pl.ds(pl.multiple_of(j * L, L), L)
        turned = pltpu.roll(colt[...], lax.rem(L - 2 * j, L), 1)
        for h in range(2):
            raw = lax.dot_general(
                q[at, h * DK : (h + 1) * DK], k[at, h * DK : (h + 1) * DK],
                (((1,), (1,)), ((), ())), preferred_element_type=F32,
            ) * SCALE
            logit = rows[0, pl.ds(2 * j + h, 1), :] - turned[:, h : h + 1]
            sc = raw * jnp.exp(jnp.where(causal, logit, NEG))
            nl[j, h, :, :DV] = jnp.dot(
                sc.astype(BF), v[at, h * DV : (h + 1) * DV], preferred_element_type=F32
            )
            nl[j, h, :, DV:] = jnp.broadcast_to(jnp.sum(sc, axis=1, keepdims=True), (L, L))
        return 0

    lax.fori_loop(0, 2, within, 0)

    mark('within2')
    cf = jnp.full((1, L), c, jnp.int32).astype(F32)
    arrived(s1)

    def aux(ref, *at):
        block = ref[at] if at else ref[...]
        return block[0:1], block[1:2], block[2:3]

    def pack(n, tot, m):
        return jnp.concatenate([n, tot, m, jnp.zeros((5, L), F32)], axis=0)

    mark('s1_arr')
    n_o, t_o, m_o = aux(ax1, c)
    n_r, t_r, m_r = aux(ax1r, c)
    log_o = m_o + (1.0 - cf) * t_r
    log_r = m_r + cf * t_o
    m = jnp.maximum(log_o, log_r)
    w_o, w_r = jnp.exp(log_o - m), jnp.exp(log_r - m)
    st2[0] = (w_o[:, 0:1] * st1[c].astype(F32) + w_r[:, 0:1] * st1r[c].astype(F32)).astype(BF)
    ax2[0] = pack(w_o * n_o + w_r * n_r, t_o + t_r, m)
    s2 = []
    for n in (1, 2, 3):
        s2.append(send(st2.at[0], st2.at[n], {"sp_1": up(y, n)}))
        s2.append(send(ax2.at[0], ax2.at[n], {"sp_1": up(y, n)}))

    mark('s2_sent')
    lax.fori_loop(2, 5, within, 0)

    def scan_of(st, ax, me, whole):
        parts = [aux(ax, n) for n in range(4)]
        mine = jnp.full((1, L), me, jnp.int32)
        below = [None] + [mine >= n for n in (1, 2, 3)]
        zero = jnp.zeros((1, L), F32)
        after = zero
        for n in (1, 2, 3):
            after = after + jnp.where(below[n], 0.0, parts[n][1])
        run, run_up = zero, zero
        log_in, log_all = [None] * 4, [parts[0][2] + after] + [None] * 3
        for n in (1, 2, 3):
            log_in[n] = jnp.where(below[n], parts[n][2] + run, NEG)
            log_all[n] = jnp.where(
                below[n], parts[n][2] + run + parts[0][1] + after, parts[n][2] + run_up
            )
            run = run + jnp.where(below[n], parts[n][1], 0.0)
            run_up = run_up + jnp.where(below[n], 0.0, parts[n][1])
        m_in = jnp.maximum(jnp.maximum(log_in[1], log_in[2]), log_in[3])
        w_in = [None] + [jnp.where(below[n], jnp.exp(log_in[n] - m_in), 0.0) for n in (1, 2, 3)]
        blocks = [st[n].astype(F32) for n in range(4)]
        c_in = sum(w_in[n][:, 0:1] * blocks[n] for n in (1, 2, 3))
        n_in = sum(w_in[n] * parts[n][0] for n in (1, 2, 3))
        inside = (c_in, n_in, run, m_in)
        if not whole:
            return inside, None
        m_all = jnp.maximum(
            jnp.maximum(log_all[0], log_all[1]), jnp.maximum(log_all[2], log_all[3])
        )
        w_all = [jnp.exp(t - m_all) for t in log_all]
        c_all = sum(w_all[n][:, 0:1] * blocks[n] for n in range(4))
        n_all = sum(w_all[n] * parts[n][0] for n in range(4))
        return inside, (c_all, n_all, run + run_up + parts[0][1], m_all)

    mark('within5')
    arrived(s2)
    mark('s2_arr')
    y_in, y_all = scan_of(st2, ax2, y, True)
    st3[0] = y_all[0].astype(BF)
    ax3[0] = pack(*y_all[1:])
    s3 = []
    for n in (1, 2, 3):
        s3.append(send(st3.at[0], st3.at[n], {"sp_0": up(z, n)}))
        s3.append(send(ax3.at[0], ax3.at[n], {"sp_0": up(z, n)}))
    cpri[0, :, :DV] = y_in[0]

    mark('s3_sent')
    arrived(xo1a)
    xo2a = wo_onward(False)
    near_a, wpair = wo_spread(x1)
    near_b, more = wo_spread(x3)
    wpair += more
    mark('xo1_arr')
    mark('p2_sent')
    lax.fori_loop(5, CH, within, 0)

    mark('within8')
    arrived(xo1b)
    xo2b = wo_onward(True)
    arrived(xo2a)
    mark('xo2_arr')
    near_c, more = wo_spread(x2)
    wpair += more
    arrived(p1)
    p2 = []
    for ref in (wgv, wd):
        for src, dev in (
            (halves(ref, z, y3, 0, 16), {"sp_1": y1}),
            (halves(ref, z, y1, 16, 16), {"sp_1": y3}),
            (halves(ref, z3, y, 32, 16), {"sp_0": z1}),
            (halves(ref, z1, y, 48, 16), {"sp_0": z3}),
        ):
            p2.append(send(src, src, dev))
    g_far1 = slab(wgv, 0) + slab(wgv, 1) + slab(wgv, 3)
    arrived(s3)
    mark('s3_arr')
    z_in, _ = scan_of(st3, ax3, z, False)
    m = jnp.maximum(y_in[2] + z_in[3], y_in[3])
    w_z, w_y = jnp.exp(y_in[2] + z_in[3] - m), jnp.exp(y_in[3] - m)
    st4[...] = (w_z[:, 0:1] * z_in[0] + w_y[:, 0:1] * cpri[0, :, :DV]).astype(BF)
    ax4[...] = pack(w_z * z_in[1] + w_y * y_in[1], z_in[2] + y_in[2], m)
    s4 = [send(st4, st4r, {"sp_2": other}), send(ax4, ax4r, {"sp_2": other})]

    mark('s4_sent')
    arrived(s4)
    mark('s4_arr')
    last_in = jnp.full((1, L), c, jnp.int32) == 1
    for h, st, ax in ((c, st4, ax4), (other, st4r, ax4r)):
        n_b, t_b, m_b = aux(ax)
        n_p, t_p, m_p = aux(ax1r, h)
        m_p = jnp.where(last_in, m_p, NEG)
        m_b = m_b + cf * t_p
        m = jnp.maximum(m_b, m_p)
        w_b, w_p = jnp.exp(m_b - m), jnp.where(last_in, jnp.exp(m_p - m), 0.0)
        cpri[h, :, :DV] = w_b[:, 0:1] * st[...].astype(F32) + w_p[:, 0:1] * st1r[h].astype(F32)
        n_row = w_b * n_b + w_p * n_p
        cpri[h, :, DV:] = jnp.transpose(jnp.broadcast_to(n_row, (L, L)))
        mpri[h] = m

    def carry(j, _):
        for h in range(2):
            state, m_old = cpri[h], mpri[h]
            cs[j, h] = state.astype(BF)
            row = pl.ds(2 * j + h, 1)
            rs_rows[row, :] = m_old
            decayed, fresh = rows[2, row, :] + m_old, rows[3, row, :]
            m_new = jnp.maximum(decayed, fresh)
            cpri[h] = (
                jnp.exp(decayed - m_new)[:, 0:1] * state
                + jnp.exp(fresh - m_new)[:, 0:1] * dc[j, h]
            )
            mpri[h] = m_new
        return 0

    mark('prior')
    lax.fori_loop(0, CH, carry, 0)

    mark('carried')
    ld_og.wait()

    def finish(j, _):
        at = pl.ds(pl.multiple_of(j * L, L), L)
        turned = pltpu.roll(colt[...], lax.rem(L - 2 * j, L), 1)
        for h in range(2):
            r = rs_rows[pl.ds(2 * j + h, 1), :][:, 0:1]
            cmc, cuc = turned[:, h : h + 1], turned[:, 16 + h : 17 + h]
            g = jnp.maximum(cmc, r)
            e1, e2 = jnp.exp(cmc - g), jnp.exp(r - g) * SCALE
            qc = jnp.dot(q[at, h * DK : (h + 1) * DK], cs[j, h], preferred_element_type=F32)
            both = e1 * nl[j, h] + e2 * qc
            inv = 1.0 / jnp.maximum(jnp.abs(both[:, DV:]), jnp.exp(-cuc - g))
            mo = both[:, :DV] * jnp.concatenate([inv, inv], axis=1)
            norm = lax.rsqrt(jnp.mean(mo * mo, axis=1, keepdims=True) + EPS)
            gate = jax.nn.sigmoid(og[at, h * DV : (h + 1) * DV].astype(F32))
            gated[at, h * DV : (h + 1) * DV] = (mo * norm * gain[h : h + 1, :] * gate).astype(BF)
        return 0

    a2a, legs, relayed = [[], []], [None, None], [None, None]

    def pass_on(half):
        arrived(legs[half])
        relayed[half] = [
            send(al.at[half, 0], orr.at[x3, pl.ds(128 * half, 64)], {"tp": x1}),
            send(al.at[half, 1], orr.at[x1, pl.ds(128 * half + 64, 64)], {"tp": x3}),
        ]

    for half in (0, 1):
        for n in (2, 1, 3, 0):
            j = 2 * up(tp, n) + half
            lax.fori_loop(j, j + 1, finish, 0)
            start = pl.multiple_of(j * L, L)
            place_of = pl.ds(128 * half, 128)
            if n == 2:
                legs[half] = [
                    send(gated.at[pl.ds(start, 64)], al.at[half, 0], {"tp": x1}),
                    send(gated.at[pl.ds(start + 64, 64)], al.at[half, 1], {"tp": x3}),
                ]
                if half:
                    mark('cell_hi2')
                    pass_on(0)
                    mark('leg0_arr')
            elif n:
                a2a[half].append(
                    send(gated.at[pl.ds(start, 128)], orr.at[tp, place_of], {"tp": up(tp, n)})
                )
            else:
                orr[tp, place_of] = gated[pl.ds(start, 128), :]
        if not half:
            mark('cell_lo')
            arrived(near_a)
            arrived(near_b)
            mark('near_ab')
            wpair += wo_near_swaps(x1) + wo_near_swaps(x3)
            for t in (x1, x3):
                wpair += [wo_swap(piece) for piece in wo_pieces(t, True)]
    pass_on(1)
    mark('cell_done')
    arrived(near_c)
    mark('near_c')
    arrived(xo2b)
    wpair += wo_near_swaps(x2) + [wo_swap(piece) for piece in wo_pieces(x2, True)]
    arrived(p2)
    mark('p2_arr')
    g_far1 += slab(wgv, 2)
    g_pair = row_swap(wgv)
    d_far1 = slab(wd, 0)

    mark('w2_arr')
    ld_res.wait()

    def half_rows(b, h):
        return gr.at[2 * b + h, pl.ds(16, 128)]

    gather = [None, None]
    for half in (0, 1):
        at = slice(128 * half, 128 * half + 128)
        arrived(relayed[half] + a2a[half])
        mark('a2a_arr')
        if not half:
            arrived(wpair)
            mark('wpair_arr')

        def project(n, ss):
            cols = pl.ds(pl.multiple_of(n * 256, 256), 256)
            acc = rsd[at, cols].astype(F32)
            for t in range(4):
                acc = acc + jnp.dot(
                    orr[t, at], wo[t, :, :, :, :, cols].reshape(512, 256),
                    preferred_element_type=F32,
                )
            low = acc.astype(BF)
            stream[at, cols] = low
            wide = low.astype(F32)
            sq = wide * wide
            return ss + sq[:, :L] + sq[:, L:]

        ss = lax.fori_loop(0, 8, project, jnp.zeros((128, L), F32))
        norm = lax.rsqrt(jnp.sum(ss, axis=1, keepdims=True) * (1.0 / D) + EPS)

        def normed(n, _):
            cols = pl.ds(pl.multiple_of(n * 256, 256), 256)
            rows_n = (stream[at, cols].astype(F32) * norm * fgain[:, cols]).astype(BF)
            gr[2 * tp + half, pl.ds(16, 128), cols] = rows_n
            if half:
                hs[:, cols] = rows_n[126:128].astype(F32)
            return 0

        lax.fori_loop(0, 8, normed, 0)
        mark('normed')
        mine = half_rows(tp, half)
        gather[half] = [send(mine, mine, {"tp": x1}), send(mine, mine, {"tp": x3})]

    halo = send(hs, hl, {"tp": x2})
    s_next = [take("s") for _ in range(4)]
    r_next = take("r")

    def next_copy(t):
        return pltpu.make_async_remote_copy(
            src_ref=hs, dst_ref=hp, send_sem=ssem.at[s_next[t]], recv_sem=rsem.at[r_next],
            device_id={**at_place(place + 1), "tp": t}, device_id_type=MESH,
        )

    @pl.when(tp == 3)
    def _():
        for t in range(4):
            next_copy(t).start()

    mark('g1_sent')
    arrived(g_far1)
    mark('gfar1_arr')
    g_far2, more = across_two(wgv)
    g_pair += more
    for n in (1, 3, 2):
        d_far1 += slab(wd, n)
    d_pair = row_swap(wd)
    arrived(gather[0])
    mark('g1a_arr')
    part_a = half_rows(x3, 0)
    g2 = [send(part_a, part_a, {"tp": x1})]
    arrived(g_far2)
    mark('gfar2_arr')
    g_pair += last_swap(wgv)
    arrived(d_far1)
    mark('dfar1_arr')
    d_far2, more = across_two(wd)
    d_pair += more
    arrived(gather[1])
    mark('g1b_arr')
    part_b = half_rows(x1, 1)
    g2.append(send(part_b, part_b, {"tp": x3}))
    arrived([halo])
    next_copy(0).wait_recv()
    mark('halo_arr')
    arrived(g_pair)
    mark('gpair_arr')

    def tail_of(two):
        return jnp.concatenate([jnp.zeros((14, D), F32), two], axis=0)

    from_before = tail_of(jnp.where(jnp.full((2, D), place, jnp.int32) == 0, 0.0, hp[...]))

    def copy_of(src, dst, dev):
        cp = pltpu.make_async_remote_copy(
            src_ref=src, dst_ref=dst, send_sem=ssem.at[take("s")], recv_sem=rsem.at[take("r")],
            device_id=dev, device_id_type=MESH,
        )
        open_sends.append(cp)
        return cp

    lo, hi = pl.ds(0, 128), pl.ds(128, 128)
    direct = [
        copy_of(ps.at[0, lo], rr.at[0, hi], {"tp": x1}),
        copy_of(ps.at[0, hi], rr.at[1, lo], {"tp": x3}),
    ]
    far = [
        copy_of(ps.at[2, lo], rl.at[0], {"tp": x1}),
        copy_of(ps.at[2, hi], rl.at[1], {"tp": x3}),
    ]
    summed = [
        copy_of(ps.at[1, lo], rr.at[0, lo], {"tp": x1}),
        copy_of(ps.at[1, hi], rr.at[1, hi], {"tp": x3}),
    ]

    def rows_of(i):
        pair = i // 2
        h0 = (1 - pair) * (1 - i)
        b0 = up(tp, 1 - pair + pair * (6 - 2 * i))
        b1 = up(tp, 3 * (1 - pair) + pair * (6 - 2 * i))
        return (b0, h0), (b1, 1 - h0)

    def widen(i):
        spots = rows_of(i)
        for m, (b, h) in enumerate(spots):
            if i is FIRST and m:
                near = tail_of(hl[...])
            else:
                near = gr[2 * up(b, 3 + h) + 1 - h, pl.ds(128, 16), :].astype(F32)
            starts = jnp.full((16, D), b + 4 * h, jnp.int32) == 0
            gr[2 * b + h, pl.ds(0, 16), :] = jnp.where(starts, from_before, near).astype(BF)
        e0, e1 = (2 * b + h for b, h in spots)

        def product(n):
            w = wgv[:, :, :, :, n * 256 : n * 256 + 256].reshape(D, 256)
            both = jnp.concatenate([gr[e0], gr[e1]], axis=0)
            gvs[n % 2] = jnp.dot(both, w, preferred_element_type=F32)

        def gate_of(n):
            cols = slice(n * L, n * L + L)
            for p in range(2):
                at = 144 * p + 14

                def conv(lanes, tap):
                    return (
                        tap[0:1, cols] * gvs[n % 2, at : at + 128, lanes]
                        + tap[1:2, cols] * gvs[n % 2, at + 1 : at + 129, lanes]
                        + tap[2:3, cols] * gvs[n % 2, at + 2 : at + 130, lanes]
                    )

                cg, cv = conv(slice(0, L), gtap), conv(slice(L, 256), vtap)
                hid[lax.rem(i, 2), 128 * p : 128 * p + 128, cols] = (
                    cg / (1.0 + jnp.exp(-cg)) * cv
                ).astype(BF)

        product(0)
        for n in range(1, NT):
            product(n)
            gate_of(n - 1)
        gate_of(NT - 1)

    def narrow(i):
        for n in range(8):
            w = wd[n // 2, 2 * (n % 2) : 2 * (n % 2) + 2].reshape(256, FFD)
            p = lax.dot_general(
                hid[lax.rem(i, 2)], w, (((1,), (1,)), ((), ())), preferred_element_type=F32
            )
            ps[i, :, n * 256 : n * 256 + 256] = p.astype(BF)

    widen(FIRST)
    mark('up0')
    arrived(d_far2)
    mark('dfar2_arr')
    d_pair += last_swap(wd)
    arrived(d_pair)
    mark('dpair_arr')
    narrow(FIRST)
    mark('down0')
    for cp in direct:
        cp.start()
    widen(1)
    narrow(1)
    mark('down1')
    arrived(g2)
    mark('g2_arr')

    def rest(i, _):
        widen(i)
        narrow(i)

        @pl.when(i == 2)
        def _():
            mark('down2')
            for cp in far:
                cp.start()

        return 0

    lax.fori_loop(2, 4, rest, 0)
    mark('fed')
    for n, (cp, half) in enumerate(zip(far, (lo, hi))):
        cp.wait_recv()
        mark('far_arr')

        def relay(m, _):
            cols = pl.ds(pl.multiple_of(m * 256, 256), 256)
            ps[1, half, cols] = (
                ps[1, half, cols].astype(F32) + rl[n, :, cols].astype(F32)
            ).astype(BF)
            return 0

        lax.fori_loop(0, 8, relay, 0)
        summed[n].start()
    arrived(direct)
    mark('direct_arr')
    arrived(summed)
    mark('back_arr')

    def add(n, _):
        cols = pl.ds(pl.multiple_of(n * 256, 256), 256)
        s = ps[3, :, cols].astype(F32) + rr[0, :, cols].astype(F32) + rr[1, :, cols].astype(F32)
        out[:, cols] = (stream[:, cols].astype(F32) + s).astype(BF)
        return 0

    lax.fori_loop(0, 8, add, 0)

    mark('added')
    assert count['s'] <= ssem.shape[0] and count['r'] <= rsem.shape[0], count
    for cp in open_sends:
        cp.wait_send()

    mark('sends_done')
    @pl.when(tp == 3)
    def _():
        for t in range(4):
            next_copy(t).wait_send()


def local(
    residual_entry_input, query_matrix_rows, key_matrix_rows, value_matrix_rows,
    output_gate_logits, input_gate_logits, forget_gate_logits, forget_decay_offset,
    head_norm_gain, cell_output_weight, feedforward_norm_gain, gate_up_weight,
    value_up_weight, gate_filter_taps, value_filter_taps, down_projection_weight,
):
    def chunks(gate):
        return gate.T.reshape(2, CH, L).transpose(1, 0, 2).reshape(2 * CH, L)

    hbm = pl.BlockSpec(memory_space=pl.ANY)
    vmem = pl.BlockSpec(memory_space=pltpu.VMEM)
    scratch = [
        pltpu.VMEM((1024, 256), BF), pltpu.VMEM((1024, 256), BF), pltpu.VMEM((1024, 512), BF),
        pltpu.VMEM((1024, 512), BF), pltpu.VMEM((256, D), BF),
        pltpu.VMEM((4, 4, 2, 64, 2 * FFD), BF), pltpu.VMEM((4, 4, 2, 64, FFD), BF),
        pltpu.VMEM((4, 2, 2, 4, 32, D), BF),
        pltpu.VMEM((CH, 2, DK, DV + L), F32), pltpu.VMEM((CH, 2, L, DV + L), F32),
        pltpu.VMEM((L, L), F32), pltpu.VMEM((4, 2 * CH, L), F32),
        pltpu.VMEM((CH, 2, DK, DV + L), BF), pltpu.VMEM((2, DK, DV + L), F32),
        pltpu.VMEM((2, 1, L), F32), pltpu.VMEM((2 * CH, L), F32),
        pltpu.VMEM((2, DK, DV), BF), pltpu.VMEM((2, 8, L), F32),
        pltpu.VMEM((2, DK, DV), BF), pltpu.VMEM((2, 8, L), F32),
        pltpu.VMEM((4, DK, DV), BF), pltpu.VMEM((4, 8, L), F32),
        pltpu.VMEM((4, DK, DV), BF), pltpu.VMEM((4, 8, L), F32),
        pltpu.VMEM((DK, DV), BF), pltpu.VMEM((8, L), F32),
        pltpu.VMEM((DK, DV), BF), pltpu.VMEM((8, L), F32),
        pltpu.VMEM((1024, 512), BF), pltpu.VMEM((2, 2, 64, 512), BF), pltpu.VMEM((4, 256, 512), BF),
        pltpu.VMEM((256, D), BF),
        pltpu.VMEM((8, 144, D), BF), pltpu.VMEM((2, D), F32), pltpu.VMEM((2, D), F32),
        pltpu.VMEM((2, D), F32), pltpu.VMEM((2, 288, 256), F32), pltpu.VMEM((2, 256, FFD), BF),
        pltpu.VMEM((4, 256, D), BF), pltpu.VMEM((2, 128, D), BF), pltpu.VMEM((2, 256, D), BF),
        pltpu.SemaphoreType.DMA((32,)), pltpu.SemaphoreType.DMA((176,)),
        pltpu.SemaphoreType.DMA((176,)),
    ]
    return pl.pallas_call(
        kernel,
        out_shape=jax.ShapeDtypeStruct((256, D), BF),
        in_specs=[hbm, hbm, hbm, hbm, hbm, vmem, vmem, vmem, vmem, hbm, vmem, hbm, hbm, hbm, vmem, vmem],
        out_specs=vmem,
        scratch_shapes=scratch,
        compiler_params=pltpu.CompilerParams(
            collective_id=0, has_side_effects=True, vmem_limit_bytes=67_043_328
        ),
    )(
        residual_entry_input, query_matrix_rows, key_matrix_rows, value_matrix_rows,
        output_gate_logits, chunks(input_gate_logits), chunks(forget_gate_logits),
        chunks(forget_decay_offset), head_norm_gain, cell_output_weight.reshape(2, 2, 4, 32, D),
        feedforward_norm_gain.reshape(1, D), gate_up_weight, value_up_weight,
        down_projection_weight.T, gate_filter_taps, value_filter_taps,
    )


def solution(mesh):
    split = Mesh(mesh.devices.reshape(4, 4, 2, mesh.shape["tp"]), SP_TP)
    placed = (
        P(SP_TP, None), P(SP, "tp"), P(SP, "tp"), P(SP, "tp"), P(SP, "tp"), P(SP, "tp"),
        P(SP, "tp"), P(SP, "tp"), P("tp", None), P("tp", None), P(), P(SP, "tp"), P(SP, "tp"),
        P(None, "tp"), P(None, "tp"), P("tp", SP),
    )
    return jax.shard_map(
        local, mesh=split, in_specs=placed, out_specs=P(SP_TP, None), check_vma=False
    )
```

```python
import jax
import jax.numpy as jnp
from jax import lax
from jax.experimental import pallas as pl
from jax.experimental.pallas import tpu as pltpu
from jax.sharding import Mesh
from jax.sharding import PartitionSpec as P

SP = ("sp_0", "sp_1", "sp_2")
SP_TP = ("sp_0", "sp_1", "sp_2", "tp")
MESH = pl.DeviceIdType.MESH

EPS = 1e-06
FIRST = 0
NEG = -1e30
L = 128
CH = 8
DK = 128
DV = 256
D = 2048
FFD = 1408
NT = FFD // 128
SCALE = DK**-0.5
F32 = jnp.float32
BF = jnp.bfloat16


def log1p_of(e):
    series = e * (1.0 - e * (0.5 - e * (1.0 / 3.0 - e * (0.25 - e * 0.2))))
    return jnp.where(e < 0.03, series, jnp.log(1.0 + e))


def kernel(
    res, q_in, k_in, v_in, og_in, ig, fg, off, gain, wo_in, fgain, gup, vup, dwn, gtap, vtap,
    out,
    q, k, v, og, rsd, wgv, wd, wo, dc, nl, colt, rows, cs, cpri, mpri, rs_rows,
    st1, ax1, st1r, ax1r, st2, ax2, st3, ax3, st4, ax4, st4r, ax4r,
    gated, al, orr, stream, gr, hs, hl, hp, gvs, hid, ps, rl, rr,
    lsem, ssem, rsem,
):
    z, y, c, tp = (lax.axis_index(a) for a in SP_TP)

    def up(i, n):
        return lax.rem(i + n, 4)

    y1, y3 = up(y, 1), up(y, 3)
    z1, z3 = up(z, 1), up(z, 3)
    x1, x2, x3 = up(tp, 1), up(tp, 2), up(tp, 3)
    other = 1 - c
    place = z * 8 + y * 2 + c

    def at_place(n):
        n = lax.rem(n + 32, 32)
        return {"sp_0": n // 8, "sp_1": lax.rem(n // 2, 4), "sp_2": lax.rem(n, 2)}

    count = {"l": 0, "s": 0, "r": 0}
    open_sends = []

    def take(kind):
        count[kind] += 1
        return count[kind] - 1

    def load(src, dst):
        cp = pltpu.make_async_copy(src, dst, lsem.at[take("l")])
        cp.start()
        return cp

    def send(src, dst, dev):
        cp = pltpu.make_async_remote_copy(
            src_ref=src, dst_ref=dst, send_sem=ssem.at[take("s")], recv_sem=rsem.at[take("r")],
            device_id=dev, device_id_type=MESH,
        )
        cp.start()
        open_sends.append(cp)
        return cp

    def arrived(copies):
        for cp in copies:
            cp.wait_recv()

    def mark(name):
        pass

    mark('entry')
    ld_k = load(k_in, k)
    ld_v = load(v_in, v)
    ld_w = [load(dwn, wd.at[z, y, c])]
    for n in range(NT):
        ld_w.append(load(gup.at[:, pl.ds(n * 128, 128)], wgv.at[z, y, c, :, pl.ds(n * 256, 128)]))
        ld_w.append(load(vup.at[:, pl.ds(n * 128, 128)], wgv.at[z, y, c, :, pl.ds(n * 256 + 128, 128)]))
    ld_wo = load(wo_in, wo.at[tp])
    ld_q = load(q_in, q)
    ld_og = load(og_in, og)
    ld_res = load(res, rsd)

    barrier = pltpu.get_barrier_semaphore()

    def hello(dev):
        pl.semaphore_signal(barrier, inc=1, device_id=dev, device_id_type=MESH)

    hello({"sp_2": other})
    for n in (1, 2, 3):
        hello({"sp_1": up(y, n)})
        hello({"sp_0": up(z, n)})
        hello({"tp": up(tp, n)})
    hello({**at_place(place - 1), "tp": 3})

    @pl.when(tp == 3)
    def _():
        for t in range(4):
            hello({**at_place(place + 1), "tp": t})
        pl.semaphore_wait(barrier, 15)

    @pl.when(tp != 3)
    def _():
        pl.semaphore_wait(barrier, 11)

    def halves(ref, zz, yy, lo, n):
        return ref.at[zz, yy, c, pl.ds(lo, n)]

    mark('barrier_done')
    for cp in ld_w:
        cp.wait()
    p1 = []
    for ref in (wgv, wd):
        mine_a, mine_b = halves(ref, z, y, 0, 32), halves(ref, z, y, 32, 32)
        p1 += [
            send(mine_a, mine_a, {"sp_1": y1}),
            send(mine_a, mine_a, {"sp_1": y3}),
            send(mine_b, mine_b, {"sp_0": z1}),
            send(mine_b, mine_b, {"sp_0": z3}),
        ]
    mark('w_issued')
    ld_wo.wait()
    y2, z2 = up(y, 2), up(z, 2)

    def wo_pieces(t, far):
        return wo.at[t, c, 0, y2 if far else y], wo.at[t, c, 1, z2 if far else z]

    xo1a, xo1b = (
        [send(piece, piece, {"tp": dev}) for piece in wo_pieces(tp, n) for dev in (x1, x3)]
        for n in (False, True)
    )

    def wo_swap(piece):
        return send(piece, piece, {"sp_2": other})

    def wo_onward(far):
        py, pz = wo_pieces(x3, far)[0], wo_pieces(x1, far)[1]
        return [send(py, py, {"tp": x1}), send(pz, pz, {"tp": x3})]

    def wo_spread(t):
        py, pz = wo_pieces(t, False)
        near = [
            send(py, py, {"sp_1": y1}), send(py, py, {"sp_1": y3}),
            send(pz, pz, {"sp_0": z1}), send(pz, pz, {"sp_0": z3}),
        ]
        return near, [wo_swap(py), wo_swap(pz)]

    def wo_near_swaps(t):
        return [
            wo_swap(piece)
            for piece in (
                wo.at[t, c, 0, y1], wo.at[t, c, 0, y3], wo.at[t, c, 1, z1], wo.at[t, c, 1, z3]
            )
        ]

    def slab(ref, n):
        piece_a, piece_b = halves(ref, z, up(y, n), 0, 32), halves(ref, up(z, n), y, 32, 32)
        return [
            send(piece_a, piece_a, {"sp_0": z1}),
            send(piece_a, piece_a, {"sp_0": z3}),
            send(piece_b, piece_b, {"sp_1": y1}),
            send(piece_b, piece_b, {"sp_1": y3}),
        ]

    def row_swap(ref):
        row_a = ref.at[z, :, c, pl.ds(0, 32)]
        row_b = ref.at[:, y, c, pl.ds(32, 32)]
        return [send(row_a, row_a, {"sp_2": other}), send(row_b, row_b, {"sp_2": other})]

    def across_two(ref):
        far = [
            send(src, src, dev)
            for src, dev in (
                (ref.at[z3, :, c, pl.ds(0, 16)], {"sp_0": z1}),
                (ref.at[z1, :, c, pl.ds(16, 16)], {"sp_0": z3}),
                (ref.at[:, y3, c, pl.ds(32, 16)], {"sp_1": y1}),
                (ref.at[:, y1, c, pl.ds(48, 16)], {"sp_1": y3}),
            )
        ]
        swap = [
            send(src, src, {"sp_2": other})
            for src in (
                ref.at[z1, :, c, pl.ds(0, 32)],
                ref.at[z3, :, c, pl.ds(0, 32)],
                ref.at[:, y1, c, pl.ds(32, 32)],
                ref.at[:, y3, c, pl.ds(32, 32)],
            )
        ]
        return far, swap

    def last_swap(ref):
        return [
            send(src, src, {"sp_2": other})
            for src in (ref.at[z2, :, c, pl.ds(0, 32)], ref.at[:, y2, c, pl.ds(32, 32)])
        ]

    mark('wo_issued')
    il = 15.0 * jnp.tanh(ig[...] / 15.0)
    xf = 15.0 * jnp.tanh(fg[...] / 15.0)
    fl = jnp.minimum(xf, 0.0) - log1p_of(jnp.exp(-jnp.abs(xf))) + off[...]
    r_i = lax.broadcasted_iota(jnp.int32, (L, L), 0)
    c_i = lax.broadcasted_iota(jnp.int32, (L, L), 1)
    causal = r_i >= c_i
    upper = (r_i <= c_i).astype(F32)
    cum = jnp.dot(fl, upper, preferred_element_type=F32, precision=lax.Precision.HIGHEST)
    a = il - cum
    lane = lax.broadcasted_iota(jnp.int32, (2 * CH, L), 1)
    cm = a
    for s in (1, 2, 4, 8, 16, 32, 64):
        cm = jnp.where(lane >= s, jnp.maximum(cm, pltpu.roll(cm, s, 1)), cm)
    last = jnp.broadcast_to(cum[:, L - 1 :], (2 * CH, L))
    peak = jnp.broadcast_to(cm[:, L - 1 :], (2 * CH, L))
    weight = jnp.exp(a - peak)
    mm = last + peak
    rows[0], rows[1], rows[2], rows[3] = a, weight, last, mm
    colt[...] = jnp.transpose(jnp.concatenate([cm, cum, jnp.zeros((96, L), F32)], axis=0))

    mark('gates')
    ld_k.wait()
    ld_v.wait()

    def chunk_state(j, _):
        at = pl.ds(pl.multiple_of(j * L, L), L)
        for h in range(2):
            kt = jnp.transpose(k[at, h * DK : (h + 1) * DK].astype(F32))
            kw = kt * rows[1, pl.ds(2 * j + h, 1), :]
            dc[j, h, :, :DV] = jnp.dot(
                kw.astype(BF), v[at, h * DV : (h + 1) * DV], preferred_element_type=F32
            )
            dc[j, h, :, DV:] = jnp.broadcast_to(jnp.sum(kw, axis=1, keepdims=True), (DK, L))
        return 0

    lax.fori_loop(0, CH, chunk_state, 0)

    mark('chunkstates')
    for h in range(2):
        tot = jnp.zeros((1, L), F32)
        logs = [None] * CH
        for j in reversed(range(CH)):
            row = 2 * j + h
            logs[j] = mm[row : row + 1] + tot
            tot = tot + last[row : row + 1]
        m = logs[0]
        for j in range(1, CH):
            m = jnp.maximum(m, logs[j])
        total = jnp.zeros((DK, DV + L), F32)
        for j in range(CH):
            total = total + jnp.exp(logs[j] - m)[:, 0:1] * dc[j, h]
        st1[h] = total[:, :DV].astype(BF)
        n_row = jnp.transpose(total[:, DV:])[0:1]
        ax1[h] = jnp.concatenate([n_row, tot, m, jnp.zeros((5, L), F32)], axis=0)

    mark('devstate')
    s1 = [send(st1, st1r, {"sp_2": other}), send(ax1, ax1r, {"sp_2": other})]

    ld_q.wait()

    def within(j, _):
        at = pl.ds(pl.multiple_of(j * L, L), L)
        turned = pltpu.roll(colt[...], lax.rem(L - 2 * j, L), 1)
        for h in range(2):
            raw = lax.dot_general(
                q[at, h * DK : (h + 1) * DK], k[at, h * DK : (h + 1) * DK],
                (((1,), (1,)), ((), ())), preferred_element_type=F32,
            ) * SCALE
            logit = rows[0, pl.ds(2 * j + h, 1), :] - turned[:, h : h + 1]
            sc = raw * jnp.exp(jnp.where(causal, logit, NEG))
            nl[j, h, :, :DV] = jnp.dot(
                sc.astype(BF), v[at, h * DV : (h + 1) * DV], preferred_element_type=F32
            )
            nl[j, h, :, DV:] = jnp.broadcast_to(jnp.sum(sc, axis=1, keepdims=True), (L, L))
        return 0

    lax.fori_loop(0, 2, within, 0)

    mark('within2')
    cf = jnp.full((1, L), c, jnp.int32).astype(F32)
    arrived(s1)

    def aux(ref, *at):
        block = ref[at] if at else ref[...]
        return block[0:1], block[1:2], block[2:3]

    def pack(n, tot, m):
        return jnp.concatenate([n, tot, m, jnp.zeros((5, L), F32)], axis=0)

    mark('s1_arr')
    n_o, t_o, m_o = aux(ax1, c)
    n_r, t_r, m_r = aux(ax1r, c)
    log_o = m_o + (1.0 - cf) * t_r
    log_r = m_r + cf * t_o
    m = jnp.maximum(log_o, log_r)
    w_o, w_r = jnp.exp(log_o - m), jnp.exp(log_r - m)
    st2[0] = (w_o[:, 0:1] * st1[c].astype(F32) + w_r[:, 0:1] * st1r[c].astype(F32)).astype(BF)
    ax2[0] = pack(w_o * n_o + w_r * n_r, t_o + t_r, m)
    s2 = []
    for n in (1, 2, 3):
        s2.append(send(st2.at[0], st2.at[n], {"sp_1": up(y, n)}))
        s2.append(send(ax2.at[0], ax2.at[n], {"sp_1": up(y, n)}))

    mark('s2_sent')
    lax.fori_loop(2, 5, within, 0)

    def scan_of(st, ax, me, whole):
        parts = [aux(ax, n) for n in range(4)]
        mine = jnp.full((1, L), me, jnp.int32)
        below = [None] + [mine >= n for n in (1, 2, 3)]
        zero = jnp.zeros((1, L), F32)
        after = zero
        for n in (1, 2, 3):
            after = after + jnp.where(below[n], 0.0, parts[n][1])
        run, run_up = zero, zero
        log_in, log_all = [None] * 4, [parts[0][2] + after] + [None] * 3
        for n in (1, 2, 3):
            log_in[n] = jnp.where(below[n], parts[n][2] + run, NEG)
            log_all[n] = jnp.where(
                below[n], parts[n][2] + run + parts[0][1] + after, parts[n][2] + run_up
            )
            run = run + jnp.where(below[n], parts[n][1], 0.0)
            run_up = run_up + jnp.where(below[n], 0.0, parts[n][1])
        m_in = jnp.maximum(jnp.maximum(log_in[1], log_in[2]), log_in[3])
        w_in = [None] + [jnp.where(below[n], jnp.exp(log_in[n] - m_in), 0.0) for n in (1, 2, 3)]
        blocks = [st[n].astype(F32) for n in range(4)]
        c_in = sum(w_in[n][:, 0:1] * blocks[n] for n in (1, 2, 3))
        n_in = sum(w_in[n] * parts[n][0] for n in (1, 2, 3))
        inside = (c_in, n_in, run, m_in)
        if not whole:
            return inside, None
        m_all = jnp.maximum(
            jnp.maximum(log_all[0], log_all[1]), jnp.maximum(log_all[2], log_all[3])
        )
        w_all = [jnp.exp(t - m_all) for t in log_all]
        c_all = sum(w_all[n][:, 0:1] * blocks[n] for n in range(4))
        n_all = sum(w_all[n] * parts[n][0] for n in range(4))
        return inside, (c_all, n_all, run + run_up + parts[0][1], m_all)

    mark('within5')
    arrived(s2)
    mark('s2_arr')
    y_in, y_all = scan_of(st2, ax2, y, True)
    st3[0] = y_all[0].astype(BF)
    ax3[0] = pack(*y_all[1:])
    s3 = []
    for n in (1, 2, 3):
        s3.append(send(st3.at[0], st3.at[n], {"sp_0": up(z, n)}))
        s3.append(send(ax3.at[0], ax3.at[n], {"sp_0": up(z, n)}))
    cpri[0, :, :DV] = y_in[0]

    mark('s3_sent')
    arrived(xo1a)
    xo2a = wo_onward(False)
    near_a, wpair = wo_spread(x1)
    near_b, more = wo_spread(x3)
    wpair += more
    mark('xo1_arr')
    mark('p2_sent')
    lax.fori_loop(5, CH, within, 0)

    mark('within8')
    arrived(xo1b)
    xo2b = wo_onward(True)
    arrived(xo2a)
    mark('xo2_arr')
    near_c, more = wo_spread(x2)
    wpair += more
    arrived(p1)
    p2 = []
    for ref in (wgv, wd):
        for src, dev in (
            (halves(ref, z, y3, 0, 16), {"sp_1": y1}),
            (halves(ref, z, y1, 16, 16), {"sp_1": y3}),
            (halves(ref, z3, y, 32, 16), {"sp_0": z1}),
            (halves(ref, z1, y, 48, 16), {"sp_0": z3}),
        ):
            p2.append(send(src, src, dev))
    g_far1 = slab(wgv, 0) + slab(wgv, 1) + slab(wgv, 3)
    arrived(s3)
    mark('s3_arr')
    z_in, _ = scan_of(st3, ax3, z, False)
    m = jnp.maximum(y_in[2] + z_in[3], y_in[3])
    w_z, w_y = jnp.exp(y_in[2] + z_in[3] - m), jnp.exp(y_in[3] - m)
    st4[...] = (w_z[:, 0:1] * z_in[0] + w_y[:, 0:1] * cpri[0, :, :DV]).astype(BF)
    ax4[...] = pack(w_z * z_in[1] + w_y * y_in[1], z_in[2] + y_in[2], m)
    s4 = [send(st4, st4r, {"sp_2": other}), send(ax4, ax4r, {"sp_2": other})]

    mark('s4_sent')
    arrived(s4)
    mark('s4_arr')
    last_in = jnp.full((1, L), c, jnp.int32) == 1
    for h, st, ax in ((c, st4, ax4), (other, st4r, ax4r)):
        n_b, t_b, m_b = aux(ax)
        n_p, t_p, m_p = aux(ax1r, h)
        m_p = jnp.where(last_in, m_p, NEG)
        m_b = m_b + cf * t_p
        m = jnp.maximum(m_b, m_p)
        w_b, w_p = jnp.exp(m_b - m), jnp.where(last_in, jnp.exp(m_p - m), 0.0)
        cpri[h, :, :DV] = w_b[:, 0:1] * st[...].astype(F32) + w_p[:, 0:1] * st1r[h].astype(F32)
        n_row = w_b * n_b + w_p * n_p
        cpri[h, :, DV:] = jnp.transpose(jnp.broadcast_to(n_row, (L, L)))
        mpri[h] = m

    def carry(j, _):
        for h in range(2):
            state, m_old = cpri[h], mpri[h]
            cs[j, h] = state.astype(BF)
            row = pl.ds(2 * j + h, 1)
            rs_rows[row, :] = m_old
            decayed, fresh = rows[2, row, :] + m_old, rows[3, row, :]
            m_new = jnp.maximum(decayed, fresh)
            cpri[h] = (
                jnp.exp(decayed - m_new)[:, 0:1] * state
                + jnp.exp(fresh - m_new)[:, 0:1] * dc[j, h]
            )
            mpri[h] = m_new
        return 0

    mark('prior')
    lax.fori_loop(0, CH, carry, 0)

    mark('carried')
    ld_og.wait()

    def finish(j, _):
        at = pl.ds(pl.multiple_of(j * L, L), L)
        turned = pltpu.roll(colt[...], lax.rem(L - 2 * j, L), 1)
        for h in range(2):
            r = rs_rows[pl.ds(2 * j + h, 1), :][:, 0:1]
            cmc, cuc = turned[:, h : h + 1], turned[:, 16 + h : 17 + h]
            g = jnp.maximum(cmc, r)
            e1, e2 = jnp.exp(cmc - g), jnp.exp(r - g) * SCALE
            qc = jnp.dot(q[at, h * DK : (h + 1) * DK], cs[j, h], preferred_element_type=F32)
            both = e1 * nl[j, h] + e2 * qc
            inv = 1.0 / jnp.maximum(jnp.abs(both[:, DV:]), jnp.exp(-cuc - g))
            mo = both[:, :DV] * jnp.concatenate([inv, inv], axis=1)
            norm = lax.rsqrt(jnp.mean(mo * mo, axis=1, keepdims=True) + EPS)
            gate = jax.nn.sigmoid(og[at, h * DV : (h + 1) * DV].astype(F32))
            gated[at, h * DV : (h + 1) * DV] = (mo * norm * gain[h : h + 1, :] * gate).astype(BF)
        return 0

    a2a, legs, relayed = [[], []], [None, None], [None, None]

    def pass_on(half):
        arrived(legs[half])
        relayed[half] = [
            send(al.at[half, 0], orr.at[x3, pl.ds(128 * half, 64)], {"tp": x1}),
            send(al.at[half, 1], orr.at[x1, pl.ds(128 * half + 64, 64)], {"tp": x3}),
        ]

    for half in (0, 1):
        for n in (2, 1, 3, 0):
            j = 2 * up(tp, n) + half
            lax.fori_loop(j, j + 1, finish, 0)
            start = pl.multiple_of(j * L, L)
            place_of = pl.ds(128 * half, 128)
            if n == 2:
                legs[half] = [
                    send(gated.at[pl.ds(start, 64)], al.at[half, 0], {"tp": x1}),
                    send(gated.at[pl.ds(start + 64, 64)], al.at[half, 1], {"tp": x3}),
                ]
                if half:
                    mark('cell_hi2')
                    pass_on(0)
                    mark('leg0_arr')
            elif n:
                a2a[half].append(
                    send(gated.at[pl.ds(start, 128)], orr.at[tp, place_of], {"tp": up(tp, n)})
                )
            else:
                orr[tp, place_of] = gated[pl.ds(start, 128), :]
        if not half:
            mark('cell_lo')
            arrived(near_a)
            arrived(near_b)
            mark('near_ab')
            wpair += wo_near_swaps(x1) + wo_near_swaps(x3)
            for t in (x1, x3):
                wpair += [wo_swap(piece) for piece in wo_pieces(t, True)]
    pass_on(1)
    mark('cell_done')
    arrived(near_c)
    mark('near_c')
    arrived(xo2b)
    wpair += wo_near_swaps(x2) + [wo_swap(piece) for piece in wo_pieces(x2, True)]
    arrived(p2)
    mark('p2_arr')
    g_far1 += slab(wgv, 2)
    g_pair = row_swap(wgv)
    d_far1 = slab(wd, 0)

    mark('w2_arr')
    ld_res.wait()

    def half_rows(b, h):
        return gr.at[2 * b + h, pl.ds(16, 128)]

    s_next = [take("s") for _ in range(4)]
    r_next = take("r")

    def next_copy(t):
        return pltpu.make_async_remote_copy(
            src_ref=hs, dst_ref=hp, send_sem=ssem.at[s_next[t]], recv_sem=rsem.at[r_next],
            device_id={**at_place(place + 1), "tp": t}, device_id_type=MESH,
        )

    gather = [None, None]
    for half in (0, 1):
        at = slice(128 * half, 128 * half + 128)
        arrived(relayed[half] + a2a[half])
        mark('a2a_arr')
        if not half:
            arrived(wpair)
            mark('wpair_arr')

        def project(n, ss):
            cols = pl.ds(pl.multiple_of(n * 256, 256), 256)
            acc = rsd[at, cols].astype(F32)
            for t in range(4):
                acc = acc + jnp.dot(
                    orr[t, at], wo[t, :, :, :, :, cols].reshape(512, 256),
                    preferred_element_type=F32,
                )
            low = acc.astype(BF)
            stream[at, cols] = low
            wide = low.astype(F32)
            sq = wide * wide
            return ss + sq[:, :L] + sq[:, L:]

        ss = lax.fori_loop(0, 8, project, jnp.zeros((128, L), F32))
        norm = lax.rsqrt(jnp.sum(ss, axis=1, keepdims=True) * (1.0 / D) + EPS)

        def normed(n, _):
            cols = pl.ds(pl.multiple_of(n * 256, 256), 256)
            rows_n = (stream[at, cols].astype(F32) * norm * fgain[:, cols]).astype(BF)
            gr[2 * tp + half, pl.ds(16, 128), cols] = rows_n
            if half:
                hs[:, cols] = rows_n[126:128].astype(F32)
            return 0

        lax.fori_loop(0, 8, normed, 0)
        mark('normed')
        if half:
            halo = send(hs, hl, {"tp": x2})

            @pl.when(tp == 3)
            def _():
                for t in range(4):
                    next_copy(t).start()

        mine = half_rows(tp, half)
        gather[half] = [send(mine, mine, {"tp": x1}), send(mine, mine, {"tp": x3})]

    mark('g1_sent')
    arrived(g_far1)
    mark('gfar1_arr')
    g_far2, more = across_two(wgv)
    g_pair += more
    for n in (1, 3, 2):
        d_far1 += slab(wd, n)
    d_pair = row_swap(wd)
    arrived(gather[0])
    mark('g1a_arr')
    part_a = half_rows(x3, 0)
    g2 = [send(part_a, part_a, {"tp": x1})]
    arrived(g_far2)
    mark('gfar2_arr')
    g_pair += last_swap(wgv)
    arrived(d_far1)
    mark('dfar1_arr')
    d_far2, more = across_two(wd)
    d_pair += more
    arrived(gather[1])
    mark('g1b_arr')
    part_b = half_rows(x1, 1)
    g2.append(send(part_b, part_b, {"tp": x3}))
    arrived([halo])
    next_copy(0).wait_recv()
    mark('halo_arr')
    arrived(g_pair)
    mark('gpair_arr')

    def tail_of(two):
        return jnp.concatenate([jnp.zeros((14, D), F32), two], axis=0)

    from_before = tail_of(jnp.where(jnp.full((2, D), place, jnp.int32) == 0, 0.0, hp[...]))

    def copy_of(src, dst, dev):
        cp = pltpu.make_async_remote_copy(
            src_ref=src, dst_ref=dst, send_sem=ssem.at[take("s")], recv_sem=rsem.at[take("r")],
            device_id=dev, device_id_type=MESH,
        )
        open_sends.append(cp)
        return cp

    lo, hi = pl.ds(0, 128), pl.ds(128, 128)
    col_halves = (pl.ds(0, 1024), pl.ds(1024, 1024))
    direct = [
        (
            copy_of(ps.at[0, lo, q], rr.at[0, hi, q], {"tp": x1}),
            copy_of(ps.at[0, hi, q], rr.at[1, lo, q], {"tp": x3}),
        )
        for q in col_halves
    ]
    far = [
        (
            copy_of(ps.at[2, lo, q], rl.at[0, :, q], {"tp": x1}),
            copy_of(ps.at[2, hi, q], rl.at[1, :, q], {"tp": x3}),
        )
        for q in col_halves
    ]
    summed = [
        (
            copy_of(ps.at[1, lo, q], rr.at[0, lo, q], {"tp": x1}),
            copy_of(ps.at[1, hi, q], rr.at[1, hi, q], {"tp": x3}),
        )
        for q in col_halves
    ]

    def rows_of(i):
        pair = i // 2
        h0 = (1 - pair) * (1 - i)
        b0 = up(tp, 1 - pair + pair * (6 - 2 * i))
        b1 = up(tp, 3 * (1 - pair) + pair * (6 - 2 * i))
        return (b0, h0), (b1, 1 - h0)

    def widen(i):
        spots = rows_of(i)
        for m, (b, h) in enumerate(spots):
            if i is FIRST and m:
                near = tail_of(hl[...])
            else:
                near = gr[2 * up(b, 3 + h) + 1 - h, pl.ds(128, 16), :].astype(F32)
            starts = jnp.full((16, D), b + 4 * h, jnp.int32) == 0
            gr[2 * b + h, pl.ds(0, 16), :] = jnp.where(starts, from_before, near).astype(BF)
        e0, e1 = (2 * b + h for b, h in spots)

        def product(n):
            w = wgv[:, :, :, :, n * 256 : n * 256 + 256].reshape(D, 256)
            both = jnp.concatenate([gr[e0], gr[e1]], axis=0)
            gvs[n % 2] = jnp.dot(both, w, preferred_element_type=F32)

        def gate_of(n):
            cols = slice(n * L, n * L + L)
            for p in range(2):
                at = 144 * p + 14

                def conv(lanes, tap):
                    return (
                        tap[0:1, cols] * gvs[n % 2, at : at + 128, lanes]
                        + tap[1:2, cols] * gvs[n % 2, at + 1 : at + 129, lanes]
                        + tap[2:3, cols] * gvs[n % 2, at + 2 : at + 130, lanes]
                    )

                cg, cv = conv(slice(0, L), gtap), conv(slice(L, 256), vtap)
                hid[lax.rem(i, 2), 128 * p : 128 * p + 128, cols] = (
                    cg / (1.0 + jnp.exp(-cg)) * cv
                ).astype(BF)

        product(0)
        for n in range(1, NT):
            product(n)
            gate_of(n - 1)
        gate_of(NT - 1)

    def narrow(i, leave=None):
        for n in range(8):
            w = wd[n // 2, 2 * (n % 2) : 2 * (n % 2) + 2].reshape(256, FFD)
            p = lax.dot_general(
                hid[lax.rem(i, 2)], w, (((1,), (1,)), ((), ())), preferred_element_type=F32
            )
            ps[i, :, n * 256 : n * 256 + 256] = p.astype(BF)
            if leave and n % 4 == 3:
                leave(n // 4)

    widen(FIRST)
    mark('up0')
    arrived(d_far2)
    mark('dfar2_arr')
    d_pair += last_swap(wd)
    arrived(d_pair)
    mark('dpair_arr')

    def start_direct(m):
        for cp in direct[m]:
            cp.start()

    narrow(FIRST, start_direct)
    mark('down0')
    widen(1)
    narrow(1)
    mark('down1')
    arrived(g2)
    mark('g2_arr')

    def start_far(m):
        for cp in far[m]:
            cp.start()

    widen(2)
    narrow(2, start_far)
    mark('down2')
    widen(3)
    narrow(3)
    mark('fed')
    for m in (0, 1):
        for n, half in enumerate((lo, hi)):
            far[m][n].wait_recv()
            mark('far_arr')

            def relay(t, _):
                cols = pl.ds(pl.multiple_of(t * 256, 256), 256)
                ps[1, half, cols] = (
                    ps[1, half, cols].astype(F32) + rl[n, :, cols].astype(F32)
                ).astype(BF)
                return 0

            lax.fori_loop(4 * m, 4 * m + 4, relay, 0)
            summed[m][n].start()

    def add(n, _):
        cols = pl.ds(pl.multiple_of(n * 256, 256), 256)
        s = ps[3, :, cols].astype(F32) + rr[0, :, cols].astype(F32) + rr[1, :, cols].astype(F32)
        out[:, cols] = (stream[:, cols].astype(F32) + s).astype(BF)
        return 0

    for m in (0, 1):
        arrived(direct[m] + summed[m])
        mark('back_arr')
        lax.fori_loop(4 * m, 4 * m + 4, add, 0)

    mark('added')
    assert count['s'] <= ssem.shape[0] and count['r'] <= rsem.shape[0], count
    for cp in open_sends:
        cp.wait_send()

    mark('sends_done')
    @pl.when(tp == 3)
    def _():
        for t in range(4):
            next_copy(t).wait_send()


def local(
    residual_entry_input, query_matrix_rows, key_matrix_rows, value_matrix_rows,
    output_gate_logits, input_gate_logits, forget_gate_logits, forget_decay_offset,
    head_norm_gain, cell_output_weight, feedforward_norm_gain, gate_up_weight,
    value_up_weight, gate_filter_taps, value_filter_taps, down_projection_weight,
):
    def chunks(gate):
        return gate.T.reshape(2, CH, L).transpose(1, 0, 2).reshape(2 * CH, L)

    hbm = pl.BlockSpec(memory_space=pl.ANY)
    vmem = pl.BlockSpec(memory_space=pltpu.VMEM)
    scratch = [
        pltpu.VMEM((1024, 256), BF), pltpu.VMEM((1024, 256), BF), pltpu.VMEM((1024, 512), BF),
        pltpu.VMEM((1024, 512), BF), pltpu.VMEM((256, D), BF),
        pltpu.VMEM((4, 4, 2, 64, 2 * FFD), BF), pltpu.VMEM((4, 4, 2, 64, FFD), BF),
        pltpu.VMEM((4, 2, 2, 4, 32, D), BF),
        pltpu.VMEM((CH, 2, DK, DV + L), F32), pltpu.VMEM((CH, 2, L, DV + L), F32),
        pltpu.VMEM((L, L), F32), pltpu.VMEM((4, 2 * CH, L), F32),
        pltpu.VMEM((CH, 2, DK, DV + L), BF), pltpu.VMEM((2, DK, DV + L), F32),
        pltpu.VMEM((2, 1, L), F32), pltpu.VMEM((2 * CH, L), F32),
        pltpu.VMEM((2, DK, DV), BF), pltpu.VMEM((2, 8, L), F32),
        pltpu.VMEM((2, DK, DV), BF), pltpu.VMEM((2, 8, L), F32),
        pltpu.VMEM((4, DK, DV), BF), pltpu.VMEM((4, 8, L), F32),
        pltpu.VMEM((4, DK, DV), BF), pltpu.VMEM((4, 8, L), F32),
        pltpu.VMEM((DK, DV), BF), pltpu.VMEM((8, L), F32),
        pltpu.VMEM((DK, DV), BF), pltpu.VMEM((8, L), F32),
        pltpu.VMEM((1024, 512), BF), pltpu.VMEM((2, 2, 64, 512), BF), pltpu.VMEM((4, 256, 512), BF),
        pltpu.VMEM((256, D), BF),
        pltpu.VMEM((8, 144, D), BF), pltpu.VMEM((2, D), F32), pltpu.VMEM((2, D), F32),
        pltpu.VMEM((2, D), F32), pltpu.VMEM((2, 288, 256), F32), pltpu.VMEM((2, 256, FFD), BF),
        pltpu.VMEM((4, 256, D), BF), pltpu.VMEM((2, 128, D), BF), pltpu.VMEM((2, 256, D), BF),
        pltpu.SemaphoreType.DMA((32,)), pltpu.SemaphoreType.DMA((176,)),
        pltpu.SemaphoreType.DMA((176,)),
    ]
    return pl.pallas_call(
        kernel,
        out_shape=jax.ShapeDtypeStruct((256, D), BF),
        in_specs=[hbm, hbm, hbm, hbm, hbm, vmem, vmem, vmem, vmem, hbm, vmem, hbm, hbm, hbm, vmem, vmem],
        out_specs=vmem,
        scratch_shapes=scratch,
        compiler_params=pltpu.CompilerParams(
            collective_id=0, has_side_effects=True, vmem_limit_bytes=67_043_328
        ),
    )(
        residual_entry_input, query_matrix_rows, key_matrix_rows, value_matrix_rows,
        output_gate_logits, chunks(input_gate_logits), chunks(forget_gate_logits),
        chunks(forget_decay_offset), head_norm_gain, cell_output_weight.reshape(2, 2, 4, 32, D),
        feedforward_norm_gain.reshape(1, D), gate_up_weight, value_up_weight,
        down_projection_weight.T, gate_filter_taps, value_filter_taps,
    )


def solution(mesh):
    split = Mesh(mesh.devices.reshape(4, 4, 2, mesh.shape["tp"]), SP_TP)
    placed = (
        P(SP_TP, None), P(SP, "tp"), P(SP, "tp"), P(SP, "tp"), P(SP, "tp"), P(SP, "tp"),
        P(SP, "tp"), P(SP, "tp"), P("tp", None), P("tp", None), P(), P(SP, "tp"), P(SP, "tp"),
        P(None, "tp"), P(None, "tp"), P("tp", SP),
    )
    return jax.shard_map(
        local, mesh=split, in_specs=placed, out_specs=P(SP_TP, None), check_vma=False
    )
```

```python
import jax
import jax.numpy as jnp
from jax import lax
from jax.experimental import pallas as pl
from jax.experimental.pallas import tpu as pltpu
from jax.sharding import Mesh
from jax.sharding import PartitionSpec as P

SP = ("sp_0", "sp_1", "sp_2")
SP_TP = ("sp_0", "sp_1", "sp_2", "tp")
MESH = pl.DeviceIdType.MESH

EPS = 1e-06
FIRST = 0
NEG = -1e30
L = 128
CH = 8
DK = 128
DV = 256
D = 2048
FFD = 1408
NT = FFD // 128
SCALE = DK**-0.5
F32 = jnp.float32
BF = jnp.bfloat16


def log1p_of(e):
    series = e * (1.0 - e * (0.5 - e * (1.0 / 3.0 - e * (0.25 - e * 0.2))))
    return jnp.where(e < 0.03, series, jnp.log(1.0 + e))


def kernel(
    res, q_in, k_in, v_in, og_in, ig, fg, off, gain, wo_in, fgain, gup, vup, dwn, gtap, vtap,
    out,
    q, k, v, og, rsd, wgv, wd, wo, dc, nl, colt, rows, cs, cpri, mpri, rs_rows,
    st1, ax1, st1r, ax1r, st2, ax2, st3, ax3, st4, ax4, st4r, ax4r,
    gated, al, orr, stream, gr, hs, hl, hp, gvs, hid, ps, rl, rr,
    lsem, ssem, rsem,
):
    z, y, c, tp = (lax.axis_index(a) for a in SP_TP)

    def up(i, n):
        return lax.rem(i + n, 4)

    y1, y3 = up(y, 1), up(y, 3)
    z1, z3 = up(z, 1), up(z, 3)
    x1, x2, x3 = up(tp, 1), up(tp, 2), up(tp, 3)
    other = 1 - c
    place = z * 8 + y * 2 + c

    def at_place(n):
        n = lax.rem(n + 32, 32)
        return {"sp_0": n // 8, "sp_1": lax.rem(n // 2, 4), "sp_2": lax.rem(n, 2)}

    count = {"l": 0, "s": 0, "r": 0}
    open_sends = []

    def take(kind):
        count[kind] += 1
        return count[kind] - 1

    def load(src, dst):
        cp = pltpu.make_async_copy(src, dst, lsem.at[take("l")])
        cp.start()
        return cp

    def send(src, dst, dev):
        cp = pltpu.make_async_remote_copy(
            src_ref=src, dst_ref=dst, send_sem=ssem.at[take("s")], recv_sem=rsem.at[take("r")],
            device_id=dev, device_id_type=MESH,
        )
        cp.start()
        open_sends.append(cp)
        return cp

    def arrived(copies):
        for cp in copies:
            cp.wait_recv()

    def mark(name):
        pass

    mark('entry')
    ld_k = load(k_in, k)
    ld_v = load(v_in, v)
    ld_w = [load(dwn, wd.at[z, y, c])]
    for n in range(NT):
        ld_w.append(load(gup.at[:, pl.ds(n * 128, 128)], wgv.at[z, y, c, :, pl.ds(n * 256, 128)]))
        ld_w.append(load(vup.at[:, pl.ds(n * 128, 128)], wgv.at[z, y, c, :, pl.ds(n * 256 + 128, 128)]))
    ld_wo = load(wo_in, wo.at[tp])
    ld_q = load(q_in, q)
    ld_og = load(og_in, og)
    ld_res = load(res, rsd)

    barrier = pltpu.get_barrier_semaphore()

    def hello(dev):
        pl.semaphore_signal(barrier, inc=1, device_id=dev, device_id_type=MESH)

    hello({"sp_2": other})
    for n in (1, 2, 3):
        hello({"sp_1": up(y, n)})
        hello({"sp_0": up(z, n)})
        hello({"tp": up(tp, n)})
    hello({**at_place(place - 1), "tp": 3})

    @pl.when(tp == 3)
    def _():
        for t in range(4):
            hello({**at_place(place + 1), "tp": t})
        pl.semaphore_wait(barrier, 15)

    @pl.when(tp != 3)
    def _():
        pl.semaphore_wait(barrier, 11)

    def halves(ref, zz, yy, lo, n):
        return ref.at[zz, yy, c, pl.ds(lo, n)]

    mark('barrier_done')
    for cp in ld_w:
        cp.wait()
    p1 = []
    for ref in (wgv, wd):
        mine_a, mine_b = halves(ref, z, y, 0, 32), halves(ref, z, y, 32, 32)
        p1 += [
            send(mine_a, mine_a, {"sp_1": y1}),
            send(mine_a, mine_a, {"sp_1": y3}),
            send(mine_b, mine_b, {"sp_0": z1}),
            send(mine_b, mine_b, {"sp_0": z3}),
        ]
    mark('w_issued')
    ld_wo.wait()
    y2, z2 = up(y, 2), up(z, 2)

    def wo_pieces(t, far):
        return wo.at[t, c, 0, y2 if far else y], wo.at[t, c, 1, z2 if far else z]

    xo1a, xo1b = (
        [send(piece, piece, {"tp": dev}) for piece in wo_pieces(tp, n) for dev in (x1, x3)]
        for n in (False, True)
    )

    def wo_swap(piece):
        return send(piece, piece, {"sp_2": other})

    def wo_onward(far):
        py, pz = wo_pieces(x3, far)[0], wo_pieces(x1, far)[1]
        return [send(py, py, {"tp": x1}), send(pz, pz, {"tp": x3})]

    def wo_spread(t):
        py, pz = wo_pieces(t, False)
        near = [
            send(py, py, {"sp_1": y1}), send(py, py, {"sp_1": y3}),
            send(pz, pz, {"sp_0": z1}), send(pz, pz, {"sp_0": z3}),
        ]
        return near, [wo_swap(py), wo_swap(pz)]

    def wo_near_swaps(t):
        return [
            wo_swap(piece)
            for piece in (
                wo.at[t, c, 0, y1], wo.at[t, c, 0, y3], wo.at[t, c, 1, z1], wo.at[t, c, 1, z3]
            )
        ]

    def slab(ref, n):
        piece_a, piece_b = halves(ref, z, up(y, n), 0, 32), halves(ref, up(z, n), y, 32, 32)
        return [
            send(piece_a, piece_a, {"sp_0": z1}),
            send(piece_a, piece_a, {"sp_0": z3}),
            send(piece_b, piece_b, {"sp_1": y1}),
            send(piece_b, piece_b, {"sp_1": y3}),
        ]

    def row_swap(ref):
        row_a = ref.at[z, :, c, pl.ds(0, 32)]
        row_b = ref.at[:, y, c, pl.ds(32, 32)]
        return [send(row_a, row_a, {"sp_2": other}), send(row_b, row_b, {"sp_2": other})]

    def across_two(ref):
        far = [
            send(src, src, dev)
            for src, dev in (
                (ref.at[z3, :, c, pl.ds(0, 16)], {"sp_0": z1}),
                (ref.at[z1, :, c, pl.ds(16, 16)], {"sp_0": z3}),
                (ref.at[:, y3, c, pl.ds(32, 16)], {"sp_1": y1}),
                (ref.at[:, y1, c, pl.ds(48, 16)], {"sp_1": y3}),
            )
        ]
        swap = [
            send(src, src, {"sp_2": other})
            for src in (
                ref.at[z1, :, c, pl.ds(0, 32)],
                ref.at[z3, :, c, pl.ds(0, 32)],
                ref.at[:, y1, c, pl.ds(32, 32)],
                ref.at[:, y3, c, pl.ds(32, 32)],
            )
        ]
        return far, swap

    def last_swap(ref):
        return [
            send(src, src, {"sp_2": other})
            for src in (ref.at[z2, :, c, pl.ds(0, 32)], ref.at[:, y2, c, pl.ds(32, 32)])
        ]

    mark('wo_issued')
    il = 15.0 * jnp.tanh(ig[...] / 15.0)
    xf = 15.0 * jnp.tanh(fg[...] / 15.0)
    fl = jnp.minimum(xf, 0.0) - log1p_of(jnp.exp(-jnp.abs(xf))) + off[...]
    r_i = lax.broadcasted_iota(jnp.int32, (L, L), 0)
    c_i = lax.broadcasted_iota(jnp.int32, (L, L), 1)
    causal = r_i >= c_i
    upper = (r_i <= c_i).astype(F32)
    cum = jnp.dot(fl, upper, preferred_element_type=F32, precision=lax.Precision.HIGHEST)
    a = il - cum
    lane = lax.broadcasted_iota(jnp.int32, (2 * CH, L), 1)
    cm = a
    for s in (1, 2, 4, 8, 16, 32, 64):
        cm = jnp.where(lane >= s, jnp.maximum(cm, pltpu.roll(cm, s, 1)), cm)
    last = jnp.broadcast_to(cum[:, L - 1 :], (2 * CH, L))
    peak = jnp.broadcast_to(cm[:, L - 1 :], (2 * CH, L))
    weight = jnp.exp(a - peak)
    mm = last + peak
    rows[0], rows[1], rows[2], rows[3] = a, weight, last, mm
    colt[...] = jnp.transpose(jnp.concatenate([cm, cum, jnp.zeros((96, L), F32)], axis=0))

    mark('gates')
    ld_k.wait()
    ld_v.wait()

    def chunk_state(j, _):
        at = pl.ds(pl.multiple_of(j * L, L), L)
        for h in range(2):
            kt = jnp.transpose(k[at, h * DK : (h + 1) * DK].astype(F32))
            kw = kt * rows[1, pl.ds(2 * j + h, 1), :]
            dc[j, h, :, :DV] = jnp.dot(
                kw.astype(BF), v[at, h * DV : (h + 1) * DV], preferred_element_type=F32
            )
            dc[j, h, :, DV:] = jnp.broadcast_to(jnp.sum(kw, axis=1, keepdims=True), (DK, L))
        return 0

    lax.fori_loop(0, CH, chunk_state, 0)

    mark('chunkstates')
    for h in range(2):
        tot = jnp.zeros((1, L), F32)
        logs = [None] * CH
        for j in reversed(range(CH)):
            row = 2 * j + h
            logs[j] = mm[row : row + 1] + tot
            tot = tot + last[row : row + 1]
        m = logs[0]
        for j in range(1, CH):
            m = jnp.maximum(m, logs[j])
        total = jnp.zeros((DK, DV + L), F32)
        for j in range(CH):
            total = total + jnp.exp(logs[j] - m)[:, 0:1] * dc[j, h]
        st1[h] = total[:, :DV].astype(BF)
        n_row = jnp.transpose(total[:, DV:])[0:1]
        ax1[h] = jnp.concatenate([n_row, tot, m, jnp.zeros((5, L), F32)], axis=0)

    mark('devstate')
    s1 = [send(st1, st1r, {"sp_2": other}), send(ax1, ax1r, {"sp_2": other})]

    ld_q.wait()

    def within(j, _):
        at = pl.ds(pl.multiple_of(j * L, L), L)
        turned = pltpu.roll(colt[...], lax.rem(L - 2 * j, L), 1)
        for h in range(2):
            raw = lax.dot_general(
                q[at, h * DK : (h + 1) * DK], k[at, h * DK : (h + 1) * DK],
                (((1,), (1,)), ((), ())), preferred_element_type=F32,
            ) * SCALE
            logit = rows[0, pl.ds(2 * j + h, 1), :] - turned[:, h : h + 1]
            sc = raw * jnp.exp(jnp.where(causal, logit, NEG))
            nl[j, h, :, :DV] = jnp.dot(
                sc.astype(BF), v[at, h * DV : (h + 1) * DV], preferred_element_type=F32
            )
            nl[j, h, :, DV:] = jnp.broadcast_to(jnp.sum(sc, axis=1, keepdims=True), (L, L))
        return 0

    lax.fori_loop(0, 2, within, 0)

    mark('within2')
    cf = jnp.full((1, L), c, jnp.int32).astype(F32)
    arrived(s1)

    def aux(ref, *at):
        block = ref[at] if at else ref[...]
        return block[0:1], block[1:2], block[2:3]

    def pack(n, tot, m):
        return jnp.concatenate([n, tot, m, jnp.zeros((5, L), F32)], axis=0)

    mark('s1_arr')
    n_o, t_o, m_o = aux(ax1, c)
    n_r, t_r, m_r = aux(ax1r, c)
    log_o = m_o + (1.0 - cf) * t_r
    log_r = m_r + cf * t_o
    m = jnp.maximum(log_o, log_r)
    w_o, w_r = jnp.exp(log_o - m), jnp.exp(log_r - m)
    st2[0] = (w_o[:, 0:1] * st1[c].astype(F32) + w_r[:, 0:1] * st1r[c].astype(F32)).astype(BF)
    ax2[0] = pack(w_o * n_o + w_r * n_r, t_o + t_r, m)
    s2 = []
    for n in (1, 2, 3):
        s2.append(send(st2.at[0], st2.at[n], {"sp_1": up(y, n)}))
        s2.append(send(ax2.at[0], ax2.at[n], {"sp_1": up(y, n)}))

    mark('s2_sent')
    lax.fori_loop(2, 5, within, 0)

    def scan_of(st, ax, me, whole):
        parts = [aux(ax, n) for n in range(4)]
        mine = jnp.full((1, L), me, jnp.int32)
        below = [None] + [mine >= n for n in (1, 2, 3)]
        zero = jnp.zeros((1, L), F32)
        after = zero
        for n in (1, 2, 3):
            after = after + jnp.where(below[n], 0.0, parts[n][1])
        run, run_up = zero, zero
        log_in, log_all = [None] * 4, [parts[0][2] + after] + [None] * 3
        for n in (1, 2, 3):
            log_in[n] = jnp.where(below[n], parts[n][2] + run, NEG)
            log_all[n] = jnp.where(
                below[n], parts[n][2] + run + parts[0][1] + after, parts[n][2] + run_up
            )
            run = run + jnp.where(below[n], parts[n][1], 0.0)
            run_up = run_up + jnp.where(below[n], 0.0, parts[n][1])
        m_in = jnp.maximum(jnp.maximum(log_in[1], log_in[2]), log_in[3])
        w_in = [None] + [jnp.where(below[n], jnp.exp(log_in[n] - m_in), 0.0) for n in (1, 2, 3)]
        blocks = [st[n].astype(F32) for n in range(4)]
        c_in = sum(w_in[n][:, 0:1] * blocks[n] for n in (1, 2, 3))
        n_in = sum(w_in[n] * parts[n][0] for n in (1, 2, 3))
        inside = (c_in, n_in, run, m_in)
        if not whole:
            return inside, None
        m_all = jnp.maximum(
            jnp.maximum(log_all[0], log_all[1]), jnp.maximum(log_all[2], log_all[3])
        )
        w_all = [jnp.exp(t - m_all) for t in log_all]
        c_all = sum(w_all[n][:, 0:1] * blocks[n] for n in range(4))
        n_all = sum(w_all[n] * parts[n][0] for n in range(4))
        return inside, (c_all, n_all, run + run_up + parts[0][1], m_all)

    mark('within5')
    arrived(s2)
    mark('s2_arr')
    y_in, y_all = scan_of(st2, ax2, y, True)
    st3[0] = y_all[0].astype(BF)
    ax3[0] = pack(*y_all[1:])
    s3 = []
    for n in (1, 2, 3):
        s3.append(send(st3.at[0], st3.at[n], {"sp_0": up(z, n)}))
        s3.append(send(ax3.at[0], ax3.at[n], {"sp_0": up(z, n)}))
    cpri[0, :, :DV] = y_in[0]

    mark('s3_sent')
    arrived(xo1a)
    xo2a = wo_onward(False)
    near_a, wpair = wo_spread(x1)
    near_b, more = wo_spread(x3)
    wpair += more
    mark('xo1_arr')
    mark('p2_sent')
    lax.fori_loop(5, CH, within, 0)

    mark('within8')
    arrived(xo1b)
    xo2b = wo_onward(True)
    arrived(xo2a)
    mark('xo2_arr')
    near_c, more = wo_spread(x2)
    wpair += more
    arrived(p1)
    p2 = []
    for ref in (wgv, wd):
        for src, dev in (
            (halves(ref, z, y3, 0, 16), {"sp_1": y1}),
            (halves(ref, z, y1, 16, 16), {"sp_1": y3}),
            (halves(ref, z3, y, 32, 16), {"sp_0": z1}),
            (halves(ref, z1, y, 48, 16), {"sp_0": z3}),
        ):
            p2.append(send(src, src, dev))
    g_far1 = slab(wgv, 0) + slab(wgv, 1) + slab(wgv, 3)
    arrived(s3)
    mark('s3_arr')
    z_in, _ = scan_of(st3, ax3, z, False)
    m = jnp.maximum(y_in[2] + z_in[3], y_in[3])
    w_z, w_y = jnp.exp(y_in[2] + z_in[3] - m), jnp.exp(y_in[3] - m)
    st4[...] = (w_z[:, 0:1] * z_in[0] + w_y[:, 0:1] * cpri[0, :, :DV]).astype(BF)
    ax4[...] = pack(w_z * z_in[1] + w_y * y_in[1], z_in[2] + y_in[2], m)
    s4 = [send(st4, st4r, {"sp_2": other}), send(ax4, ax4r, {"sp_2": other})]

    mark('s4_sent')
    arrived(s4)
    mark('s4_arr')
    last_in = jnp.full((1, L), c, jnp.int32) == 1
    for h, st, ax in ((c, st4, ax4), (other, st4r, ax4r)):
        n_b, t_b, m_b = aux(ax)
        n_p, t_p, m_p = aux(ax1r, h)
        m_p = jnp.where(last_in, m_p, NEG)
        m_b = m_b + cf * t_p
        m = jnp.maximum(m_b, m_p)
        w_b, w_p = jnp.exp(m_b - m), jnp.where(last_in, jnp.exp(m_p - m), 0.0)
        cpri[h, :, :DV] = w_b[:, 0:1] * st[...].astype(F32) + w_p[:, 0:1] * st1r[h].astype(F32)
        n_row = w_b * n_b + w_p * n_p
        cpri[h, :, DV:] = jnp.transpose(jnp.broadcast_to(n_row, (L, L)))
        mpri[h] = m

    def carry(j, _):
        for h in range(2):
            state, m_old = cpri[h], mpri[h]
            cs[j, h] = state.astype(BF)
            row = pl.ds(2 * j + h, 1)
            rs_rows[row, :] = m_old
            decayed, fresh = rows[2, row, :] + m_old, rows[3, row, :]
            m_new = jnp.maximum(decayed, fresh)
            cpri[h] = (
                jnp.exp(decayed - m_new)[:, 0:1] * state
                + jnp.exp(fresh - m_new)[:, 0:1] * dc[j, h]
            )
            mpri[h] = m_new
        return 0

    mark('prior')
    lax.fori_loop(0, CH, carry, 0)

    mark('carried')
    ld_og.wait()

    def finish(j, _):
        at = pl.ds(pl.multiple_of(j * L, L), L)
        turned = pltpu.roll(colt[...], lax.rem(L - 2 * j, L), 1)
        for h in range(2):
            r = rs_rows[pl.ds(2 * j + h, 1), :][:, 0:1]
            cmc, cuc = turned[:, h : h + 1], turned[:, 16 + h : 17 + h]
            g = jnp.maximum(cmc, r)
            e1, e2 = jnp.exp(cmc - g), jnp.exp(r - g) * SCALE
            qc = jnp.dot(q[at, h * DK : (h + 1) * DK], cs[j, h], preferred_element_type=F32)
            both = e1 * nl[j, h] + e2 * qc
            inv = 1.0 / jnp.maximum(jnp.abs(both[:, DV:]), jnp.exp(-cuc - g))
            mo = both[:, :DV] * jnp.concatenate([inv, inv], axis=1)
            norm = lax.rsqrt(jnp.mean(mo * mo, axis=1, keepdims=True) + EPS)
            gate = jax.nn.sigmoid(og[at, h * DV : (h + 1) * DV].astype(F32))
            gated[at, h * DV : (h + 1) * DV] = (mo * norm * gain[h : h + 1, :] * gate).astype(BF)
        return 0

    a2a, legs, relayed = [[], []], [None, None], [None, None]

    def pass_on(half):
        arrived(legs[half])
        relayed[half] = [
            send(al.at[half, 0], orr.at[x3, pl.ds(128 * half, 64)], {"tp": x1}),
            send(al.at[half, 1], orr.at[x1, pl.ds(128 * half + 64, 64)], {"tp": x3}),
        ]

    for half in (0, 1):
        for n in (2, 1, 3, 0):
            j = 2 * up(tp, n) + half
            lax.fori_loop(j, j + 1, finish, 0)
            start = pl.multiple_of(j * L, L)
            place_of = pl.ds(128 * half, 128)
            if n == 2:
                legs[half] = [
                    send(gated.at[pl.ds(start, 64)], al.at[half, 0], {"tp": x1}),
                    send(gated.at[pl.ds(start + 64, 64)], al.at[half, 1], {"tp": x3}),
                ]
                if half:
                    mark('cell_hi2')
                    pass_on(0)
                    mark('leg0_arr')
            elif n:
                a2a[half].append(
                    send(gated.at[pl.ds(start, 128)], orr.at[tp, place_of], {"tp": up(tp, n)})
                )
            else:
                orr[tp, place_of] = gated[pl.ds(start, 128), :]
        if not half:
            mark('cell_lo')
            arrived(near_a)
            arrived(near_b)
            mark('near_ab')
            wpair += wo_near_swaps(x1) + wo_near_swaps(x3)
            for t in (x1, x3):
                wpair += [wo_swap(piece) for piece in wo_pieces(t, True)]
    pass_on(1)
    mark('cell_done')
    arrived(near_c)
    mark('near_c')
    arrived(xo2b)
    wpair += wo_near_swaps(x2) + [wo_swap(piece) for piece in wo_pieces(x2, True)]
    arrived(p2)
    mark('p2_arr')
    g_far1 += slab(wgv, 2)
    g_pair = row_swap(wgv)
    d_far1 = slab(wd, 0)

    mark('w2_arr')
    ld_res.wait()

    def half_rows(b, h):
        return gr.at[2 * b + h, pl.ds(16, 128)]

    s_next = [take("s") for _ in range(4)]
    r_next = take("r")

    def next_copy(t):
        return pltpu.make_async_remote_copy(
            src_ref=hs, dst_ref=hp, send_sem=ssem.at[s_next[t]], recv_sem=rsem.at[r_next],
            device_id={**at_place(place + 1), "tp": t}, device_id_type=MESH,
        )

    gather = [None, None]
    for half in (0, 1):
        at = slice(128 * half, 128 * half + 128)
        arrived(relayed[half] + a2a[half])
        mark('a2a_arr')
        if not half:
            arrived(wpair)
            mark('wpair_arr')

        def project(n, ss):
            cols = pl.ds(pl.multiple_of(n * 256, 256), 256)
            acc = rsd[at, cols].astype(F32)
            for t in range(4):
                acc = acc + jnp.dot(
                    orr[t, at], wo[t, :, :, :, :, cols].reshape(512, 256),
                    preferred_element_type=F32,
                )
            low = acc.astype(BF)
            stream[at, cols] = low
            wide = low.astype(F32)
            sq = wide * wide
            return ss + sq[:, :L] + sq[:, L:]

        ss = lax.fori_loop(0, 8, project, jnp.zeros((128, L), F32))
        norm = lax.rsqrt(jnp.sum(ss, axis=1, keepdims=True) * (1.0 / D) + EPS)

        def normed(n, _):
            cols = pl.ds(pl.multiple_of(n * 256, 256), 256)
            rows_n = (stream[at, cols].astype(F32) * norm * fgain[:, cols]).astype(BF)
            gr[2 * tp + half, pl.ds(16, 128), cols] = rows_n
            if half:
                hs[:, cols] = rows_n[126:128].astype(F32)
            return 0

        lax.fori_loop(0, 8, normed, 0)
        mark('normed')
        if half:
            halo = send(hs, hl, {"tp": x2})

            @pl.when(tp == 3)
            def _():
                for t in range(4):
                    next_copy(t).start()

        mine = half_rows(tp, half)
        gather[half] = [send(mine, mine, {"tp": x1}), send(mine, mine, {"tp": x3})]

    mark('g1_sent')
    arrived(g_far1)
    mark('gfar1_arr')
    g_far2, more = across_two(wgv)
    g_pair += more
    for n in (1, 3, 2):
        d_far1 += slab(wd, n)
    d_pair = row_swap(wd)
    arrived(gather[0])
    mark('g1a_arr')

    def onward(h):
        part_a = gr.at[2 * x3 + h, pl.ds(16, 64)]
        part_b = gr.at[2 * x1 + h, pl.ds(80, 64)]
        return [send(part_a, part_a, {"tp": x1}), send(part_b, part_b, {"tp": x3})]

    g2 = onward(0)
    arrived(g_far2)
    mark('gfar2_arr')
    g_pair += last_swap(wgv)
    arrived(d_far1)
    mark('dfar1_arr')
    d_far2, more = across_two(wd)
    d_pair += more
    arrived(gather[1])
    mark('g1b_arr')
    g2 += onward(1)
    arrived([halo])
    next_copy(0).wait_recv()
    mark('halo_arr')
    arrived(g_pair)
    mark('gpair_arr')

    def tail_of(two):
        return jnp.concatenate([jnp.zeros((14, D), F32), two], axis=0)

    from_before = tail_of(jnp.where(jnp.full((2, D), place, jnp.int32) == 0, 0.0, hp[...]))

    def copy_of(src, dst, dev):
        cp = pltpu.make_async_remote_copy(
            src_ref=src, dst_ref=dst, send_sem=ssem.at[take("s")], recv_sem=rsem.at[take("r")],
            device_id=dev, device_id_type=MESH,
        )
        open_sends.append(cp)
        return cp

    lo, hi = pl.ds(0, 128), pl.ds(128, 128)
    col_halves = (pl.ds(0, 1024), pl.ds(1024, 1024))
    direct = [
        (
            copy_of(ps.at[0, lo, q], rr.at[0, hi, q], {"tp": x1}),
            copy_of(ps.at[0, hi, q], rr.at[1, lo, q], {"tp": x3}),
        )
        for q in col_halves
    ]
    far = [
        (
            copy_of(ps.at[2, lo, q], rl.at[0, :, q], {"tp": x1}),
            copy_of(ps.at[2, hi, q], rl.at[1, :, q], {"tp": x3}),
        )
        for q in col_halves
    ]
    summed = [
        (
            copy_of(ps.at[1, lo, q], rr.at[0, lo, q], {"tp": x1}),
            copy_of(ps.at[1, hi, q], rr.at[1, hi, q], {"tp": x3}),
        )
        for q in col_halves
    ]

    def rows_of(i):
        pair = i // 2
        h0 = (1 - pair) * (1 - i)
        b0 = up(tp, 1 - pair + pair * (6 - 2 * i))
        b1 = up(tp, 3 * (1 - pair) + pair * (6 - 2 * i))
        return (b0, h0), (b1, 1 - h0)

    def widen(i):
        spots = rows_of(i)
        for m, (b, h) in enumerate(spots):
            if i is FIRST and m:
                near = tail_of(hl[...])
            else:
                near = gr[2 * up(b, 3 + h) + 1 - h, pl.ds(128, 16), :].astype(F32)
            starts = jnp.full((16, D), b + 4 * h, jnp.int32) == 0
            gr[2 * b + h, pl.ds(0, 16), :] = jnp.where(starts, from_before, near).astype(BF)
        e0, e1 = (2 * b + h for b, h in spots)

        def product(n):
            w = wgv[:, :, :, :, n * 256 : n * 256 + 256].reshape(D, 256)
            both = jnp.concatenate([gr[e0], gr[e1]], axis=0)
            gvs[n % 2] = jnp.dot(both, w, preferred_element_type=F32)

        def gate_of(n):
            cols = slice(n * L, n * L + L)
            for p in range(2):
                at = 144 * p + 14

                def conv(lanes, tap):
                    return (
                        tap[0:1, cols] * gvs[n % 2, at : at + 128, lanes]
                        + tap[1:2, cols] * gvs[n % 2, at + 1 : at + 129, lanes]
                        + tap[2:3, cols] * gvs[n % 2, at + 2 : at + 130, lanes]
                    )

                cg, cv = conv(slice(0, L), gtap), conv(slice(L, 256), vtap)
                hid[lax.rem(i, 2), 128 * p : 128 * p + 128, cols] = (
                    cg / (1.0 + jnp.exp(-cg)) * cv
                ).astype(BF)

        product(0)
        for n in range(1, NT):
            product(n)
            gate_of(n - 1)
        gate_of(NT - 1)

    def narrow(i, leave=None):
        for n in range(8):
            w = wd[n // 2, 2 * (n % 2) : 2 * (n % 2) + 2].reshape(256, FFD)
            p = lax.dot_general(
                hid[lax.rem(i, 2)], w, (((1,), (1,)), ((), ())), preferred_element_type=F32
            )
            ps[i, :, n * 256 : n * 256 + 256] = p.astype(BF)
            if leave and n % 4 == 3:
                leave(n // 4)

    widen(FIRST)
    mark('up0')
    arrived(d_far2)
    mark('dfar2_arr')
    d_pair += last_swap(wd)
    arrived(d_pair)
    mark('dpair_arr')

    def start_direct(m):
        for cp in direct[m]:
            cp.start()

    narrow(FIRST, start_direct)
    mark('down0')
    widen(1)
    narrow(1)
    mark('down1')
    arrived(g2)
    mark('g2_arr')

    def start_far(m):
        for cp in far[m]:
            cp.start()

    widen(2)
    narrow(2, start_far)
    mark('down2')
    widen(3)
    narrow(3)
    mark('fed')
    for m in (0, 1):
        for n, half in enumerate((lo, hi)):
            far[m][n].wait_recv()
            mark('far_arr')

            def relay(t, _):
                cols = pl.ds(pl.multiple_of(t * 256, 256), 256)
                ps[1, half, cols] = (
                    ps[1, half, cols].astype(F32) + rl[n, :, cols].astype(F32)
                ).astype(BF)
                return 0

            lax.fori_loop(4 * m, 4 * m + 4, relay, 0)
            summed[m][n].start()

    def add(n, _):
        cols = pl.ds(pl.multiple_of(n * 256, 256), 256)
        s = ps[3, :, cols].astype(F32) + rr[0, :, cols].astype(F32) + rr[1, :, cols].astype(F32)
        out[:, cols] = (stream[:, cols].astype(F32) + s).astype(BF)
        return 0

    for m in (0, 1):
        arrived(direct[m] + summed[m])
        mark('back_arr')
        lax.fori_loop(4 * m, 4 * m + 4, add, 0)

    mark('added')
    assert count['s'] <= ssem.shape[0] and count['r'] <= rsem.shape[0], count
    for cp in open_sends:
        cp.wait_send()

    mark('sends_done')
    @pl.when(tp == 3)
    def _():
        for t in range(4):
            next_copy(t).wait_send()


def local(
    residual_entry_input, query_matrix_rows, key_matrix_rows, value_matrix_rows,
    output_gate_logits, input_gate_logits, forget_gate_logits, forget_decay_offset,
    head_norm_gain, cell_output_weight, feedforward_norm_gain, gate_up_weight,
    value_up_weight, gate_filter_taps, value_filter_taps, down_projection_weight,
):
    def chunks(gate):
        return gate.T.reshape(2, CH, L).transpose(1, 0, 2).reshape(2 * CH, L)

    hbm = pl.BlockSpec(memory_space=pl.ANY)
    vmem = pl.BlockSpec(memory_space=pltpu.VMEM)
    scratch = [
        pltpu.VMEM((1024, 256), BF), pltpu.VMEM((1024, 256), BF), pltpu.VMEM((1024, 512), BF),
        pltpu.VMEM((1024, 512), BF), pltpu.VMEM((256, D), BF),
        pltpu.VMEM((4, 4, 2, 64, 2 * FFD), BF), pltpu.VMEM((4, 4, 2, 64, FFD), BF),
        pltpu.VMEM((4, 2, 2, 4, 32, D), BF),
        pltpu.VMEM((CH, 2, DK, DV + L), F32), pltpu.VMEM((CH, 2, L, DV + L), F32),
        pltpu.VMEM((L, L), F32), pltpu.VMEM((4, 2 * CH, L), F32),
        pltpu.VMEM((CH, 2, DK, DV + L), BF), pltpu.VMEM((2, DK, DV + L), F32),
        pltpu.VMEM((2, 1, L), F32), pltpu.VMEM((2 * CH, L), F32),
        pltpu.VMEM((2, DK, DV), BF), pltpu.VMEM((2, 8, L), F32),
        pltpu.VMEM((2, DK, DV), BF), pltpu.VMEM((2, 8, L), F32),
        pltpu.VMEM((4, DK, DV), BF), pltpu.VMEM((4, 8, L), F32),
        pltpu.VMEM((4, DK, DV), BF), pltpu.VMEM((4, 8, L), F32),
        pltpu.VMEM((DK, DV), BF), pltpu.VMEM((8, L), F32),
        pltpu.VMEM((DK, DV), BF), pltpu.VMEM((8, L), F32),
        pltpu.VMEM((1024, 512), BF), pltpu.VMEM((2, 2, 64, 512), BF), pltpu.VMEM((4, 256, 512), BF),
        pltpu.VMEM((256, D), BF),
        pltpu.VMEM((8, 144, D), BF), pltpu.VMEM((2, D), F32), pltpu.VMEM((2, D), F32),
        pltpu.VMEM((2, D), F32), pltpu.VMEM((2, 288, 256), F32), pltpu.VMEM((2, 256, FFD), BF),
        pltpu.VMEM((4, 256, D), BF), pltpu.VMEM((2, 128, D), BF), pltpu.VMEM((2, 256, D), BF),
        pltpu.SemaphoreType.DMA((32,)), pltpu.SemaphoreType.DMA((176,)),
        pltpu.SemaphoreType.DMA((176,)),
    ]
    return pl.pallas_call(
        kernel,
        out_shape=jax.ShapeDtypeStruct((256, D), BF),
        in_specs=[hbm, hbm, hbm, hbm, hbm, vmem, vmem, vmem, vmem, hbm, vmem, hbm, hbm, hbm, vmem, vmem],
        out_specs=vmem,
        scratch_shapes=scratch,
        compiler_params=pltpu.CompilerParams(
            collective_id=0, has_side_effects=True, vmem_limit_bytes=67_043_328
        ),
    )(
        residual_entry_input, query_matrix_rows, key_matrix_rows, value_matrix_rows,
        output_gate_logits, chunks(input_gate_logits), chunks(forget_gate_logits),
        chunks(forget_decay_offset), head_norm_gain, cell_output_weight.reshape(2, 2, 4, 32, D),
        feedforward_norm_gain.reshape(1, D), gate_up_weight, value_up_weight,
        down_projection_weight.T, gate_filter_taps, value_filter_taps,
    )


def solution(mesh):
    split = Mesh(mesh.devices.reshape(4, 4, 2, mesh.shape["tp"]), SP_TP)
    placed = (
        P(SP_TP, None), P(SP, "tp"), P(SP, "tp"), P(SP, "tp"), P(SP, "tp"), P(SP, "tp"),
        P(SP, "tp"), P(SP, "tp"), P("tp", None), P("tp", None), P(), P(SP, "tp"), P(SP, "tp"),
        P(None, "tp"), P(None, "tp"), P("tp", SP),
    )
    return jax.shard_map(
        local, mesh=split, in_specs=placed, out_specs=P(SP_TP, None), check_vma=False
    )
```
